128 devices in a mesh: sp: 64 (over z, y, x), tp: 2 (over core).
Axes of the slice: x: 4, y: 4, z: 4, core: 2. Of those that a mesh axis runs over, the one named last changes fastest.
Arguments:
- out_grad: bfloat16 [14336, 2048], P('sp'), may hold values from -16 to 16
- routes: int32 [14336, 2], P('sp'), may hold values from 0 to 63, all different within a row; in each aligned block of 224 rows (0 to 223, 224 to 447, ...) at most 18 rows name the same one
- route_weights: float32 [14336, 2], P('sp'), may hold values from 0.5 to 2
- routed_rows: bfloat16 [64, 64, 18, 2048], P('sp'), may hold values from -6 to 6
- gate_weight: bfloat16 [64, 2048, 1024], P('sp', None, 'tp'), may hold values from -0.125 to 0.125
- up_weight: bfloat16 [64, 2048, 1024], P('sp', None, 'tp'), may hold values from -0.125 to 0.125
- down_weight: bfloat16 [64, 1024, 2048], P('sp', 'tp'), may hold values from -0.1875 to 0.1875
- values: bfloat16 [14336, 1024], P('sp', 'tp'), may hold values from -0.625 to 0.625
- key_side: bfloat16 [14336, 512], P('sp', 'tp'), may hold values from -0.625 to 0.625
- query_side: bfloat16 [14336, 512], P('sp', 'tp'), may hold values from -0.625 to 0.625
- decay_log: float32 [16, 14336], P('tp', 'sp'), may hold values from -0.09 to 0, as said below
- gate_in: bfloat16 [14336, 1024], P('sp', 'tp'), may hold values from -6 to 6
- entry_states: float32 [64, 16, 64, 128], P('sp', 'tp'), may hold values from -6 to 6
- out_weight: bfloat16 [2048, 1024], P(None, 'tp'), may hold values from -0.1875 to 0.1875
Outputs:
- grad_hidden: bfloat16 [14336, 2048], P('sp')
- grad_gate_weight: bfloat16 [64, 2048, 1024], P('sp', None, 'tp')
- grad_up_weight: bfloat16 [64, 2048, 1024], P('sp', None, 'tp')
- grad_down_weight: bfloat16 [64, 1024, 2048], P('sp', 'tp')
- grad_out_weight: float32 [2048, 1024], P('sp', 'tp')
- grad_values: bfloat16 [14336, 1024], P('sp', 'tp')
- grad_key_side: bfloat16 [14336, 512], P('sp', 'tp')
- grad_query_side: bfloat16 [14336, 512], P('sp', 'tp')
- grad_decay: float32 [16, 14336], P('tp', 'sp')
- grad_gate_in: bfloat16 [14336, 1024], P('sp', 'tp')
The draws below stay inside these ranges and needn't reach their ends.
Inputs may be any that keep to these rules, and one draw needn't show every extreme that they name: Each row names 2 different experts. Among the routes of one segment of 224 tokens no expert is named more than 18 times, and in some segments one expert is named exactly 18 times. `decay_log`: every entry is negative.
All inputs are finite; a program needn't handle non-finite values.
Results may differ from the reference program's by a relative error of at most 0.0072.
Values may be sent and summed in bfloat16 or wider, within the bound.
No kernel may reach another device: no remote copies, remote signals or barrier semaphores. Data moves between devices by JAX's collectives and lax.ppermute only.
A program may use at most 128 MiB of HBM per device.

```python
import math
import jax
import jax.numpy as jnp
import numpy as np
from jax import lax

D = 2048
HEADS = 16
HEAD_DIM = 64
GROUPS = 4
NSTATE = 128
INNER = 1024
FE = 1024
TOP = 2
EXPERTS = 64
TOK_DEV = 224
TOKENS = 14336
CAP = 18
N_SP = 64
N_TP = 2


def draw_decay_log(key, part):
    keys = jax.random.split(key, 5)
    fast_share = 0.5
    fast = jax.random.uniform(keys[0], (HEADS,), jnp.float32) < fast_share
    slow_rate = math.log(10.0) / TOKENS * jnp.exp(jax.random.uniform(keys[1], (HEADS,), jnp.float32, math.log(0.15), math.log(0.6)))
    fast_rate = 1.0 / jax.random.uniform(keys[2], (HEADS,), jnp.float32, 30.0, 100.0)
    rate = jnp.where(fast, fast_rate, slow_rate)
    device_factor = jnp.repeat(jnp.exp(jax.random.uniform(keys[3], (TOKENS // TOK_DEV,), jnp.float32, math.log(0.5), math.log(2.0))), TOK_DEV)
    token_factor = jax.random.uniform(keys[4], (HEADS, TOKENS), jnp.float32, 0.7, 1.3)
    return -(rate[:, None] * device_factor[None, :] * token_factor)


def spiked(drawn, key, source, target, shards_of, factor):
    def block_of(dim):
        return (jnp.arange(drawn.shape[dim]) // (drawn.shape[dim] // shards_of)).reshape((-1,) + (1,) * (drawn.ndim - 1 - dim))

    one_side = jax.random.permutation(key, shards_of)[block_of(target)]
    second = (block_of(target) + shards_of // 2) % shards_of
    return jnp.where((block_of(source) == one_side) | (block_of(source) == second), factor * drawn, drawn)


def steps_of(rng, shape, cuts, low, largest):
    loudness = 1.0
    for position, shards_of in cuts:
        steps = jax.random.uniform(jax.random.fold_in(jax.random.fold_in(rng, 6), position), (shards_of,), jnp.float32, low / len(cuts), largest / len(cuts))
        loudness = loudness * jnp.repeat(jnp.exp(steps), shape[position] // shards_of).reshape((-1,) + (1,) * (len(shape) - 1 - position))
    return loudness


def shared_out(stream_key, own, number, rows, amount, top, most, lean):
    sequence = jax.random.permutation(stream_key, amount)
    packed, ordinary = portions_of(amount, rows * top, most, lean, True), portions_of(amount, rows * top, most, lean, False)
    places = jnp.arange(amount)

    def named(lengths, rotation):
        used = int((lengths > 0).sum())
        fixed = max(1, used // 4)
        shifted = fixed + (places - fixed + rotation * (used - fixed)) % max(1, amount - fixed)
        return jnp.zeros((amount,), jnp.int32).at[sequence[jnp.where(places < fixed, places, shifted)]].set(jnp.asarray(lengths, jnp.int32))

    lengths = jnp.where(number % 4 == 0, named(packed, number // 4), named(ordinary, number - number // 4 - 1))
    mixed = jax.random.permutation(jax.random.fold_in(own, 3), amount)
    source_of, sink = mixed[0:amount // 2 * 2:2], mixed[1:amount // 2 * 2:2]
    margin = jnp.minimum(lengths[source_of] - 1, most - lengths[sink]) // 2
    margin = jnp.where((source_of == sequence[0]) | (sink == sequence[0]) | (lengths[sink] == 0), 0, jnp.maximum(margin, 0))
    shifted = jax.random.randint(jax.random.fold_in(own, 4), (amount // 2,), 0, 1 << 20) % (margin + 1)
    lengths = lengths.at[source_of].add(-shifted).at[sink].add(shifted)
    members = jnp.searchsorted(jnp.cumsum(lengths), jnp.arange(rows * top), side="right").astype(jnp.int32)
    table = members.reshape(top, rows).T
    table = table[jax.random.permutation(jax.random.fold_in(own, 1), rows)]
    rotation = jax.random.randint(jax.random.fold_in(own, 2), (rows, 1), 0, top)
    return jnp.take_along_axis(table, (jnp.arange(top)[None, :] + rotation) % top, axis=1)


def portions_of(number_of, total, limit, lean, full):
    loads = [(1 << 20) // math.isqrt(standing ** lean) + 1 for standing in range(1, number_of + 1)]
    largest = limit if full else min(limit, max(-(-total // number_of), total * loads[0] // sum(loads)))
    least = 1 if total - largest >= number_of - 1 else 0
    holding, rest = [largest] + [least] * (number_of - 1), total - largest - least * (number_of - 1)
    while rest > 0:
        movable = [i for i in range(1, number_of) if holding[i] < largest] or [i for i in range(1, number_of) if holding[i] < limit]
        pool, budget = sum([loads[i] for i in movable]), rest
        for i in movable:
            more = min(limit - holding[i], max(1, budget * loads[i] // pool), rest)
            holding[i] = holding[i] + more
            rest = rest - more
    return np.array(holding)


def normal_values(stream_key, shape, scale, most, cuts=(), kind=jnp.bfloat16):
    factor_of = steps_of(stream_key, shape, cuts, -0.22, 0.18) if cuts else 1.0
    values = jax.random.normal(stream_key, shape, jnp.float32) * scale * factor_of
    return jnp.minimum(jnp.maximum(values, -most), most).astype(kind)


def heavy_noise(stream_key, extent, width, most, shards, heavy, kind=jnp.bfloat16):
    values = width * jax.random.normal(stream_key, extent, jnp.float32)
    if shards:
        values = values * steps_of(stream_key, extent, shards, -0.22, 0.18)
    return jnp.clip(spiked(values, jax.random.fold_in(stream_key, 3), *heavy), -most, most).astype(kind)


def setup_inputs(seed: int = 0) -> dict:
    key_list = jax.random.split(jax.random.key(seed), 15)
    out_grad = heavy_noise(key_list[0], (TOKENS, D), 1.0, 16.0, ((0, 64),), (0, 1, 64, 4.0))
    routes_keys = jax.random.split(jax.random.fold_in(key_list[1], 1), TOKENS // TOK_DEV)
    routes_turns = jax.random.permutation(jax.random.fold_in(key_list[1], 3), TOKENS // TOK_DEV)
    routes = jax.vmap(lambda own, number: shared_out(jax.random.fold_in(key_list[1], 2), own, number, TOK_DEV, EXPERTS, TOP, CAP, 1))(routes_keys, routes_turns).reshape((TOKENS, TOP))
    route_weights = jnp.clip(0.5 + 1.5 * jax.random.uniform(key_list[2], (TOKENS, TOP), jnp.float32) ** steps_of(key_list[2], (TOKENS, TOP), ((0, 64),), -0.2, 0.2), 0.5, 2.0)
    routed_rows = normal_values(key_list[3], (EXPERTS, N_SP, CAP, D), 1.0, 6.0, ((0, 64),))
    gate_weight = normal_values(key_list[4], (EXPERTS, D, FE), D ** -0.5, 0.125, ((0, 64), (2, 2)))
    up_weight = normal_values(key_list[5], (EXPERTS, D, FE), D ** -0.5, 0.125, ((0, 64), (2, 2)))
    down_weight = normal_values(key_list[6], (EXPERTS, FE, D), FE ** -0.5, 0.1875, ((0, 64), (1, 2)))
    values = normal_values(key_list[7], (TOKENS, INNER), 0.1, 0.625, ((0, 64), (1, 2)))
    key_side = normal_values(key_list[8], (TOKENS, GROUPS * NSTATE), 0.1, 0.625, ((0, 64), (1, 2)))
    query_side = normal_values(key_list[9], (TOKENS, GROUPS * NSTATE), 0.1, 0.625, ((0, 64), (1, 2)))
    decay_log = draw_decay_log(jax.random.fold_in(key_list[14], 71), 0)
    gate_in = normal_values(key_list[11], (TOKENS, INNER), 1.0, 6.0, ((0, 64), (1, 2)))
    entry_states = normal_values(key_list[12], (N_SP, HEADS, HEAD_DIM, NSTATE), 1.0, 6.0, ((0, 64), (1, 2)), jnp.float32)
    out_weight = normal_values(key_list[13], (D, INNER), INNER ** -0.5, 0.1875, ((1, 2),))
    return {"out_grad": out_grad, "routes": routes, "route_weights": route_weights, "routed_rows": routed_rows, "gate_weight": gate_weight, "up_weight": up_weight, "down_weight": down_weight, "values": values, "key_side": key_side, "query_side": query_side, "decay_log": decay_log, "gate_in": gate_in, "entry_states": entry_states, "out_weight": out_weight}


precise = lax.Precision.HIGHEST

def route_slots(routes_dev, expert_count):
    flat_routes = routes_dev.reshape(-1)
    onehot = (flat_routes[:, None] == jnp.arange(expert_count, dtype=jnp.int32)[None, :]).astype(jnp.int32)
    earlier = jnp.cumsum(onehot, axis=0) - onehot
    return lax.optimization_barrier(jnp.sum(earlier * onehot, axis=1)).astype(jnp.int32)

def block_forward(values, key_side, query_side, decay_log, gate_in, entry_state):
    length = values.shape[0]
    head_count = decay_log.shape[0]
    per_group = HEADS // GROUPS
    group_count = head_count // per_group
    grouped = values.reshape(length, group_count, per_group, HEAD_DIM)
    key_rows = key_side.reshape(length, group_count, NSTATE)
    query_rows = query_side.reshape(length, group_count, NSTATE)
    cumulative = jnp.cumsum(decay_log, axis=1)
    causal = jnp.tril(jnp.ones((length, length), bool))
    spread = cumulative[:, :, None] - cumulative[:, None, :]
    weights = jnp.where(causal, jnp.exp(jnp.where(causal, spread, 0.0)), 0.0)
    weights = weights.reshape(group_count, per_group, length, length)
    scores = jnp.einsum('tgn,sgn->gts', query_rows, key_rows, precision=precise)
    within = jnp.einsum('ghts,sghp->tghp', scores[:, None] * weights, grouped, precision=precise)
    carried = jnp.einsum('tgn,ghpn->tghp', query_rows, entry_state.reshape(group_count, per_group, HEAD_DIM, NSTATE), precision=precise)
    growth = jnp.exp(cumulative).reshape(group_count, per_group, length).transpose(2, 0, 1)
    core_out = (within + carried * growth[..., None]).reshape(length, head_count * HEAD_DIM)
    return core_out * jax.nn.silu(gate_in)

def end_state(values, key_side, decay_log, entry_state):
    length = values.shape[0]
    head_count = decay_log.shape[0]
    per_group = HEADS // GROUPS
    group_count = head_count // per_group
    grouped = values.reshape(length, group_count, per_group, HEAD_DIM)
    key_rows = key_side.reshape(length, group_count, NSTATE)
    cumulative = jnp.cumsum(decay_log, axis=1)
    final_sum = cumulative[:, -1]
    tail_decay = jnp.exp(final_sum[:, None] - cumulative).reshape(group_count, per_group, length)
    fresh_state = jnp.einsum('sgn,ghs,sghp->ghpn', key_rows, tail_decay, grouped, precision=precise)
    return jnp.exp(final_sum)[:, None, None] * entry_state + fresh_state.reshape(head_count, HEAD_DIM, NSTATE)

def reference(out_grad, routes, route_weights, routed_rows, gate_weight, up_weight, down_weight, values, key_side, query_side, decay_log, gate_in, entry_states, out_weight):
    route_count = TOKENS * TOP
    slot_index = jax.vmap(lambda device_routes: route_slots(device_routes, EXPERTS))(routes.reshape(N_SP, TOK_DEV, TOP)).reshape(-1)
    flat_routes = routes.reshape(-1)
    route_ids = jnp.arange(route_count, dtype=jnp.int32)
    source = (route_ids // (TOK_DEV * TOP)).astype(jnp.int32)
    owner_table = jnp.zeros((EXPERTS, N_SP, CAP), jnp.int32).at[flat_routes, source, slot_index].set(route_ids + 1)
    cot_rows = (route_weights[:, :, None] * out_grad.astype(jnp.float32)[:, None, :]).astype(jnp.bfloat16)
    cot_rows = cot_rows.reshape(route_count, D)
    span_width = FE // N_TP

    def expert_step(carried_sum, inputs):
        owner_e, rows_e, gate_e, up_e, down_e = inputs
        filled = (owner_e > 0).reshape(-1)
        picked = jnp.maximum(owner_e.reshape(-1) - 1, 0).astype(jnp.int32)
        cot_block = jnp.where(filled[:, None], cot_rows[picked], jnp.zeros((), jnp.bfloat16))
        row_block = rows_e.reshape(-1, D)
        gate_pre = jnp.dot(row_block, gate_e, preferred_element_type=jnp.float32)
        up_pre = jnp.dot(row_block, up_e, preferred_element_type=jnp.float32)
        act = (jax.nn.silu(gate_pre) * up_pre).astype(jnp.bfloat16)
        act_grad = jnp.dot(cot_block, down_e.T, preferred_element_type=jnp.float32)
        gate_sigmoid = jax.nn.sigmoid(gate_pre)
        gate_grad = (act_grad * up_pre * gate_sigmoid * (1.0 + gate_pre * (1.0 - gate_sigmoid))).astype(jnp.bfloat16)
        up_grad = (act_grad * jax.nn.silu(gate_pre)).astype(jnp.bfloat16)
        grad_down = jnp.dot(act.T, cot_block, preferred_element_type=jnp.float32).astype(jnp.bfloat16)
        grad_gate = jnp.dot(row_block.T, gate_grad, preferred_element_type=jnp.float32).astype(jnp.bfloat16)
        grad_up = jnp.dot(row_block.T, up_grad, preferred_element_type=jnp.float32).astype(jnp.bfloat16)
        back_rows = jnp.zeros((row_block.shape[0], D), jnp.float32)
        for span_index in range(N_TP):
            offset = span_index * span_width
            span_back = jnp.dot(gate_grad[:, offset:offset + span_width], gate_e[:, offset:offset + span_width].T, preferred_element_type=jnp.float32)
            span_back = span_back + jnp.dot(up_grad[:, offset:offset + span_width], up_e[:, offset:offset + span_width].T, preferred_element_type=jnp.float32)
            back_rows = back_rows + lax.optimization_barrier(span_back.astype(jnp.bfloat16)).astype(jnp.float32)
        back_rows = lax.optimization_barrier(back_rows.astype(jnp.bfloat16)).astype(jnp.float32)
        back_rows = jnp.where(filled[:, None], back_rows, 0.0)
        carried_sum = carried_sum.at[picked // TOP].add(back_rows)
        return (carried_sum, (grad_gate, grad_up, grad_down))
    moe_sum, (grad_gate_weight, grad_up_weight, grad_down_weight) = lax.scan(expert_step, jnp.zeros((TOKENS, D), jnp.float32), (owner_table, routed_rows, gate_weight, up_weight, down_weight))
    grad_hidden = (out_grad.astype(jnp.float32) + moe_sum).astype(jnp.bfloat16)
    mix_cot = jnp.dot(grad_hidden, out_weight, preferred_element_type=jnp.float32)

    def joint(value_seg, key_seg, query_seg, decay_seg, gate_seg, entry_state):
        return (block_forward(value_seg, key_seg, query_seg, decay_seg, gate_seg, entry_state), end_state(value_seg, key_seg, decay_seg, entry_state))

    def segment_step(state_cot, inputs):
        value_seg, key_seg, query_seg, decay_seg, gate_seg, entry_state, cot_seg = inputs
        (mixed_out, _), pull_back = jax.vjp(joint, value_seg, key_seg, query_seg, decay_seg, gate_seg, entry_state)
        grads = pull_back((cot_seg, state_cot))
        return (grads[5], (mixed_out, grads[0], grads[1], grads[2], grads[3], grads[4]))
    segment_inputs = (values.astype(jnp.float32).reshape(N_SP, TOK_DEV, INNER), key_side.astype(jnp.float32).reshape(N_SP, TOK_DEV, GROUPS * NSTATE), query_side.astype(jnp.float32).reshape(N_SP, TOK_DEV, GROUPS * NSTATE), decay_log.reshape(HEADS, N_SP, TOK_DEV).transpose(1, 0, 2), gate_in.astype(jnp.float32).reshape(N_SP, TOK_DEV, INNER), entry_states, mix_cot.reshape(N_SP, TOK_DEV, INNER))
    _, (mixed_all, grad_val, grad_key, grad_query, grad_dec, grad_gate_seg) = lax.scan(segment_step, jnp.zeros((HEADS, HEAD_DIM, NSTATE), jnp.float32), segment_inputs, reverse=True)
    mixer_out = mixed_all.reshape(TOKENS, INNER).astype(jnp.bfloat16)
    grad_out_weight = jnp.dot(grad_hidden.T, mixer_out, preferred_element_type=jnp.float32)
    grad_values = grad_val.reshape(TOKENS, INNER).astype(jnp.bfloat16)
    grad_key_side = grad_key.reshape(TOKENS, GROUPS * NSTATE).astype(jnp.bfloat16)
    grad_query_side = grad_query.reshape(TOKENS, GROUPS * NSTATE).astype(jnp.bfloat16)
    grad_decay = grad_dec.transpose(1, 0, 2).reshape(HEADS, TOKENS)
    grad_gate_in = grad_gate_seg.reshape(TOKENS, INNER).astype(jnp.bfloat16)
    return (grad_hidden, grad_gate_weight, grad_up_weight, grad_down_weight, grad_out_weight, grad_values, grad_key_side, grad_query_side, grad_decay, grad_gate_in)
```

```python
import jax
import jax.numpy as jnp
from jax import lax
from jax.experimental import pallas as pl
from jax.experimental.pallas import tpu as pltpu
from jax.sharding import Mesh
from jax.sharding import PartitionSpec as P

BF = jnp.bfloat16
F32 = jnp.float32
SP = ("sp_0", "sp_1", "sp_2")
PEERS = 64
CAP = 18
MAIN = 16
TAIL = CAP - MAIN
TOK = 224
HALF = 1024
COLS = HALF // 128
MSG = COLS * CAP
FH = 512
HEADS = 8
HD = 64
NS = 128
PER_GROUP = 4
GROUPS = 2
VMEM = 60 * 1024 * 1024

NT = (((1,), (1,)), ((), ()))
TN = (((0,), (0,)), ((), ()))
NN = (((1,), (0,)), ((), ()))


def params():
    return pltpu.CompilerParams(vmem_limit_bytes=VMEM)


def cost(flops, nbytes):
    return pl.CostEstimate(flops=flops, bytes_accessed=nbytes, transcendentals=0)


def iota(shape, dim):
    return lax.broadcasted_iota(jnp.int32, shape, dim)


def dot(a, b, dims=NN):
    return lax.dot_general(a, b, dims, preferred_element_type=F32)


def split(a):
    hi = a.astype(BF)
    return hi, (a - hi.astype(F32)).astype(BF)


def dot2(a, b, dims=NN):
    hi, lo = split(a)
    return dot(hi, b, dims) + dot(lo, b, dims)


def dot2r(a, b, dims=NN):
    hi, lo = split(b)
    return dot(a, hi, dims) + dot(a, lo, dims)


def dot3(a, b, dims=NN):
    ah, al = split(a)
    bh, bl = split(b)
    return dot(ah, bh, dims) + (dot(ah, bl, dims) + dot(al, bh, dims))


def dotp(a, b, dims=NN):
    return lax.dot_general(
        a, b, dims, precision=lax.Precision.HIGHEST, preferred_element_type=F32
    )


def tail_rows(shape, row_dim):
    r = iota(shape, row_dim)
    return (r // TAIL) * 16 + (r % TAIL) * 8


def pack_tail(dt):
    place = iota((1024, 128), 0) - tail_rows((1024, 128), 1)
    out = None
    for c in range(COLS):
        mask = jnp.where(place == c, 1.0, 0.0).astype(BF)
        part = dot(mask, dt[:, c * 128 : (c + 1) * 128])
        out = part if out is None else out + part
    return out


def dispatch_kernel(tp_ref, routes_ref, w_ref, og_ref, out_ref, meta_ref):
    del tp_ref
    experts = iota((PEERS, TOK), 0)
    r0, r1 = routes_ref[0:1, :], routes_ref[1:2, :]
    w0, w1 = w_ref[0:1, :], w_ref[1:2, :]
    h0, h1 = experts == r0, experts == r1
    counts = jnp.where(h0, 1.0, 0.0) + jnp.where(h1, 1.0, 0.0)
    before = jnp.where(iota((TOK, TOK), 0) < iota((TOK, TOK), 1), 1.0, 0.0).astype(BF)
    earlier = dot(counts.astype(BF), before)
    f0 = jnp.sum(jnp.where(h0, earlier, 0.0), axis=0, keepdims=True)
    f1 = jnp.sum(jnp.where(h1, earlier, 0.0), axis=0, keepdims=True)
    s0, s1 = f0.astype(jnp.int32), f1.astype(jnp.int32)
    m0 = jnp.where(s0 < MAIN, r0 * MAIN + s0, -1)
    m1 = jnp.where(s1 < MAIN, r1 * MAIN + s1, -1)
    t0 = jnp.where(s0 >= MAIN, r0 * TAIL + s0 - MAIN, -1)
    t1 = jnp.where(s1 >= MAIN, r1 * TAIL + s1 - MAIN, -1)
    og = og_ref[...]

    def rows_of(first, count, a0, a1):
        rows = iota((count, TOK), 0) + first
        q0, q1 = rows == a0, rows == a1
        pick = jnp.where(q0 | q1, 1.0, 0.0).astype(BF)
        scale = jnp.where(q0, w0, jnp.where(q1, w1, 0.0))
        scale = jnp.sum(scale, axis=1, keepdims=True)
        return (dot(pick, og) * scale).astype(BF)

    for b in range(4):
        block = rows_of(256 * b, 256, m0, m1)
        for c in range(COLS):
            out_ref[16 * b : 16 * b + 16, 16 * c : 16 * c + 16, :] = block[
                :, 128 * c : 128 * c + 128
            ].reshape(16, 16, 128)
    tail = pack_tail(rows_of(0, 128, t0, t1)).astype(BF)
    out_ref[:, 16 * COLS : MSG, :] = tail.reshape(PEERS, 16, 128)
    zero = jnp.zeros((4, TOK), F32)
    table = jnp.concatenate([r0.astype(F32), f0, r1.astype(F32), f1, zero], axis=0).astype(BF)
    eye = jnp.where(iota((TOK, TOK), 0) == iota((TOK, TOK), 1), 1.0, 0.0).astype(BF)
    meta_ref[...] = dot(eye, table, NT)


def whole(shape):
    return pl.BlockSpec(shape, lambda i, tp: (0,) * len(shape))


def tp_call(kernel, tp, in_specs, outs, args, flops, nbytes, scratch=(), name=None):
    return pl.pallas_call(
        kernel,
        grid_spec=pltpu.PrefetchScalarGridSpec(
            num_scalar_prefetch=1,
            grid=(1,),
            in_specs=in_specs,
            out_specs=[whole(o.shape) for o in outs],
            scratch_shapes=list(scratch),
        ),
        out_shape=outs,
        compiler_params=params(),
        cost_estimate=cost(flops, nbytes),
        name=name,
    )(tp, *args)


def sds(shape, dtype):
    return jax.ShapeDtypeStruct(shape, dtype)


def dispatch(tp, routes_t, weights_t, out_grad):
    return tp_call(
        dispatch_kernel,
        tp,
        [
            whole((2, TOK)),
            whole((2, TOK)),
            pl.BlockSpec((TOK, HALF), lambda i, tp: (0, tp[0])),
        ],
        [sds((PEERS, MSG, 128), BF), sds((TOK, 8), F32)],
        (routes_t, weights_t, out_grad),
        10**9,
        3 * 10**6,
        name="dispatch",
    )


def combine_kernel(tp_ref, meta_ref, ret_ref, og_ref, out_ref):
    del tp_ref
    meta = meta_ref[...].astype(jnp.int32)
    e0, s0, e1, s1 = (meta[:, k : k + 1] for k in range(4))
    m0 = jnp.where(s0 < MAIN, e0 * MAIN + s0, -1)
    m1 = jnp.where(s1 < MAIN, e1 * MAIN + s1, -1)
    t0 = jnp.where(s0 >= MAIN, e0 * 16 + (s0 - MAIN) * 8, -100)
    t1 = jnp.where(s1 >= MAIN, e1 * 16 + (s1 - MAIN) * 8, -100)
    lanes = iota((TOK, 1024), 1)
    pick = jnp.where((lanes == m0) | (lanes == m1), 1.0, 0.0).astype(BF)
    tail = ret_ref[:, 16 * COLS : MSG, :].reshape(1024, 128)
    d0, d1 = lanes - t0, lanes - t1
    for c in range(COLS):
        main = ret_ref[:, 16 * c : 16 * c + 16, :].reshape(1024, 128)
        tpick = jnp.where((d0 == c) | (d1 == c), 1.0, 0.0).astype(BF)
        moe = dot(pick, main) + dot(tpick, tail)
        cols = slice(128 * c, 128 * c + 128)
        out_ref[:, cols] = (og_ref[:, cols].astype(F32) + moe).astype(BF)


def combine_rows(tp, meta, returned, out_grad):
    return tp_call(
        combine_kernel,
        tp,
        [
            whole((TOK, 8)),
            whole((PEERS, MSG, 128)),
            pl.BlockSpec((TOK, HALF), lambda i, tp: (0, tp[0])),
        ],
        [sds((TOK, HALF), BF)],
        (meta, returned, out_grad),
        10**9,
        3 * 10**6,
        name="combine",
    )[0]


def hidden_kernel(tp_ref, mine_ref, other_ref, down_ref, a1_ref, a2_ref, arr_ref, gg_ref, ug_ref):
    first = tp_ref[0] == 0

    def place(b, carry):
        peers = pl.ds(pl.multiple_of(b * 8, 8), 8)
        rows = pl.ds(pl.multiple_of(b * 128, 128), 128)
        for c in range(COLS):
            x = mine_ref[peers, 16 * c : 16 * c + 16, :].reshape(128, 128)
            y = other_ref[peers, 16 * c : 16 * c + 16, :].reshape(128, 128)
            arr_ref[rows, 128 * c : 128 * c + 128] = jnp.where(first, x, y)
            arr_ref[rows, HALF + 128 * c : HALF + 128 * c + 128] = jnp.where(first, y, x)
        return carry

    lax.fori_loop(0, 8, place, 0)
    x = mine_ref[:, 16 * COLS : MSG, :].reshape(1024, 128)
    y = other_ref[:, 16 * COLS : MSG, :].reshape(1024, 128)
    both = jnp.concatenate([jnp.where(first, x, y), jnp.where(first, y, x)], axis=1)
    at = iota((128, 1024), 1) - tail_rows((128, 1024), 0)
    for c in range(COLS):
        mask = jnp.where(at == c, 1.0, 0.0).astype(BF)
        got = dot(mask, both).astype(BF)
        arr_ref[1024:1152, 128 * c : 128 * c + 128] = got[:, :128]
        arr_ref[1024:1152, HALF + 128 * c : HALF + 128 * c + 128] = got[:, 128:]

    def grads(b, carry):
        rows = pl.ds(pl.multiple_of(b * 384, 384), 384)
        act_grad = dot(arr_ref[rows, :], down_ref[...], NT)
        gg_ref[rows, :] = (act_grad * a1_ref[rows, :]).astype(BF)
        ug_ref[rows, :] = (act_grad * a2_ref[rows, :]).astype(BF)
        return carry

    lax.fori_loop(0, 3, grads, 0)


def hidden_grads(tp, mine, other, down, a1, a2):
    return tp_call(
        hidden_kernel,
        tp,
        [
            whole((PEERS, MSG, 128)),
            whole((PEERS, MSG, 128)),
            whole((FH, 2 * HALF)),
            whole((PEERS * CAP, FH)),
            whole((PEERS * CAP, FH)),
        ],
        [
            sds((PEERS * CAP, 2 * HALF), BF),
            sds((PEERS * CAP, FH), BF),
            sds((PEERS * CAP, FH), BF),
        ],
        (mine, other, down, a1, a2),
        4 * 10**9,
        2 * 10**7,
        name="hidden_grads",
    )


def span_kernel(half_ref, gg_ref, ug_ref, gw_ref, uw_ref, out_ref, tail_ref):
    del half_ref

    for n in range(4):
        gw = gw_ref[256 * n : 256 * n + 256, :]
        uw = uw_ref[256 * n : 256 * n + 256, :]

        def rows_step(b, carry, gw=gw, uw=uw, n=n):
            rows = pl.ds(pl.multiple_of(b * 256, 256), 256)
            peers = pl.ds(pl.multiple_of(b * 16, 16), 16)
            d = (dot(gg_ref[rows, :], gw, NT) + dot(ug_ref[rows, :], uw, NT)).astype(BF)
            for k in range(2):
                c = 2 * n + k
                out_ref[peers, 16 * c : 16 * c + 16, :] = d[:, 128 * k : 128 * k + 128].reshape(
                    16, 16, 128
                )
            return carry

        lax.fori_loop(0, 4, rows_step, 0)
        d = dot(gg_ref[1024:1152, :], gw, NT) + dot(ug_ref[1024:1152, :], uw, NT)
        tail_ref[:, 256 * n : 256 * n + 256] = d.astype(BF)
    tail = pack_tail(tail_ref[...]).astype(BF)
    out_ref[:, 16 * COLS : MSG, :] = tail.reshape(PEERS, 16, 128)


def span_half(half, gg, ug, gw, uw):
    weights = pl.BlockSpec((HALF, FH), lambda i, h: (h[0], 0))
    return tp_call(
        span_kernel,
        half,
        [whole((PEERS * CAP, FH)), whole((PEERS * CAP, FH)), weights, weights],
        [sds((PEERS, MSG, 128), BF)],
        (gg, ug, gw, uw),
        4 * 10**9,
        10**7,
        scratch=[pltpu.VMEM((128, HALF), BF)],
        name="span_half",
    )[0]


def decay_sums(decay):
    upto = jnp.where(iota((TOK, TOK), 0) <= iota((TOK, TOK), 1), 1.0, 0.0)
    down = jnp.where(iota((TOK, TOK), 0) >= iota((TOK, TOK), 1), 1.0, 0.0)
    return dotp(decay, upto), dotp(down, decay, NT)


def decay_weights(cum, cum_t, h):
    causal = iota((TOK, TOK), 0) >= iota((TOK, TOK), 1)
    spread = cum_t[:, h : h + 1] - cum[h : h + 1, :]
    return jnp.where(causal, jnp.exp(jnp.where(causal, spread, 0.0)), 0.0)


def head(h):
    return slice(HD * h, HD * h + HD)


def group(g):
    return slice(NS * g, NS * g + NS)


def forward_kernel(v_ref, k_ref, q_ref, decay_ref, gate_ref, e_ref, core_ref, mixed_ref):
    cum, cum_t = decay_sums(decay_ref[...])
    for g in range(GROUPS):
        q, k = q_ref[:, group(g)], k_ref[:, group(g)]
        scores = dot(q, k, NT)
        for h in range(PER_GROUP * g, PER_GROUP * g + PER_GROUP):
            m = scores * decay_weights(cum, cum_t, h)
            within = dot2(m, v_ref[:, head(h)])
            carried = dot2r(q, e_ref[h], NT)
            core = within + carried * jnp.exp(cum_t[:, h : h + 1])
            core_ref[:, head(h)] = core
            gate = gate_ref[:, head(h)].astype(F32)
            mixed_ref[:, head(h)] = (core * (gate * jax.nn.sigmoid(gate))).astype(BF)


def plain_call(kernel, outs, args, flops, nbytes, scratch=(), name=None):
    return pl.pallas_call(
        kernel,
        out_shape=outs,
        scratch_shapes=list(scratch),
        compiler_params=params(),
        cost_estimate=cost(flops, nbytes),
        name=name,
    )(*args)


def cotangent_kernel(
    tp_ref, mine_ref, other_ref, ow_ref, core_ref, gate_ref, decay_ref, q_ref,
    hidden_ref, dcore_ref, dgate_ref, g_ref,
):
    first = tp_ref[0] == 0
    x, y = mine_ref[...], other_ref[...]
    lo, hi = jnp.where(first, x, y), jnp.where(first, y, x)
    hidden_ref[:, :HALF] = lo
    hidden_ref[:, HALF:] = hi
    cot = dot(lo, ow_ref[:HALF, :]) + dot(hi, ow_ref[HALF:, :])
    gate = gate_ref[...].astype(F32)
    sig = jax.nn.sigmoid(gate)
    dcore = cot * (gate * sig)
    dcore_ref[...] = dcore
    dgate_ref[...] = (cot * core_ref[...] * (sig * (1.0 + gate * (1.0 - sig)))).astype(BF)
    _, cum_t = decay_sums(decay_ref[...])
    growth = jnp.exp(cum_t)
    for h in range(HEADS):
        q = q_ref[:, group(h // PER_GROUP)]
        g_ref[h] = dot2(dcore[:, head(h)] * growth[:, h : h + 1], q, TN)


def backward_kernel(
    v_ref, k_ref, q_ref, decay_ref, e_ref, dcore_ref, dv_ref, dk_ref, dq_ref
):
    cum, cum_t = decay_sums(decay_ref[...])
    for g in range(GROUPS):
        q, k = q_ref[:, group(g)], k_ref[:, group(g)]
        scores = dot(q, k, NT)
        ds = jnp.zeros((TOK, TOK), F32)
        dq = jnp.zeros((TOK, NS), F32)
        for h in range(PER_GROUP * g, PER_GROUP * g + PER_GROUP):
            w = decay_weights(cum, cum_t, h)
            dcore = dcore_ref[:, head(h)]
            dv_ref[:, head(h)] = dot3(scores * w, dcore, TN)
            ds = ds + dot2(dcore, v_ref[:, head(h)], NT) * w
            dq = dq + dot3(dcore * jnp.exp(cum_t[:, h : h + 1]), e_ref[h])
        dq_ref[:, group(g)] = (dq + dot2(ds, k)).astype(BF)
        dk_ref[:, group(g)] = dot2(ds, q, TN)


def ending_kernel(
    x_ref, s0_ref, s1_ref, s2_ref, s3_ref, v_ref, k_ref, decay_ref, e_ref, core_ref, dcore_ref,
    dv_ref, dk_ref, gv_ref, gk_ref, gd_ref, state_ref,
):
    mine = x_ref[0]
    for d, ref in enumerate((s0_ref, s1_ref, s2_ref, s3_ref)):
        rows = pl.ds(pl.multiple_of(((mine - d + 4) % 4) * 16, 16), 16)
        state_ref[:, rows, :] = ref[...]
    cum, cum_t = decay_sums(decay_ref[...])
    last = cum_t[TOK - 1 : TOK, :]
    tail = jnp.exp(last - cum_t)
    fresh = []
    kept = []
    diff = []
    for g in range(GROUPS):
        k = k_ref[:, group(g)]
        dk = dk_ref[:, group(g)]
        for h in range(PER_GROUP * g, PER_GROUP * g + PER_GROUP):
            state = state_ref[h]
            v = v_ref[:, head(h)].astype(F32)
            t = tail[:, h : h + 1]
            dv2 = t * dot2r(k, state, NT)
            dk = dk + dot3(v * t, state)
            dv = dv_ref[:, head(h)] + dv2
            gv_ref[:, head(h)] = dv.astype(BF)
            diff.append(
                jnp.sum(dcore_ref[:, head(h)] * core_ref[:, head(h)] - v * dv, axis=1, keepdims=True)
            )
            fresh.append(jnp.sum(v * dv2).reshape(1, 1))
            kept.append(jnp.sum(e_ref[h] * state).reshape(1, 1))
        gk_ref[:, group(g)] = dk.astype(BF)
    diff = jnp.concatenate(diff, axis=1)
    at_end = jnp.concatenate(fresh, axis=1) + jnp.exp(last) * jnp.concatenate(kept, axis=1)
    diff = diff + jnp.where(iota((TOK, HEADS), 0) == TOK - 1, at_end, 0.0)
    later = jnp.where(iota((TOK, TOK), 0) >= iota((TOK, TOK), 1), 1.0, 0.0)
    gd_ref[...] = dotp(diff, later, TN)


def shift(x, axis, d):
    return lax.ppermute(x, axis, [(i, (i + d) % 4) for i in range(4)])


def gathered(x, axis):
    return [x] + [shift(x, axis, d) for d in range(1, 4)]


def masked_exp(logs, mask):
    return jnp.exp(jnp.sum(jnp.where(mask[..., None], logs, 0.0), axis=-2))


def chain_factors(decay_log):
    steps = jnp.arange(4)
    pos = [lax.axis_index(a) for a in SP]
    at = [(p - steps) % 4 for p in pos]
    to = (pos[2] + steps) % 4
    logs = jnp.sum(decay_log, axis=1)
    x_logs = jnp.stack(gathered(logs, SP[2]))
    y_logs = jnp.stack(gathered(jnp.sum(x_logs, axis=0), SP[1]))
    z_logs = jnp.stack(gathered(jnp.sum(y_logs, axis=0), SP[0]))
    ax, ay, az = (a for a in (at[2], at[1], at[0]))

    def before(a):
        return a[None, :] < a[:, None]

    row_total = masked_exp(x_logs, before(ax))
    inside = masked_exp(x_logs, (to[:, None, None] < ax) & before(ax))
    inside = jnp.where((ax > to[:, None])[..., None], inside, 0.0)
    through = masked_exp(x_logs, ax > to[:, None])
    plane_total = masked_exp(y_logs, before(ay))
    rows_after = jnp.where(
        (ay > pos[1])[:, None], masked_exp(y_logs, (ay > pos[1]) & before(ay)), 0.0
    )
    past_rows = masked_exp(y_logs, ay > pos[1])
    planes_after = jnp.where(
        (az > pos[0])[:, None], masked_exp(z_logs, (az > pos[0]) & before(az)), 0.0
    )
    return row_total, inside, through, plane_total, rows_after, past_rows, planes_after


def weighted(factors, parts):
    out = factors[0][:, None, None] * parts[0]
    for f, p in zip(factors[1:], parts[1:]):
        out = out + f[:, None, None] * p
    return out


def chain(own, factors):
    row_total, inside, through, plane_total, rows_after, past_rows, planes_after = factors
    x = lax.axis_index(SP[2])

    def cut(d):
        return lax.dynamic_slice_in_dim(own, ((x + d) % 4) * 16, 16, 1)

    parts = [cut(0)] + [shift(cut(d), SP[2], d) for d in range(1, 4)]
    rows = gathered(weighted(row_total, parts), SP[1])
    planes = gathered(weighted(plane_total, rows), SP[0])
    entering = weighted(rows_after, rows) + past_rows[:, None, None] * weighted(
        planes_after, planes
    )
    back = []
    for d in range(4):
        piece = weighted(inside[d], parts) + through[d][:, None, None] * entering
        back.append(piece if d == 0 else shift(piece, SP[2], d))
    return back


def per_device(
    out_grad,
    routes,
    route_weights,
    routed_rows,
    gate_weight,
    up_weight,
    down_weight,
    values,
    key_side,
    query_side,
    decay_log,
    gate_in,
    entry_states,
    out_weight,
):
    tp_index = lax.axis_index("tp").astype(jnp.int32)
    tp = tp_index.reshape(1)
    peer = (1 - tp_index).reshape(1)
    gate_w, up_w, down_w = gate_weight[0], up_weight[0], down_weight[0]
    entry = entry_states[0]

    def swap(x):
        return lax.ppermute(x, "tp", [(0, 1), (1, 0)])

    message, meta = dispatch(tp, routes.T, route_weights.T, out_grad)
    moved = lax.all_to_all(message, SP, split_axis=0, concat_axis=0, tiled=True)

    rows = routed_rows[0]
    rows = jnp.concatenate(
        [rows[:, :MAIN].reshape(PEERS * MAIN, -1), rows[:, MAIN:].reshape(PEERS * TAIL, -1)], axis=0
    )
    gate_pre = jnp.dot(rows, gate_w, preferred_element_type=F32)
    up_pre = jnp.dot(rows, up_w, preferred_element_type=F32)
    sig = jax.nn.sigmoid(gate_pre)
    silu = gate_pre * sig
    act = (silu * up_pre).astype(BF)
    a1 = up_pre * sig * (1.0 + gate_pre * (1.0 - sig))
    core, mixer_out = plain_call(
        forward_kernel,
        [sds((TOK, HEADS * HD), F32), sds((TOK, HEADS * HD), BF)],
        (values, key_side, query_side, decay_log, gate_in, entry),
        10**9,
        10**6,
        name="mixer_forward",
    )
    later_decay, core = lax.optimization_barrier((decay_log, core))
    factors = chain_factors(later_decay)
    moved, rows, act, a1, silu, core, mixer_out, factors = lax.optimization_barrier(
        (moved, rows, act, a1, silu, core, mixer_out, factors)
    )

    arrived, gate_grad, up_grad = hidden_grads(tp, moved, swap(moved), down_w, a1, silu)
    for_peer = swap(span_half(peer, gate_grad, up_grad, gate_w, up_w))
    own_span = span_half(tp, gate_grad, up_grad, gate_w, up_w)
    back = (own_span.astype(F32) + for_peer.astype(F32)).astype(BF)
    returned = lax.all_to_all(back, SP, split_axis=0, concat_axis=0, tiled=True)

    grad_down = dot(act, arrived, TN).astype(BF)
    grad_gate = dot(rows, gate_grad, TN).astype(BF)
    grad_up = dot(rows, up_grad, TN).astype(BF)
    returned, grad_down, grad_gate, grad_up = lax.optimization_barrier(
        (returned, grad_down, grad_gate, grad_up)
    )

    hidden_half = combine_rows(tp, meta, returned, out_grad)
    grad_hidden, dcore, dgate, own_state = tp_call(
        cotangent_kernel,
        tp,
        [
            whole((TOK, HALF)),
            whole((TOK, HALF)),
            whole((2 * HALF, FH)),
            whole((TOK, FH)),
            whole((TOK, FH)),
            whole((HEADS, TOK)),
            whole((TOK, GROUPS * NS)),
        ],
        [
            sds((TOK, 2 * HALF), BF),
            sds((TOK, FH), F32),
            sds((TOK, FH), BF),
            sds((HEADS, HD, NS), F32),
        ],
        (hidden_half, swap(hidden_half), out_weight, core, gate_in, decay_log, query_side),
        10**9,
        5 * 10**6,
        name="mixer_cotangent",
    )
    states = chain(own_state, factors)
    shares = dot(grad_hidden, mixer_out, TN).astype(BF).reshape(PEERS, 32, FH)
    shares = lax.all_to_all(shares, SP, split_axis=0, concat_axis=0, tiled=True)
    grad_out_weight = jnp.sum(shares.astype(F32), axis=0)
    dv, dk, grad_query = plain_call(
        backward_kernel,
        [
            sds((TOK, HEADS * HD), F32),
            sds((TOK, GROUPS * NS), F32),
            sds((TOK, GROUPS * NS), BF),
        ],
        (values, key_side, query_side, decay_log, entry, dcore),
        2 * 10**9,
        10**6,
        name="mixer_backward",
    )
    x_index = lax.axis_index(SP[2]).astype(jnp.int32).reshape(1)
    vmem = pl.BlockSpec(memory_space=pltpu.VMEM)
    grad_values, grad_key, grad_decay = pl.pallas_call(
        ending_kernel,
        out_shape=[
            sds((TOK, HEADS * HD), BF),
            sds((TOK, GROUPS * NS), BF),
            sds((HEADS, TOK), F32),
        ],
        in_specs=[pl.BlockSpec(memory_space=pltpu.SMEM)] + [vmem] * 12,
        scratch_shapes=[pltpu.VMEM((HEADS, HD, NS), F32)],
        compiler_params=params(),
        cost_estimate=cost(10**9, 10**6),
        name="mixer_ending",
    )(x_index, *states, values, key_side, decay_log, entry, core, dcore, dv, dk)
    return (
        grad_hidden,
        grad_gate[None],
        grad_up[None],
        grad_down[None],
        grad_out_weight,
        grad_values,
        grad_key,
        grad_query,
        grad_decay,
        dgate,
    )


def solution(mesh):
    grid = Mesh(mesh.devices.reshape(4, 4, 4, mesh.shape["tp"]), ("sp_0", "sp_1", "sp_2", "tp"))
    placed = (
        P(SP, None),
        P(SP, None),
        P(SP, None),
        P(SP, None, None, None),
        P(SP, None, "tp"),
        P(SP, None, "tp"),
        P(SP, "tp", None),
        P(SP, "tp"),
        P(SP, "tp"),
        P(SP, "tp"),
        P("tp", SP),
        P(SP, "tp"),
        P(SP, "tp", None, None),
        P(None, "tp"),
    )
    return jax.shard_map(
        per_device,
        mesh=grid,
        in_specs=placed,
        out_specs=(
            P(SP, None),
            P(SP, None, "tp"),
            P(SP, None, "tp"),
            P(SP, "tp", None),
            P(SP, "tp"),
            P(SP, "tp"),
            P(SP, "tp"),
            P(SP, "tp"),
            P("tp", SP),
            P(SP, "tp"),
        ),
        check_vma=False,
    )
```

```python
import functools

import jax
import jax.numpy as jnp
from jax import lax
from jax.experimental import pallas as pl
from jax.experimental.pallas import tpu as pltpu
from jax.sharding import Mesh
from jax.sharding import PartitionSpec as P

BF = jnp.bfloat16
F32 = jnp.float32
SP = ("sp_0", "sp_1", "sp_2")
PEERS = 64
CAP = 18
MAIN = 16
TAIL = CAP - MAIN
TOK = 224
HALF = 1024
COLS = HALF // 128
MSG = COLS * CAP
FH = 512
HEADS = 8
HD = 64
NS = 128
PER_GROUP = 4
GROUPS = 2

NT = (((1,), (1,)), ((), ()))
TN = (((0,), (0,)), ((), ()))
NN = (((1,), (0,)), ((), ()))


def cost(flops, nbytes):
    return pl.CostEstimate(flops=flops, bytes_accessed=nbytes, transcendentals=0)


def iota(shape, dim):
    return lax.broadcasted_iota(jnp.int32, shape, dim)


def dot(a, b, dims=NN):
    return lax.dot_general(a, b, dims, preferred_element_type=F32)


def split(a):
    hi = a.astype(BF)
    return hi, (a - hi.astype(F32)).astype(BF)


def dot2(a, b, dims=NN):
    hi, lo = split(a)
    return dot(hi, b, dims) + dot(lo, b, dims)


def dot2r(a, b, dims=NN):
    hi, lo = split(b)
    return dot(a, hi, dims) + dot(a, lo, dims)


def dot3(a, b, dims=NN):
    ah, al = split(a)
    bh, bl = split(b)
    return dot(ah, bh, dims) + (dot(ah, bl, dims) + dot(al, bh, dims))


def dotp(a, b, dims=NN):
    return lax.dot_general(
        a, b, dims, precision=lax.Precision.HIGHEST, preferred_element_type=F32
    )


def tail_rows(shape, row_dim):
    r = iota(shape, row_dim)
    return (r // TAIL) * 16 + (r % TAIL) * 8


def pack_tail(dt):
    place = iota((1024, 128), 0) - tail_rows((1024, 128), 1)
    out = None
    for c in range(COLS):
        mask = jnp.where(place == c, 1.0, 0.0).astype(BF)
        part = dot(mask, dt[:, c * 128 : (c + 1) * 128])
        out = part if out is None else out + part
    return out


def copy_out(from_ref, to_ref, sems, b):
    peers = slice(16 * b, 16 * b + 16)
    copy = pltpu.make_async_copy(from_ref.at[peers], to_ref.at[peers], sems.at[b])
    copy.start()
    return copy


def load(pairs, sems):
    copies = [
        pltpu.make_async_copy(far, near, sems.at[i]) for i, (far, near) in enumerate(pairs)
    ]
    for copy in copies:
        copy.start()
    for copy in copies:
        copy.wait()


def slots(routes):
    experts = iota((PEERS, TOK), 0)
    r0, r1 = routes[0:1, :], routes[1:2, :]
    h0, h1 = experts == r0, experts == r1
    counts = jnp.where(h0, 1.0, 0.0) + jnp.where(h1, 1.0, 0.0)
    before = jnp.where(iota((TOK, TOK), 0) < iota((TOK, TOK), 1), 1.0, 0.0).astype(BF)
    earlier = dot(counts.astype(BF), before)
    f0 = jnp.sum(jnp.where(h0, earlier, 0.0), axis=0, keepdims=True)
    f1 = jnp.sum(jnp.where(h1, earlier, 0.0), axis=0, keepdims=True)
    return r0, r1, f0, f1


def dispatch_kernel(
    tp_ref, far_routes, far_w, far_og, to_ref, routes_ref, w_ref, og_ref, out_ref, sems, in_sems
):
    own = half_of(tp_ref)
    load(((far_routes, routes_ref), (far_w, w_ref), (far_og.at[:, own], og_ref)), in_sems)
    r0, r1, f0, f1 = slots(routes_ref[...])
    w0, w1 = w_ref[0:1, :], w_ref[1:2, :]
    s0, s1 = f0.astype(jnp.int32), f1.astype(jnp.int32)
    m0 = jnp.where(s0 < MAIN, r0 * MAIN + s0, -1)
    m1 = jnp.where(s1 < MAIN, r1 * MAIN + s1, -1)
    t0 = jnp.where(s0 >= MAIN, r0 * TAIL + s0 - MAIN, -1)
    t1 = jnp.where(s1 >= MAIN, r1 * TAIL + s1 - MAIN, -1)
    og = og_ref[...]

    def rows_of(first, count, a0, a1):
        rows = iota((count, TOK), 0) + first
        q0, q1 = rows == a0, rows == a1
        pick = jnp.where(q0 | q1, 1.0, 0.0).astype(BF)
        scale = jnp.where(q0, w0, jnp.where(q1, w1, 0.0))
        scale = jnp.sum(scale, axis=1, keepdims=True)
        return (dot(pick, og) * scale).astype(BF)

    tail = pack_tail(rows_of(0, 128, t0, t1)).astype(BF)
    out_ref[:, 16 * COLS : MSG, :] = tail.reshape(PEERS, 16, 128)
    copies = []
    for b in range(4):
        block = rows_of(256 * b, 256, m0, m1)
        for c in range(COLS):
            out_ref[16 * b : 16 * b + 16, 16 * c : 16 * c + 16, :] = block[
                :, 128 * c : 128 * c + 128
            ].reshape(16, 16, 128)
        copies.append(copy_out(out_ref, to_ref, sems, b))
    for copy in copies:
        copy.wait()


def call(
    kernel,
    outs,
    args,
    flops,
    nbytes,
    scalar=None,
    scratch=(),
    name=None,
    limit=8,
    hbm_outs=(),
    hbm_ins=(),
):
    vmem = pl.BlockSpec(memory_space=pltpu.VMEM)
    far = pl.BlockSpec(memory_space=pltpu.HBM)
    in_specs = [far if i in hbm_ins else vmem for i in range(len(args))]
    if scalar is not None:
        in_specs = [pl.BlockSpec(memory_space=pltpu.SMEM)] + in_specs
        args = (scalar, *args)
    return pl.pallas_call(
        kernel,
        out_shape=outs,
        in_specs=in_specs,
        out_specs=[far if i in hbm_outs else vmem for i in range(len(outs))],
        scratch_shapes=list(scratch),
        compiler_params=pltpu.CompilerParams(vmem_limit_bytes=limit * 1024 * 1024),
        cost_estimate=cost(flops, nbytes),
        name=name,
    )(*args)


def sds(shape, dtype):
    return jax.ShapeDtypeStruct(shape, dtype)


def dispatch(tp, routes_t, weights_t, out_grad):
    dma = pltpu.SemaphoreType.DMA
    return call(
        dispatch_kernel,
        [sds((PEERS, MSG, 128), BF)],
        (routes_t, weights_t, out_grad),
        10**9,
        3 * 10**6,
        scalar=tp,
        scratch=[
            pltpu.VMEM((2, TOK), jnp.int32),
            pltpu.VMEM((2, TOK), F32),
            pltpu.VMEM((TOK, HALF), BF),
            pltpu.VMEM((PEERS, MSG, 128), BF),
            dma((4,)),
            dma((3,)),
        ],
        hbm_ins=(0, 1, 2),
        hbm_outs=(0,),
        limit=60,
        name="dispatch",
    )[0]


def half_of(tp_ref, other=False):
    half = 1 - tp_ref[0] if other else tp_ref[0]
    return pl.ds(pl.multiple_of(half * HALF, HALF), HALF)


def combine_kernel(tp_ref, meta_ref, ret_ref, og_ref, out_ref):
    own = og_ref[:, half_of(tp_ref)].astype(F32)
    meta = meta_ref[...].astype(jnp.int32)
    e0, s0, e1, s1 = (meta[:, k : k + 1] for k in range(4))
    m0 = jnp.where(s0 < MAIN, e0 * MAIN + s0, -1)
    m1 = jnp.where(s1 < MAIN, e1 * MAIN + s1, -1)
    t0 = jnp.where(s0 >= MAIN, e0 * 16 + (s0 - MAIN) * 8, -100)
    t1 = jnp.where(s1 >= MAIN, e1 * 16 + (s1 - MAIN) * 8, -100)
    lanes = iota((TOK, 1024), 1)
    pick = jnp.where((lanes == m0) | (lanes == m1), 1.0, 0.0).astype(BF)
    tail = ret_ref[:, 16 * COLS : MSG, :].reshape(1024, 128)
    d0, d1 = lanes - t0, lanes - t1
    for c in range(COLS):
        main = ret_ref[:, 16 * c : 16 * c + 16, :].reshape(1024, 128)
        tpick = jnp.where((d0 == c) | (d1 == c), 1.0, 0.0).astype(BF)
        moe = dot(pick, main) + dot(tpick, tail)
        cols = slice(128 * c, 128 * c + 128)
        out_ref[:, cols] = (own[:, cols] + moe).astype(BF)


def combine_rows(tp, meta, returned, out_grad):
    return call(
        combine_kernel,
        [sds((TOK, HALF), BF)],
        (meta, returned, out_grad),
        10**9,
        3 * 10**6,
        scalar=tp,
        name="combine",
    )[0]


def place_rows(msg_ref, arr_ref):
    for c in range(COLS):
        main = msg_ref[:, 16 * c : 16 * c + 16, :].reshape(1024, 128)
        arr_ref[0:1024, 128 * c : 128 * c + 128] = main
    tail = msg_ref[:, 16 * COLS : MSG, :].reshape(1024, 128)
    at = iota((128, 1024), 1) - tail_rows((128, 1024), 0)
    for c in range(COLS):
        mask = jnp.where(at == c, 1.0, 0.0).astype(BF)
        arr_ref[1024:1152, 128 * c : 128 * c + 128] = dot(mask, tail).astype(BF)


def first_half_kernel(tp_ref, mine_ref, down_ref, arr_ref, part_ref):
    place_rows(mine_ref, arr_ref)
    part_ref[...] = dot(arr_ref[...], down_ref[:, half_of(tp_ref)], NT)


def second_half_kernel(
    tp_ref, other_ref, down_ref, part_ref, a1_ref, a2_ref, arr_ref, gg_ref, ug_ref
):
    place_rows(other_ref, arr_ref)
    act_grad = part_ref[...] + dot(arr_ref[...], down_ref[:, half_of(tp_ref, True)], NT)
    gg_ref[...] = (act_grad * a1_ref[...]).astype(BF)
    ug_ref[...] = (act_grad * a2_ref[...]).astype(BF)


def hidden_grads(tp, mine, other, down, a1, a2):
    rows = PEERS * CAP
    own_cols, part = call(
        first_half_kernel,
        [sds((rows, HALF), BF), sds((rows, FH), F32)],
        (mine, down),
        2 * 10**9,
        10**7,
        scalar=tp,
        name="hidden_first",
    )
    other_cols, gg, ug = call(
        second_half_kernel,
        [sds((rows, HALF), BF), sds((rows, FH), BF), sds((rows, FH), BF)],
        (other, down, part, a1, a2),
        2 * 10**9,
        10**7,
        scalar=tp,
        name="hidden_second",
    )
    return (own_cols, other_cols), gg, ug


def down_kernel(tp_ref, act_ref, own_ref, other_ref, out_ref):
    for n in range(4):
        cols = slice(256 * n, 256 * n + 256)
        for other, ref in ((False, own_ref), (True, other_ref)):
            half = 1 - tp_ref[0] if other else tp_ref[0]
            to = pl.ds(pl.multiple_of(half * HALF + 256 * n, 256), 256)
            out_ref[:, to] = dot(act_ref[...], ref[:, cols], TN).astype(BF)


def down_grad(tp, act, arrived):
    return call(
        down_kernel,
        [sds((FH, 2 * HALF), BF)],
        (act, *arrived),
        2 * 10**9,
        10**7,
        scalar=tp,
        name="down_grad",
    )[0]


def span_kernel(other, half_ref, gg_ref, ug_ref, gw_ref, uw_ref, out_ref, tail_ref):
    base = (1 - half_ref[0] if other else half_ref[0]) * HALF
    for n in range(4):
        cols = pl.ds(pl.multiple_of(base + 256 * n, 256), 256)
        d = dot(gg_ref[...], gw_ref[cols, :], NT) + dot(ug_ref[...], uw_ref[cols, :], NT)
        d = d.astype(BF)
        for k in range(2):
            c = 2 * n + k
            part = d[:, 128 * k : 128 * k + 128]
            out_ref[:, 16 * c : 16 * c + 16, :] = part[:1024].reshape(PEERS, 16, 128)
            tail_ref[:, 128 * c : 128 * c + 128] = part[1024:]
    tail = pack_tail(tail_ref[...]).astype(BF)
    out_ref[:, 16 * COLS : MSG, :] = tail.reshape(PEERS, 16, 128)


def span_half(tp, other, gg, ug, gw, uw):
    return call(
        functools.partial(span_kernel, other),
        [sds((PEERS, MSG, 128), BF)],
        (gg, ug, gw, uw),
        4 * 10**9,
        10**7,
        scalar=tp,
        scratch=[pltpu.VMEM((128, HALF), BF)],
        name="span_half",
    )[0]


def decay_sums(decay):
    upto = jnp.where(iota((TOK, TOK), 0) <= iota((TOK, TOK), 1), 1.0, 0.0)
    down = jnp.where(iota((TOK, TOK), 0) >= iota((TOK, TOK), 1), 1.0, 0.0)
    return dotp(decay, upto), dotp(down, decay, NT)


def decay_weights(cum, cum_t, h):
    causal = iota((TOK, TOK), 0) >= iota((TOK, TOK), 1)
    spread = cum_t[:, h : h + 1] - cum[h : h + 1, :]
    return jnp.where(causal, jnp.exp(jnp.where(causal, spread, 0.0)), 0.0)


def head(h):
    return slice(HD * h, HD * h + HD)


def group(g):
    return slice(NS * g, NS * g + NS)


def forward_kernel(
    v_ref, k_ref, q_ref, decay_ref, gate_ref, e_ref, routes_ref, core_ref, mixed_ref, meta_ref
):
    r0, r1, f0, f1 = slots(routes_ref[...])
    zero = jnp.zeros((4, TOK), F32)
    table = jnp.concatenate([r0.astype(F32), f0, r1.astype(F32), f1, zero], axis=0).astype(BF)
    eye = jnp.where(iota((TOK, TOK), 0) == iota((TOK, TOK), 1), 1.0, 0.0).astype(BF)
    meta_ref[...] = dot(eye, table, NT)
    cum, cum_t = decay_sums(decay_ref[...])
    for g in range(GROUPS):
        q, k = q_ref[:, group(g)], k_ref[:, group(g)]
        scores = dot(q, k, NT)
        for h in range(PER_GROUP * g, PER_GROUP * g + PER_GROUP):
            m = scores * decay_weights(cum, cum_t, h)
            within = dot2(m, v_ref[:, head(h)])
            carried = dot2r(q, e_ref[h], NT)
            core = within + carried * jnp.exp(cum_t[:, h : h + 1])
            core_ref[:, head(h)] = core
            gate = gate_ref[:, head(h)].astype(F32)
            mixed_ref[:, head(h)] = (core * (gate * jax.nn.sigmoid(gate))).astype(BF)


def low_part(a, hi):
    return a - hi.astype(F32)


def cotangent_kernel(
    tp_ref, mine_ref, other_ref, ow_ref, core_ref, gate_ref, decay_ref, q_ref, mixed_ref,
    hidden_ref, dcore_ref, dgate_ref, to_ref, msg_ref, sems,
):
    first = tp_ref[0] == 0
    x, y = mine_ref[...], other_ref[...]
    lo, hi = jnp.where(first, x, y), jnp.where(first, y, x)
    hidden_ref[:, :HALF] = lo
    hidden_ref[:, HALF:] = hi
    cot = dot(lo, ow_ref[:HALF, :]) + dot(hi, ow_ref[HALF:, :])
    gate = gate_ref[...].astype(F32)
    sig = jax.nn.sigmoid(gate)
    dcore = cot * (gate * sig)
    dcore_ref[...] = dcore
    dgate_ref[...] = (cot * core_ref[...] * (sig * (1.0 + gate * (1.0 - sig)))).astype(BF)
    _, cum_t = decay_sums(decay_ref[...])
    growth = jnp.exp(cum_t)
    logs = jnp.sum(decay_ref[...], axis=1, keepdims=True)
    high, low = split(logs)
    mid, _ = split(low_part(logs, high))
    rest = low_part(logs, high) - mid.astype(F32)
    row = iota((8, 8, 128), 1)
    states = []
    for g in range(GROUPS):
        heads = range(PER_GROUP * g, PER_GROUP * g + PER_GROUP)
        grown = [dcore[:, head(h)] * growth[:, h : h + 1] for h in heads]
        states.append(dot2(jnp.concatenate(grown, axis=1), q_ref[:, group(g)], TN))
    for h in range(HEADS):
        at = HD * (h % PER_GROUP)
        state = states[h // PER_GROUP][at : at + HD]
        parts = [
            jnp.broadcast_to(p[h : h + 1, :], (8, 128)).reshape(1, 8, 128)
            for p in (high.astype(F32), mid.astype(F32), rest)
        ]
        extra = jnp.where(row == 0, parts[0], jnp.where(row == 1, parts[1], parts[2]))
        extra = jnp.where(row < 3, extra, 0.0)
        both = jnp.concatenate([state.reshape(8, 8, 128), extra], axis=1)
        msg_ref[8 * h : 8 * h + 8, 128:144, :] = both.astype(BF)
    copies = []
    for b in range(4):
        rows = hidden_ref[:, 512 * b : 512 * b + 512]
        share = dot(rows, mixed_ref[...], TN).astype(BF)
        for c in range(4):
            msg_ref[16 * b : 16 * b + 16, 32 * c : 32 * c + 32, :] = share[
                :, 128 * c : 128 * c + 128
            ].reshape(16, 32, 128)
        copies.append(copy_out(msg_ref, to_ref, sems, b))
    for copy in copies:
        copy.wait()


def backward_kernel(
    v_ref, k_ref, q_ref, decay_ref, e_ref, core_ref, dcore_ref, dv_ref, dk_ref, dq_ref, diff_ref
):
    cum, cum_t = decay_sums(decay_ref[...])
    for g in range(GROUPS):
        q, k = q_ref[:, group(g)], k_ref[:, group(g)]
        scores = dot(q, k, NT)
        ds = jnp.zeros((TOK, TOK), F32)
        dq = jnp.zeros((TOK, NS), F32)
        for h in range(PER_GROUP * g, PER_GROUP * g + PER_GROUP):
            w = decay_weights(cum, cum_t, h)
            dcore = dcore_ref[:, head(h)]
            dv = dot3(scores * w, dcore, TN)
            dv_ref[:, head(h)] = dv
            v = v_ref[:, head(h)].astype(F32)
            diff_ref[:, h : h + 1] = jnp.sum(
                dcore * core_ref[:, head(h)] - v * dv, axis=1, keepdims=True
            )
            ds = ds + dot2(dcore, v_ref[:, head(h)], NT) * w
            dq = dq + dot3(dcore * jnp.exp(cum_t[:, h : h + 1]), e_ref[h])
        dq_ref[:, group(g)] = (dq + dot2(ds, k)).astype(BF)
        dk_ref[:, group(g)] = dot2(ds, q, TN)


def ending_kernel(
    state_far, v_far, k_far, decay_far, e_far, dv_far, dk_far, diff_far,
    gv_ref, gk_ref, gd_ref, state_ref, v_ref, k_ref, decay_ref, e_ref, dv_ref, dk_ref, diff_ref, sems,
):
    load(
        (
            (state_far, state_ref),
            (decay_far, decay_ref),
            (v_far, v_ref),
            (k_far, k_ref),
            (e_far, e_ref),
            (dv_far, dv_ref),
            (dk_far, dk_ref),
            (diff_far, diff_ref),
        ),
        sems,
    )
    cum, cum_t = decay_sums(decay_ref[...])
    last = cum_t[TOK - 1 : TOK, :]
    tail = jnp.exp(last - cum_t)
    fresh = []
    kept = []
    diff = []
    for g in range(GROUPS):
        k = k_ref[:, group(g)]
        dk = dk_ref[:, group(g)]
        for h in range(PER_GROUP * g, PER_GROUP * g + PER_GROUP):
            state = state_ref[8 * h : 8 * h + 8].astype(F32).reshape(HD, NS)
            exact = state.astype(BF)
            v = v_ref[:, head(h)].astype(F32)
            t = tail[:, h : h + 1]
            dv2 = t * dot(k, exact, NT)
            dk = dk + dot2(v * t, exact)
            dv = dv_ref[:, head(h)] + dv2
            gv_ref[:, head(h)] = dv.astype(BF)
            moved = jnp.sum(v * dv2, axis=1, keepdims=True)
            diff.append(moved)
            fresh.append(jnp.sum(moved).reshape(1, 1))
            kept.append(jnp.sum(e_ref[h] * state).reshape(1, 1))
        gk_ref[:, group(g)] = dk.astype(BF)
    diff = diff_ref[...] - jnp.concatenate(diff, axis=1)
    at_end = jnp.concatenate(fresh, axis=1) + jnp.exp(last) * jnp.concatenate(kept, axis=1)
    diff = diff + jnp.where(iota((TOK, HEADS), 0) == TOK - 1, at_end, 0.0)
    later = jnp.where(iota((TOK, TOK), 0) >= iota((TOK, TOK), 1), 1.0, 0.0)
    gd_ref[...] = dotp(diff, later, TN)


def chain_kernel(in_ref, out_ref):
    wide = in_ref[:, 128:144, :].astype(F32)
    states = wide[:, 0:8, :].reshape(512, 128).astype(BF)
    logs = jnp.sum(wide[:, 8:16, :], axis=1)
    segment, entry = iota((512, PEERS), 0) // 8, iota((512, PEERS), 1)
    before = dotp(jnp.where(entry < segment, 1.0, 0.0), logs)
    through = dotp(jnp.where(entry <= segment, 1.0, 0.0), logs)
    i, j = iota((512, 512), 0), iota((512, 512), 1)
    later = (j // 8 > i // 8) & (j % 8 == i % 8)
    spread = jnp.transpose(before)[0:1, :] - through[:, 0:1]
    weights = jnp.where(later, jnp.exp(jnp.where(later, spread, 0.0)), 0.0)
    out_ref[...] = dot2(weights, states).reshape(PEERS, 8, 128).astype(BF)


def share_kernel(in_ref, out_ref):
    for c in range(4):
        total = in_ref[0, 32 * c : 32 * c + 32, :].astype(F32)
        for peer in range(1, PEERS):
            total = total + in_ref[peer, 32 * c : 32 * c + 32, :].astype(F32)
        out_ref[:, 128 * c : 128 * c + 128] = total


def per_device(
    out_grad,
    routes,
    route_weights,
    routed_rows,
    gate_weight,
    up_weight,
    down_weight,
    values,
    key_side,
    query_side,
    decay_log,
    gate_in,
    entry_states,
    out_weight,
):
    tp_index = lax.axis_index("tp").astype(jnp.int32)
    tp = tp_index.reshape(1)
    gate_w, up_w, down_w = gate_weight[0], up_weight[0], down_weight[0]
    entry = entry_states[0]

    def swap(x):
        return lax.ppermute(x, "tp", [(0, 1), (1, 0)])

    message = dispatch(tp, routes.T, route_weights.T, out_grad)
    moved = lax.all_to_all(message, SP, split_axis=0, concat_axis=0, tiled=True)

    rows = routed_rows[0]
    rows = jnp.concatenate(
        [rows[:, :MAIN].reshape(PEERS * MAIN, -1), rows[:, MAIN:].reshape(PEERS * TAIL, -1)], axis=0
    )
    gate_pre = jnp.dot(rows, gate_w, preferred_element_type=F32)
    up_pre = jnp.dot(rows, up_w, preferred_element_type=F32)
    sig = jax.nn.sigmoid(gate_pre)
    silu = gate_pre * sig
    act = (silu * up_pre).astype(BF)
    a1 = up_pre * sig * (1.0 + gate_pre * (1.0 - sig))
    _, later_values = lax.optimization_barrier((message, values))
    core, mixer_out, meta = call(
        forward_kernel,
        [sds((TOK, HEADS * HD), F32), sds((TOK, HEADS * HD), BF), sds((TOK, 8), F32)],
        (later_values, key_side, query_side, decay_log, gate_in, entry, routes.T),
        10**9,
        10**6,
        name="mixer_forward",
    )
    moved, rows, act, a1, silu, core, mixer_out, meta = lax.optimization_barrier(
        (moved, rows, act, a1, silu, core, mixer_out, meta)
    )

    arrived, gate_grad, up_grad = hidden_grads(tp, moved, swap(moved), down_w, a1, silu)
    for_peer = swap(span_half(tp, True, gate_grad, up_grad, gate_w, up_w))
    own_span = span_half(tp, False, gate_grad, up_grad, gate_w, up_w)
    back = (own_span.astype(F32) + for_peer.astype(F32)).astype(BF)
    returned = lax.all_to_all(back, SP, split_axis=0, concat_axis=0, tiled=True)

    _, gate_grad, up_grad, act = lax.optimization_barrier((back, gate_grad, up_grad, act))
    grad_down = down_grad(tp, act, arrived)
    grad_gate = dot(rows, gate_grad, TN).astype(BF)
    grad_up = dot(rows, up_grad, TN).astype(BF)
    returned, grad_down, grad_gate, grad_up = lax.optimization_barrier(
        (returned, grad_down, grad_gate, grad_up)
    )

    hidden_half = combine_rows(tp, meta, returned, out_grad)
    grad_hidden, dcore, dgate, tail_message = call(
        cotangent_kernel,
        [
            sds((TOK, 2 * HALF), BF),
            sds((TOK, FH), F32),
            sds((TOK, FH), BF),
            sds((PEERS, 144, NS), BF),
        ],
        (
            hidden_half,
            swap(hidden_half),
            out_weight,
            core,
            gate_in,
            decay_log,
            query_side,
            mixer_out,
        ),
        10**9,
        5 * 10**6,
        scalar=tp,
        scratch=[pltpu.VMEM((PEERS, 144, NS), BF), pltpu.SemaphoreType.DMA((4,))],
        hbm_outs=(3,),
        name="mixer_cotangent",
    )
    gathered = lax.all_to_all(tail_message, SP, split_axis=0, concat_axis=0, tiled=True)
    dv, dk, grad_query, diff = call(
        backward_kernel,
        [
            sds((TOK, HEADS * HD), F32),
            sds((TOK, GROUPS * NS), F32),
            sds((TOK, GROUPS * NS), BF),
            sds((TOK, HEADS), F32),
        ],
        (values, key_side, query_side, decay_log, entry, core, dcore),
        2 * 10**9,
        10**6,
        name="mixer_backward",
    )
    gathered, dv, dk, grad_query, diff = lax.optimization_barrier(
        (gathered, dv, dk, grad_query, diff)
    )
    states = call(
        chain_kernel,
        [sds((PEERS, 8, NS), BF)],
        (gathered,),
        10**8,
        10**6,
        name="state_chain",
    )[0]
    states = lax.all_to_all(states, SP, split_axis=0, concat_axis=0, tiled=True)
    grad_out_weight = call(
        share_kernel,
        [sds((32, FH), F32)],
        (gathered,),
        10**7,
        10**6,
        name="share_sum",
    )[0]
    grad_values, grad_key, grad_decay = call(
        ending_kernel,
        [
            sds((TOK, HEADS * HD), BF),
            sds((TOK, GROUPS * NS), BF),
            sds((HEADS, TOK), F32),
        ],
        (states, values, key_side, decay_log, entry, dv, dk, diff),
        10**9,
        10**6,
        scratch=[
            pltpu.VMEM((PEERS, 8, NS), BF),
            pltpu.VMEM((TOK, HEADS * HD), BF),
            pltpu.VMEM((TOK, GROUPS * NS), BF),
            pltpu.VMEM((HEADS, TOK), F32),
            pltpu.VMEM((HEADS, HD, NS), F32),
            pltpu.VMEM((TOK, HEADS * HD), F32),
            pltpu.VMEM((TOK, GROUPS * NS), F32),
            pltpu.VMEM((TOK, HEADS), F32),
            pltpu.SemaphoreType.DMA((8,)),
        ],
        hbm_ins=tuple(range(8)),
        limit=60,
        name="mixer_ending",
    )
    return (
        grad_hidden,
        grad_gate[None],
        grad_up[None],
        grad_down[None],
        grad_out_weight,
        grad_values,
        grad_key,
        grad_query,
        grad_decay,
        dgate,
    )


def solution(mesh):
    grid = Mesh(mesh.devices.reshape(4, 4, 4, mesh.shape["tp"]), ("sp_0", "sp_1", "sp_2", "tp"))
    placed = (
        P(SP, None),
        P(SP, None),
        P(SP, None),
        P(SP, None, None, None),
        P(SP, None, "tp"),
        P(SP, None, "tp"),
        P(SP, "tp", None),
        P(SP, "tp"),
        P(SP, "tp"),
        P(SP, "tp"),
        P("tp", SP),
        P(SP, "tp"),
        P(SP, "tp", None, None),
        P(None, "tp"),
    )
    return jax.shard_map(
        per_device,
        mesh=grid,
        in_specs=placed,
        out_specs=(
            P(SP, None),
            P(SP, None, "tp"),
            P(SP, None, "tp"),
            P(SP, "tp", None),
            P(SP, "tp"),
            P(SP, "tp"),
            P(SP, "tp"),
            P(SP, "tp"),
            P("tp", SP),
            P(SP, "tp"),
        ),
        check_vma=False,
    )
```

```python
import functools

import jax
import jax.numpy as jnp
from jax import lax
from jax.experimental import pallas as pl
from jax.experimental.pallas import tpu as pltpu
from jax.sharding import Mesh
from jax.sharding import PartitionSpec as P

BF = jnp.bfloat16
F32 = jnp.float32
SP = ("sp_0", "sp_1", "sp_2")
PEERS = 64
CAP = 18
MAIN = 16
TAIL = CAP - MAIN
TOK = 224
HALF = 1024
COLS = HALF // 128
MSG = COLS * CAP
FH = 512
HEADS = 8
HD = 64
NS = 128
PER_GROUP = 4
GROUPS = 2

NT = (((1,), (1,)), ((), ()))
TN = (((0,), (0,)), ((), ()))
NN = (((1,), (0,)), ((), ()))


def cost(flops, nbytes):
    return pl.CostEstimate(flops=flops, bytes_accessed=nbytes, transcendentals=0)


def iota(shape, dim):
    return lax.broadcasted_iota(jnp.int32, shape, dim)


def dot(a, b, dims=NN):
    return lax.dot_general(a, b, dims, preferred_element_type=F32)


def split(a):
    hi = a.astype(BF)
    return hi, (a - hi.astype(F32)).astype(BF)


def dot2(a, b, dims=NN):
    hi, lo = split(a)
    return dot(hi, b, dims) + dot(lo, b, dims)


def dot2r(a, b, dims=NN):
    hi, lo = split(b)
    return dot(a, hi, dims) + dot(a, lo, dims)


def dot3(a, b, dims=NN):
    ah, al = split(a)
    bh, bl = split(b)
    return dot(ah, bh, dims) + (dot(ah, bl, dims) + dot(al, bh, dims))


def dotp(a, b, dims=NN):
    return lax.dot_general(
        a, b, dims, precision=lax.Precision.HIGHEST, preferred_element_type=F32
    )


def tail_rows(shape, row_dim):
    r = iota(shape, row_dim)
    return (r // TAIL) * 16 + (r % TAIL) * 8


def pack_tail(dt):
    place = iota((1024, 128), 0) - tail_rows((1024, 128), 1)
    out = None
    for c in range(COLS):
        mask = jnp.where(place == c, 1.0, 0.0).astype(BF)
        part = dot(mask, dt[:, c * 128 : (c + 1) * 128])
        out = part if out is None else out + part
    return out


def copy_out(from_ref, to_ref, sems, b):
    peers = slice(16 * b, 16 * b + 16)
    copy = pltpu.make_async_copy(from_ref.at[peers], to_ref.at[peers], sems.at[b])
    copy.start()
    return copy


def load(pairs, sems):
    copies = [
        pltpu.make_async_copy(far, near, sems.at[i]) for i, (far, near) in enumerate(pairs)
    ]
    for copy in copies:
        copy.start()
    for copy in copies:
        copy.wait()


def slots(routes):
    experts = iota((PEERS, TOK), 0)
    r0, r1 = routes[0:1, :], routes[1:2, :]
    h0, h1 = experts == r0, experts == r1
    counts = jnp.where(h0, 1.0, 0.0) + jnp.where(h1, 1.0, 0.0)
    before = jnp.where(iota((TOK, TOK), 0) < iota((TOK, TOK), 1), 1.0, 0.0).astype(BF)
    earlier = dot(counts.astype(BF), before)
    f0 = jnp.sum(jnp.where(h0, earlier, 0.0), axis=0, keepdims=True)
    f1 = jnp.sum(jnp.where(h1, earlier, 0.0), axis=0, keepdims=True)
    return r0, r1, f0, f1


def dispatch_kernel(
    tp_ref, far_routes, far_w, far_og, to_ref, routes_ref, w_ref, og_ref, out_ref, sems, in_sems
):
    own = half_of(tp_ref)
    load(((far_routes, routes_ref), (far_w, w_ref), (far_og.at[:, own], og_ref)), in_sems)
    r0, r1, f0, f1 = slots(routes_ref[...])
    w0, w1 = w_ref[0:1, :], w_ref[1:2, :]
    s0, s1 = f0.astype(jnp.int32), f1.astype(jnp.int32)
    m0 = jnp.where(s0 < MAIN, r0 * MAIN + s0, -1)
    m1 = jnp.where(s1 < MAIN, r1 * MAIN + s1, -1)
    t0 = jnp.where(s0 >= MAIN, r0 * TAIL + s0 - MAIN, -1)
    t1 = jnp.where(s1 >= MAIN, r1 * TAIL + s1 - MAIN, -1)
    og = og_ref[...]

    def rows_of(first, count, a0, a1):
        rows = iota((count, TOK), 0) + first
        q0, q1 = rows == a0, rows == a1
        pick = jnp.where(q0 | q1, 1.0, 0.0).astype(BF)
        scale = jnp.where(q0, w0, jnp.where(q1, w1, 0.0))
        scale = jnp.sum(scale, axis=1, keepdims=True)
        return (dot(pick, og) * scale).astype(BF)

    tail = pack_tail(rows_of(0, 128, t0, t1)).astype(BF)
    out_ref[:, 16 * COLS : MSG, :] = tail.reshape(PEERS, 16, 128)
    copies = []
    for b in range(4):
        block = rows_of(256 * b, 256, m0, m1)
        for c in range(COLS):
            out_ref[16 * b : 16 * b + 16, 16 * c : 16 * c + 16, :] = block[
                :, 128 * c : 128 * c + 128
            ].reshape(16, 16, 128)
        copies.append(copy_out(out_ref, to_ref, sems, b))
    for copy in copies:
        copy.wait()


def call(
    kernel,
    outs,
    args,
    flops,
    nbytes,
    scalar=None,
    scratch=(),
    name=None,
    limit=8,
    hbm_outs=(),
    hbm_ins=(),
    aliases=None,
):
    vmem = pl.BlockSpec(memory_space=pltpu.VMEM)
    far = pl.BlockSpec(memory_space=pltpu.HBM)
    in_specs = [far if i in hbm_ins else vmem for i in range(len(args))]
    if scalar is not None:
        in_specs = [pl.BlockSpec(memory_space=pltpu.SMEM)] + in_specs
        args = (scalar, *args)
    return pl.pallas_call(
        kernel,
        out_shape=outs,
        in_specs=in_specs,
        out_specs=[far if i in hbm_outs else vmem for i in range(len(outs))],
        scratch_shapes=list(scratch),
        input_output_aliases=aliases or {},
        compiler_params=pltpu.CompilerParams(vmem_limit_bytes=limit * 1024 * 1024),
        cost_estimate=cost(flops, nbytes),
        name=name,
    )(*args)


def sds(shape, dtype):
    return jax.ShapeDtypeStruct(shape, dtype)


def dispatch(tp, routes_t, weights_t, out_grad):
    dma = pltpu.SemaphoreType.DMA
    return call(
        dispatch_kernel,
        [sds((PEERS, MSG, 128), BF)],
        (routes_t, weights_t, out_grad),
        10**9,
        3 * 10**6,
        scalar=tp,
        scratch=[
            pltpu.VMEM((2, TOK), jnp.int32),
            pltpu.VMEM((2, TOK), F32),
            pltpu.VMEM((TOK, HALF), BF),
            pltpu.VMEM((PEERS, MSG, 128), BF),
            dma((4,)),
            dma((3,)),
        ],
        hbm_ins=(0, 1, 2),
        hbm_outs=(0,),
        limit=60,
        name="dispatch",
    )[0]


def half_of(tp_ref, other=False):
    half = 1 - tp_ref[0] if other else tp_ref[0]
    return pl.ds(pl.multiple_of(half * HALF, HALF), HALF)


def combine_kernel(tp_ref, meta_ref, ret_ref, og_ref, out_ref):
    meta = meta_ref[...].astype(jnp.int32)
    e0, s0, e1, s1 = (meta[:, k : k + 1] for k in range(4))
    m0 = jnp.where(s0 < MAIN, e0 * MAIN + s0, -1)
    m1 = jnp.where(s1 < MAIN, e1 * MAIN + s1, -1)
    t0 = jnp.where(s0 >= MAIN, e0 * 16 + (s0 - MAIN) * 8, -100)
    t1 = jnp.where(s1 >= MAIN, e1 * 16 + (s1 - MAIN) * 8, -100)
    lanes = iota((TOK, 1024), 1)
    pick = jnp.where((lanes == m0) | (lanes == m1), 1.0, 0.0).astype(BF)
    tail = ret_ref[:, 16 * COLS : MSG, :].reshape(1024, 128)
    d0, d1 = lanes - t0, lanes - t1

    for c in range(0, COLS, 2):
        pair = [ret_ref[:, 16 * k : 16 * k + 16, :].reshape(1024, 128) for k in (c, c + 1)]
        moe = dot(pick, jnp.concatenate(pair, axis=1))
        masks = [jnp.where((d0 == k) | (d1 == k), 1.0, 0.0).astype(BF) for k in (c, c + 1)]
        moe = moe + jnp.concatenate([dot(m, tail) for m in masks], axis=1)
        own = og_ref[:, pl.ds(pl.multiple_of(tp_ref[0] * HALF + c * 128, 256), 256)]
        out_ref[:, 128 * c : 128 * c + 256] = (own.astype(F32) + moe).astype(BF)


def combine_rows(tp, meta, returned, out_grad):
    return call(
        combine_kernel,
        [sds((TOK, HALF), BF)],
        (meta, returned, out_grad),
        10**9,
        3 * 10**6,
        scalar=tp,
        name="combine",
    )[0]


def place_rows(msg_ref, arr_ref):
    for c in range(COLS):
        main = msg_ref[:, 16 * c : 16 * c + 16, :].reshape(1024, 128)
        arr_ref[0:1024, 128 * c : 128 * c + 128] = main
    tail = msg_ref[:, 16 * COLS : MSG, :].reshape(1024, 128)
    at = iota((128, 1024), 1) - tail_rows((128, 1024), 0)
    for c in range(COLS):
        mask = jnp.where(at == c, 1.0, 0.0).astype(BF)
        arr_ref[1024:1152, 128 * c : 128 * c + 128] = dot(mask, tail).astype(BF)


def order_kernel(in_ref, out_ref):
    i, j = iota((256, 256), 0), iota((256, 256), 1)
    turn = jnp.where((i // 16 == j % 16) & (i % 16 == j // 16), 1.0, 0.0).astype(BF)
    for b in range(4):
        x = in_ref[0:MAIN, 16 * b : 16 * b + 16, :].reshape(256, -1)
        out_ref[256 * b : 256 * b + 256, :] = dot(turn, x).astype(BF)
    i, j = iota((128, 128), 0), iota((128, 128), 1)
    turn = jnp.where((i // 2 == j % 64) & (i % 2 == j // 64), 1.0, 0.0).astype(BF)
    x = in_ref[MAIN:CAP, :, :].reshape(128, -1)
    out_ref[1024:1152, :] = dot(turn, x).astype(BF)


def ordered_rows(rows):
    width = rows.shape[-1]
    return call(
        order_kernel,
        [sds((PEERS * CAP, width), BF)],
        (jnp.transpose(rows, (1, 0, 2)),),
        10**9,
        10**7,
        limit=16,
        name="ordered_rows",
    )[0]


def first_half_kernel(tp_ref, mine_ref, down_ref, arr_ref, part_ref):
    place_rows(mine_ref, arr_ref)
    part_ref[...] = dot(arr_ref[...], down_ref[:, half_of(tp_ref)], NT)


def second_half_kernel(
    tp_ref, other_ref, down_ref, part_ref, a1_ref, a2_ref, arr_ref, gg_ref, ug_ref
):
    place_rows(other_ref, arr_ref)
    act_grad = part_ref[...] + dot(arr_ref[...], down_ref[:, half_of(tp_ref, True)], NT)
    gg_ref[...] = (act_grad * a1_ref[...]).astype(BF)
    ug_ref[...] = (act_grad * a2_ref[...]).astype(BF)


def hidden_grads(tp, mine, other, down, a1, a2):
    rows = PEERS * CAP
    own_cols, part = call(
        first_half_kernel,
        [sds((rows, HALF), BF), sds((rows, FH), F32)],
        (mine, down),
        2 * 10**9,
        10**7,
        scalar=tp,
        name="hidden_first",
    )
    other_cols, gg, ug = call(
        second_half_kernel,
        [sds((rows, HALF), BF), sds((rows, FH), BF), sds((rows, FH), BF)],
        (other, down, part, a1, a2),
        2 * 10**9,
        10**7,
        scalar=tp,
        name="hidden_second",
    )
    return (own_cols, other_cols), gg, ug


def down_kernel(tp_ref, act_ref, own_ref, other_ref, out_ref):
    def step(n, carry):
        cols = pl.ds(pl.multiple_of(256 * n, 256), 256)
        for other, ref in ((False, own_ref), (True, other_ref)):
            half = 1 - tp_ref[0] if other else tp_ref[0]
            to = pl.ds(pl.multiple_of(half * HALF + 256 * n, 256), 256)
            out_ref[:, to] = dot(act_ref[...], ref[:, cols], TN).astype(BF)
        return carry

    lax.fori_loop(0, 4, step, 0)


def down_grad(tp, act, arrived):
    return call(
        down_kernel,
        [sds((FH, 2 * HALF), BF)],
        (act, *arrived),
        2 * 10**9,
        10**7,
        scalar=tp,
        name="down_grad",
    )[0]


def span_kernel(other, half_ref, gg_ref, ug_ref, gw_ref, uw_ref, out_ref, tail_ref):
    base = (1 - half_ref[0] if other else half_ref[0]) * HALF

    def block(n):
        cols = pl.ds(pl.multiple_of(base + 256 * n, 256), 256)
        d = dot(gg_ref[...], gw_ref[cols, :], NT) + dot(ug_ref[...], uw_ref[cols, :], NT)
        d = d.astype(BF)
        for k in range(2):
            c = 2 * n + k
            part = d[:, 128 * k : 128 * k + 128]
            rows = pl.ds(pl.multiple_of(16 * c, 16), 16)
            out_ref[:, rows, :] = part[:1024].reshape(PEERS, 16, 128)
            tail_ref[:, pl.ds(pl.multiple_of(128 * c, 128), 128)] = part[1024:]

    def step(n, carry):
        block(2 * n)
        block(2 * n + 1)
        return carry

    lax.fori_loop(0, 2, step, 0)
    tail = pack_tail(tail_ref[...]).astype(BF)
    out_ref[:, 16 * COLS : MSG, :] = tail.reshape(PEERS, 16, 128)


def span_half(tp, other, gg, ug, gw, uw):
    return call(
        functools.partial(span_kernel, other),
        [sds((PEERS, MSG, 128), BF)],
        (gg, ug, gw, uw),
        4 * 10**9,
        10**7,
        scalar=tp,
        scratch=[pltpu.VMEM((128, HALF), BF)],
        name="span_half",
    )[0]


def decay_sums(decay):
    upto = jnp.where(iota((TOK, TOK), 0) <= iota((TOK, TOK), 1), 1.0, 0.0)
    down = jnp.where(iota((TOK, TOK), 0) >= iota((TOK, TOK), 1), 1.0, 0.0)
    return dotp(decay, upto), dotp(down, decay, NT)


def decay_weights(cum, cum_t, h):
    causal = iota((TOK, TOK), 0) >= iota((TOK, TOK), 1)
    spread = cum_t[:, h : h + 1] - cum[h : h + 1, :]
    return jnp.where(causal, jnp.exp(jnp.where(causal, spread, 0.0)), 0.0)


def head(h):
    return slice(HD * h, HD * h + HD)


def group(g):
    return slice(NS * g, NS * g + NS)


def forward_kernel(
    v_ref, k_ref, q_ref, decay_ref, gate_ref, e_ref, routes_ref, core_ref, mixed_ref, meta_ref
):
    r0, r1, f0, f1 = slots(routes_ref[...])
    zero = jnp.zeros((4, TOK), F32)
    table = jnp.concatenate([r0.astype(F32), f0, r1.astype(F32), f1, zero], axis=0).astype(BF)
    eye = jnp.where(iota((TOK, TOK), 0) == iota((TOK, TOK), 1), 1.0, 0.0).astype(BF)
    meta_ref[...] = dot(eye, table, NT)
    cum, cum_t = decay_sums(decay_ref[...])
    for g in range(GROUPS):
        q, k = q_ref[:, group(g)], k_ref[:, group(g)]
        scores = dot(q, k, NT)
        for h in range(PER_GROUP * g, PER_GROUP * g + PER_GROUP):
            m = scores * decay_weights(cum, cum_t, h)
            within = dot2(m, v_ref[:, head(h)])
            carried = dot2r(q, e_ref[h], NT)
            core = within + carried * jnp.exp(cum_t[:, h : h + 1])
            core_ref[:, head(h)] = core
            gate = gate_ref[:, head(h)].astype(F32)
            mixed_ref[:, head(h)] = (core * (gate * jax.nn.sigmoid(gate))).astype(BF)


def low_part(a, hi):
    return a - hi.astype(F32)


def cotangent_kernel(
    tp_ref, mine_ref, other_ref, ow_ref, core_ref, gate_ref, decay_ref, q_ref,
    hidden_ref, dcore_ref, dgate_ref, msg_ref,
):
    first = tp_ref[0] == 0
    x, y = mine_ref[...], other_ref[...]
    lo, hi = jnp.where(first, x, y), jnp.where(first, y, x)
    hidden_ref[:, :HALF] = lo
    hidden_ref[:, HALF:] = hi
    cot = dot(lo, ow_ref[:HALF, :]) + dot(hi, ow_ref[HALF:, :])
    gate = gate_ref[...].astype(F32)
    sig = jax.nn.sigmoid(gate)
    dcore = cot * (gate * sig)
    dcore_ref[...] = dcore
    dgate_ref[...] = (cot * core_ref[...] * (sig * (1.0 + gate * (1.0 - sig)))).astype(BF)
    _, cum_t = decay_sums(decay_ref[...])
    growth = jnp.exp(cum_t)
    logs = jnp.sum(decay_ref[...], axis=1, keepdims=True)
    high, low = split(logs)
    mid, _ = split(low_part(logs, high))
    rest = low_part(logs, high) - mid.astype(F32)
    row = iota((8, 8, 128), 1)
    states = []
    for g in range(GROUPS):
        heads = range(PER_GROUP * g, PER_GROUP * g + PER_GROUP)
        grown = [dcore[:, head(h)] * growth[:, h : h + 1] for h in heads]
        states.append(dot2(jnp.concatenate(grown, axis=1), q_ref[:, group(g)], TN))
    for h in range(HEADS):
        at = HD * (h % PER_GROUP)
        state = states[h // PER_GROUP][at : at + HD]
        parts = [
            jnp.broadcast_to(p[h : h + 1, :], (8, 128)).reshape(1, 8, 128)
            for p in (high.astype(F32), mid.astype(F32), rest)
        ]
        extra = jnp.where(row == 0, parts[0], jnp.where(row == 1, parts[1], parts[2]))
        extra = jnp.where(row < 3, extra, 0.0)
        both = jnp.concatenate([state.reshape(8, 8, 128), extra], axis=1)
        msg_ref[8 * h : 8 * h + 8] = both.astype(BF)


def shares_kernel(hidden_ref, mixed_ref, msg_ref):
    def step(b, carry):
        rows = hidden_ref[:, pl.ds(pl.multiple_of(512 * b, 512), 512)]
        share = dot(rows, mixed_ref[...], TN).astype(BF)
        peers = pl.ds(pl.multiple_of(16 * b, 16), 16)
        for c in range(4):
            msg_ref[peers, 32 * c : 32 * c + 32, :] = share[:, 128 * c : 128 * c + 128].reshape(
                16, 32, 128
            )
        return carry

    lax.fori_loop(0, 4, step, 0)
    msg_ref[:, 128:136, :] = jnp.zeros((PEERS, 8, 128), BF)


def backward_kernel(
    v_far, k_far, q_far, decay_far, e_far, core_far, dcore_far,
    dv_far, dk_far, dq_far, diff_far,
    v_ref, k_ref, q_ref, decay_ref, e_ref, core_ref, dcore_ref,
    dv_ref, dk_ref, dq_ref, diff_ref, sems,
):
    load(
        (
            (decay_far, decay_ref),
            (q_far, q_ref),
            (k_far, k_ref),
            (v_far, v_ref),
            (e_far, e_ref),
            (dcore_far, dcore_ref),
            (core_far, core_ref),
        ),
        sems,
    )
    cum, cum_t = decay_sums(decay_ref[...])
    causal = iota((TOK, TOK), 0) >= iota((TOK, TOK), 1)
    lane = iota((TOK, HEADS), 1)

    def step(g, diff):
        span = pl.ds(pl.multiple_of(g * NS, NS), NS)
        wide = pl.ds(pl.multiple_of(g * 256, 256), 256)
        q, k = q_ref[:, span], k_ref[:, span]
        v4, dcore4, core4 = v_ref[:, wide], dcore_ref[:, wide], core_ref[:, wide]
        scores = dot(q, k, NT)
        ds = jnp.zeros((TOK, TOK), F32)
        dq = jnp.zeros((TOK, NS), F32)
        dvs = []
        for i in range(PER_GROUP):
            h = g * PER_GROUP + i
            row = jnp.sum(jnp.where(iota((HEADS, TOK), 0) == h, cum, 0.0), axis=0, keepdims=True)
            col = jnp.sum(jnp.where(lane == h, cum_t, 0.0), axis=1, keepdims=True)
            w = jnp.where(causal, jnp.exp(jnp.where(causal, col - row, 0.0)), 0.0)
            dcore = dcore4[:, head(i)]
            dv = dot3(scores * w, dcore, TN)
            dvs.append(dv)
            v = v4[:, head(i)]
            change = dcore * core4[:, head(i)] - v.astype(F32) * dv
            diff = diff + jnp.where(lane == h, jnp.sum(change, axis=1, keepdims=True), 0.0)
            ds = ds + dot2(dcore, v, NT) * w
            dq = dq + dot3(dcore * jnp.exp(col), e_ref[h])
        dv_ref[:, wide] = jnp.concatenate(dvs, axis=1)
        dq_ref[:, span] = (dq + dot2(ds, k)).astype(BF)
        dk_ref[:, span] = dot2(ds, q, TN)
        return diff

    diff_ref[...] = lax.fori_loop(0, GROUPS, step, jnp.zeros((TOK, HEADS), F32))
    load(((dv_ref, dv_far), (dk_ref, dk_far), (dq_ref, dq_far), (diff_ref, diff_far)), sems)


def ending_kernel(
    in_ref, v_ref, k_ref, decay_ref, e_ref, dv_ref, dk_ref, diff_ref, gv_ref, gk_ref, gd_ref
):
    cum, cum_t = decay_sums(decay_ref[...])
    last = cum_t[TOK - 1 : TOK, :]
    tail = jnp.exp(last - cum_t)
    fresh = []
    kept = []
    diff = []
    for g in range(GROUPS):
        k = k_ref[:, group(g)]
        dk = dk_ref[:, group(g)]
        for h in range(PER_GROUP * g, PER_GROUP * g + PER_GROUP):
            state = in_ref[8 * h : 8 * h + 8, 128:136, :].astype(F32).reshape(HD, NS)
            exact = state.astype(BF)
            v = v_ref[:, head(h)].astype(F32)
            t = tail[:, h : h + 1]
            dv2 = t * dot(k, exact, NT)
            dk = dk + dot2(v * t, exact)
            dv = dv_ref[:, head(h)] + dv2
            gv_ref[:, head(h)] = dv.astype(BF)
            moved = jnp.sum(v * dv2, axis=1, keepdims=True)
            diff.append(moved)
            fresh.append(jnp.sum(moved).reshape(1, 1))
            kept.append(jnp.sum(e_ref[h] * state).reshape(1, 1))
        gk_ref[:, group(g)] = dk.astype(BF)
    diff = diff_ref[...] - jnp.concatenate(diff, axis=1)
    at_end = jnp.concatenate(fresh, axis=1) + jnp.exp(last) * jnp.concatenate(kept, axis=1)
    diff = diff + jnp.where(iota((TOK, HEADS), 0) == TOK - 1, at_end, 0.0)
    later = jnp.where(iota((TOK, TOK), 0) >= iota((TOK, TOK), 1), 1.0, 0.0)
    gd_ref[...] = dotp(diff, later, TN)


def chain_kernel(in_ref, shares_ref, out_ref):
    del shares_ref
    wide = in_ref[...].astype(F32)
    states = wide[:, 0:8, :].reshape(512, 128).astype(BF)
    logs = jnp.sum(wide[:, 8:16, :], axis=1)
    segment, entry = iota((512, PEERS), 0) // 8, iota((512, PEERS), 1)
    before = dotp(jnp.where(entry < segment, 1.0, 0.0), logs)
    through = dotp(jnp.where(entry <= segment, 1.0, 0.0), logs)
    i, j = iota((512, 512), 0), iota((512, 512), 1)
    later = (j // 8 > i // 8) & (j % 8 == i % 8)
    spread = jnp.transpose(before)[0:1, :] - through[:, 0:1]
    weights = jnp.where(later, jnp.exp(jnp.where(later, spread, 0.0)), 0.0)
    out_ref[:, 128:136, :] = dot2(weights, states).reshape(PEERS, 8, 128).astype(BF)


def share_kernel(in_ref, out_ref):
    for c in range(4):
        total = in_ref[0, 32 * c : 32 * c + 32, :].astype(F32)
        for peer in range(1, PEERS):
            total = total + in_ref[peer, 32 * c : 32 * c + 32, :].astype(F32)
        out_ref[:, 128 * c : 128 * c + 128] = total


def per_device(
    out_grad,
    routes,
    route_weights,
    routed_rows,
    gate_weight,
    up_weight,
    down_weight,
    values,
    key_side,
    query_side,
    decay_log,
    gate_in,
    entry_states,
    out_weight,
):
    tp_index = lax.axis_index("tp").astype(jnp.int32)
    tp = tp_index.reshape(1)
    gate_w, up_w, down_w = gate_weight[0], up_weight[0], down_weight[0]
    entry = entry_states[0]

    def swap(x):
        return lax.ppermute(x, "tp", [(0, 1), (1, 0)])

    message = dispatch(tp, routes.T, route_weights.T, out_grad)
    moved = lax.all_to_all(message, SP, split_axis=0, concat_axis=0, tiled=True)

    _, rows = lax.optimization_barrier((message, routed_rows[0]))
    rows = ordered_rows(rows)
    gate_pre = jnp.dot(rows, gate_w, preferred_element_type=F32)
    up_pre = jnp.dot(rows, up_w, preferred_element_type=F32)
    sig = jax.nn.sigmoid(gate_pre)
    silu = gate_pre * sig
    act = (silu * up_pre).astype(BF)
    a1 = up_pre * sig * (1.0 + gate_pre * (1.0 - sig))
    _, later_values = lax.optimization_barrier((message, values))
    core, mixer_out, meta = call(
        forward_kernel,
        [sds((TOK, HEADS * HD), F32), sds((TOK, HEADS * HD), BF), sds((TOK, 8), F32)],
        (later_values, key_side, query_side, decay_log, gate_in, entry, routes.T),
        10**9,
        10**6,
        name="mixer_forward",
    )
    moved, rows, act, a1, silu, core, mixer_out, meta = lax.optimization_barrier(
        (moved, rows, act, a1, silu, core, mixer_out, meta)
    )

    arrived, gate_grad, up_grad = hidden_grads(tp, moved, swap(moved), down_w, a1, silu)
    for_peer = swap(span_half(tp, True, gate_grad, up_grad, gate_w, up_w))
    own_span = span_half(tp, False, gate_grad, up_grad, gate_w, up_w)
    back = (own_span.astype(F32) + for_peer.astype(F32)).astype(BF)
    returned = lax.all_to_all(back, SP, split_axis=0, concat_axis=0, tiled=True)

    _, gate_grad, up_grad, act = lax.optimization_barrier((back, gate_grad, up_grad, act))
    grad_down = down_grad(tp, act, arrived)
    grad_gate = dot(rows, gate_grad, TN).astype(BF)
    grad_up = dot(rows, up_grad, TN).astype(BF)
    returned, grad_down, grad_gate, grad_up = lax.optimization_barrier(
        (returned, grad_down, grad_gate, grad_up)
    )

    hidden_half = combine_rows(tp, meta, returned, out_grad)
    grad_hidden, dcore, dgate, own_state = call(
        cotangent_kernel,
        [
            sds((TOK, 2 * HALF), BF),
            sds((TOK, FH), F32),
            sds((TOK, FH), BF),
            sds((PEERS, 16, NS), BF),
        ],
        (
            hidden_half,
            swap(hidden_half),
            out_weight,
            core,
            gate_in,
            decay_log,
            query_side,
        ),
        10**9,
        5 * 10**6,
        scalar=tp,
        name="mixer_cotangent",
    )
    gathered = lax.all_to_all(own_state, SP, split_axis=0, concat_axis=0, tiled=True)
    dv, dk, grad_query, diff = call(
        backward_kernel,
        [
            sds((TOK, HEADS * HD), F32),
            sds((TOK, GROUPS * NS), F32),
            sds((TOK, GROUPS * NS), BF),
            sds((TOK, HEADS), F32),
        ],
        (values, key_side, query_side, decay_log, entry, core, dcore),
        2 * 10**9,
        10**6,
        scratch=[
            pltpu.VMEM((TOK, HEADS * HD), BF),
            pltpu.VMEM((TOK, GROUPS * NS), BF),
            pltpu.VMEM((TOK, GROUPS * NS), BF),
            pltpu.VMEM((HEADS, TOK), F32),
            pltpu.VMEM((HEADS, HD, NS), F32),
            pltpu.VMEM((TOK, HEADS * HD), F32),
            pltpu.VMEM((TOK, HEADS * HD), F32),
            pltpu.VMEM((TOK, HEADS * HD), F32),
            pltpu.VMEM((TOK, GROUPS * NS), F32),
            pltpu.VMEM((TOK, GROUPS * NS), BF),
            pltpu.VMEM((TOK, HEADS), F32),
            pltpu.SemaphoreType.DMA((7,)),
        ],
        hbm_ins=tuple(range(7)),
        hbm_outs=tuple(range(4)),
        limit=60,
        name="mixer_backward",
    )
    shares_hidden, dv, dk, grad_query, diff = lax.optimization_barrier(
        (grad_hidden, dv, dk, grad_query, diff)
    )
    shares = call(
        shares_kernel,
        [sds((PEERS, 136, NS), BF)],
        (shares_hidden, mixer_out),
        10**9,
        10**6,
        name="shares",
    )[0]
    gathered, shares, dv, dk, grad_query, diff = lax.optimization_barrier(
        (gathered, shares, dv, dk, grad_query, diff)
    )
    message = call(
        chain_kernel,
        [sds((PEERS, 136, NS), BF)],
        (gathered, shares),
        10**8,
        10**6,
        aliases={1: 0},
        name="state_chain",
    )[0]
    received = lax.all_to_all(message, SP, split_axis=0, concat_axis=0, tiled=True)
    grad_out_weight = call(
        share_kernel,
        [sds((32, FH), F32)],
        (received,),
        10**7,
        10**6,
        name="share_sum",
    )[0]
    grad_values, grad_key, grad_decay = call(
        ending_kernel,
        [
            sds((TOK, HEADS * HD), BF),
            sds((TOK, GROUPS * NS), BF),
            sds((HEADS, TOK), F32),
        ],
        (received, values, key_side, decay_log, entry, dv, dk, diff),
        10**9,
        10**6,
        name="mixer_ending",
    )
    return (
        grad_hidden,
        grad_gate[None],
        grad_up[None],
        grad_down[None],
        grad_out_weight,
        grad_values,
        grad_key,
        grad_query,
        grad_decay,
        dgate,
    )


def solution(mesh):
    grid = Mesh(mesh.devices.reshape(4, 4, 4, mesh.shape["tp"]), ("sp_0", "sp_1", "sp_2", "tp"))
    placed = (
        P(SP, None),
        P(SP, None),
        P(SP, None),
        P(SP, None, None, None),
        P(SP, None, "tp"),
        P(SP, None, "tp"),
        P(SP, "tp", None),
        P(SP, "tp"),
        P(SP, "tp"),
        P(SP, "tp"),
        P("tp", SP),
        P(SP, "tp"),
        P(SP, "tp", None, None),
        P(None, "tp"),
    )
    return jax.shard_map(
        per_device,
        mesh=grid,
        in_specs=placed,
        out_specs=(
            P(SP, None),
            P(SP, None, "tp"),
            P(SP, None, "tp"),
            P(SP, "tp", None),
            P(SP, "tp"),
            P(SP, "tp"),
            P(SP, "tp"),
            P(SP, "tp"),
            P("tp", SP),
            P(SP, "tp"),
        ),
        check_vma=False,
    )
```

```python
import functools

import jax
import jax.numpy as jnp
from jax import lax
from jax.experimental import pallas as pl
from jax.experimental.pallas import tpu as pltpu
from jax.sharding import Mesh
from jax.sharding import PartitionSpec as P

BF = jnp.bfloat16
F32 = jnp.float32
SP = ("sp_0", "sp_1", "sp_2")
PEERS = 64
CAP = 18
MAIN = 16
TAIL = CAP - MAIN
TOK = 224
HALF = 1024
COLS = HALF // 128
MSG = COLS * CAP
FH = 512
HEADS = 8
HD = 64
NS = 128
PER_GROUP = 4
GROUPS = 2

NT = (((1,), (1,)), ((), ()))
TN = (((0,), (0,)), ((), ()))
NN = (((1,), (0,)), ((), ()))


def cost(flops, nbytes):
    return pl.CostEstimate(flops=flops, bytes_accessed=nbytes, transcendentals=0)


def iota(shape, dim):
    return lax.broadcasted_iota(jnp.int32, shape, dim)


def dot(a, b, dims=NN):
    return lax.dot_general(a, b, dims, preferred_element_type=F32)


def split(a):
    hi = a.astype(BF)
    return hi, (a - hi.astype(F32)).astype(BF)


def dot2(a, b, dims=NN):
    hi, lo = split(a)
    return dot(hi, b, dims) + dot(lo, b, dims)


def dot2r(a, b, dims=NN):
    hi, lo = split(b)
    return dot(a, hi, dims) + dot(a, lo, dims)


def dot3(a, b, dims=NN):
    ah, al = split(a)
    bh, bl = split(b)
    return dot(ah, bh, dims) + (dot(ah, bl, dims) + dot(al, bh, dims))


def dotp(a, b, dims=NN):
    return lax.dot_general(
        a, b, dims, precision=lax.Precision.HIGHEST, preferred_element_type=F32
    )


def tail_rows(shape, row_dim):
    r = iota(shape, row_dim)
    return (r // TAIL) * 16 + (r % TAIL) * 8


def pack_tail(dt):
    place = iota((1024, 128), 0) - tail_rows((1024, 128), 1)
    out = None
    for c in range(COLS):
        mask = jnp.where(place == c, 1.0, 0.0).astype(BF)
        part = dot(mask, dt[:, c * 128 : (c + 1) * 128])
        out = part if out is None else out + part
    return out


def begin(far, near, sem):
    copy = pltpu.make_async_copy(far, near, sem)
    copy.start()
    return copy


def load(pairs, sems):
    copies = [
        pltpu.make_async_copy(far, near, sems.at[i]) for i, (far, near) in enumerate(pairs)
    ]
    for copy in copies:
        copy.start()
    for copy in copies:
        copy.wait()


def slots(routes):
    experts = iota((PEERS, TOK), 0)
    r0, r1 = routes[0:1, :], routes[1:2, :]
    h0, h1 = experts == r0, experts == r1
    counts = jnp.where(h0, 1.0, 0.0) + jnp.where(h1, 1.0, 0.0)
    before = jnp.where(iota((TOK, TOK), 0) < iota((TOK, TOK), 1), 1.0, 0.0).astype(BF)
    earlier = dot(counts.astype(BF), before)
    f0 = jnp.sum(jnp.where(h0, earlier, 0.0), axis=0, keepdims=True)
    f1 = jnp.sum(jnp.where(h1, earlier, 0.0), axis=0, keepdims=True)
    return r0, r1, f0, f1


def dispatch_kernel(
    tp_ref, far_routes, far_w, far_og, to_ref, routes_ref, w_ref, og_ref, out_ref, sems, in_sems
):
    own = half_of(tp_ref)
    load_routes = begin(far_routes, routes_ref, in_sems.at[0])
    load_w = begin(far_w, w_ref, in_sems.at[1])
    load_og = begin(far_og.at[:, own], og_ref, in_sems.at[2])
    load_routes.wait()
    r0, r1, f0, f1 = slots(routes_ref[...])
    load_w.wait()
    w0, w1 = w_ref[0:1, :], w_ref[1:2, :]
    s0, s1 = f0.astype(jnp.int32), f1.astype(jnp.int32)
    m0 = jnp.where(s0 < MAIN, r0 * MAIN + s0, -1)
    m1 = jnp.where(s1 < MAIN, r1 * MAIN + s1, -1)
    t0 = jnp.where(s0 >= MAIN, r0 * TAIL + s0 - MAIN, -1)
    t1 = jnp.where(s1 >= MAIN, r1 * TAIL + s1 - MAIN, -1)
    load_og.wait()
    og = og_ref[...]

    def rows_of(first, count, a0, a1):
        rows = iota((count, TOK), 0) + first
        q0, q1 = rows == a0, rows == a1
        pick = jnp.where(q0 | q1, 1.0, 0.0).astype(BF)
        scale = jnp.where(q0, w0, jnp.where(q1, w1, 0.0))
        scale = jnp.sum(scale, axis=1, keepdims=True)
        return (dot(pick, og) * scale).astype(BF)

    copies = []
    for b in range(4):
        block = rows_of(256 * b, 256, m0, m1)
        peers = slice(16 * b, 16 * b + 16)
        for c in range(COLS):
            out_ref[peers, 16 * c : 16 * c + 16, :] = block[:, 128 * c : 128 * c + 128].reshape(
                16, 16, 128
            )
        main = slice(0, 16 * COLS)
        copies.append(begin(out_ref.at[peers, main], to_ref.at[peers, main], sems.at[b]))
    tail = pack_tail(rows_of(0, 128, t0, t1)).astype(BF)
    out_ref[:, 16 * COLS : MSG, :] = tail.reshape(PEERS, 16, 128)
    rest = slice(16 * COLS, MSG)
    copies.append(begin(out_ref.at[:, rest], to_ref.at[:, rest], sems.at[4]))
    for copy in copies:
        copy.wait()


def call(
    kernel,
    outs,
    args,
    flops,
    nbytes,
    scalar=None,
    scratch=(),
    name=None,
    limit=8,
    hbm_outs=(),
    hbm_ins=(),
    aliases=None,
):
    vmem = pl.BlockSpec(memory_space=pltpu.VMEM)
    far = pl.BlockSpec(memory_space=pltpu.HBM)
    in_specs = [far if i in hbm_ins else vmem for i in range(len(args))]
    if scalar is not None:
        in_specs = [pl.BlockSpec(memory_space=pltpu.SMEM)] + in_specs
        args = (scalar, *args)
    return pl.pallas_call(
        kernel,
        out_shape=outs,
        in_specs=in_specs,
        out_specs=[far if i in hbm_outs else vmem for i in range(len(outs))],
        scratch_shapes=list(scratch),
        input_output_aliases=aliases or {},
        compiler_params=pltpu.CompilerParams(vmem_limit_bytes=limit * 1024 * 1024),
        cost_estimate=cost(flops, nbytes),
        name=name,
    )(*args)


def sds(shape, dtype):
    return jax.ShapeDtypeStruct(shape, dtype)


def dispatch(tp, routes_t, weights_t, out_grad):
    dma = pltpu.SemaphoreType.DMA
    return call(
        dispatch_kernel,
        [sds((PEERS, MSG, 128), BF)],
        (routes_t, weights_t, out_grad),
        10**9,
        3 * 10**6,
        scalar=tp,
        scratch=[
            pltpu.VMEM((2, TOK), jnp.int32),
            pltpu.VMEM((2, TOK), F32),
            pltpu.VMEM((TOK, HALF), BF),
            pltpu.VMEM((PEERS, MSG, 128), BF),
            dma((5,)),
            dma((3,)),
        ],
        hbm_ins=(0, 1, 2),
        hbm_outs=(0,),
        limit=60,
        name="dispatch",
    )[0]


def half_of(tp_ref, other=False):
    half = 1 - tp_ref[0] if other else tp_ref[0]
    return pl.ds(pl.multiple_of(half * HALF, HALF), HALF)


def combine_kernel(tp_ref, meta_ref, ret_ref, og_ref, out_ref):
    meta = meta_ref[...].astype(jnp.int32)
    e0, s0, e1, s1 = (meta[:, k : k + 1] for k in range(4))
    m0 = jnp.where(s0 < MAIN, e0 * MAIN + s0, -1)
    m1 = jnp.where(s1 < MAIN, e1 * MAIN + s1, -1)
    t0 = jnp.where(s0 >= MAIN, e0 * 16 + (s0 - MAIN) * 8, -100)
    t1 = jnp.where(s1 >= MAIN, e1 * 16 + (s1 - MAIN) * 8, -100)
    lanes = iota((TOK, 1024), 1)
    pick = jnp.where((lanes == m0) | (lanes == m1), 1.0, 0.0).astype(BF)
    tail = ret_ref[:, 16 * COLS : MSG, :].reshape(1024, 128)
    d0, d1 = lanes - t0, lanes - t1

    for c in range(0, COLS, 2):
        pair = [ret_ref[:, 16 * k : 16 * k + 16, :].reshape(1024, 128) for k in (c, c + 1)]
        moe = dot(pick, jnp.concatenate(pair, axis=1))
        masks = [jnp.where((d0 == k) | (d1 == k), 1.0, 0.0).astype(BF) for k in (c, c + 1)]
        moe = moe + jnp.concatenate([dot(m, tail) for m in masks], axis=1)
        own = og_ref[:, pl.ds(pl.multiple_of(tp_ref[0] * HALF + c * 128, 256), 256)]
        out_ref[:, 128 * c : 128 * c + 256] = (own.astype(F32) + moe).astype(BF)


def combine_rows(tp, meta, returned, out_grad):
    return call(
        combine_kernel,
        [sds((TOK, HALF), BF)],
        (meta, returned, out_grad),
        10**9,
        3 * 10**6,
        scalar=tp,
        name="combine",
    )[0]


def place_rows(msg_ref, arr_ref):
    for c in range(COLS):
        main = msg_ref[:, 16 * c : 16 * c + 16, :].reshape(1024, 128)
        arr_ref[0:1024, 128 * c : 128 * c + 128] = main
    tail = msg_ref[:, 16 * COLS : MSG, :].reshape(1024, 128)
    at = iota((128, 1024), 1) - tail_rows((128, 1024), 0)
    for c in range(COLS):
        mask = jnp.where(at == c, 1.0, 0.0).astype(BF)
        arr_ref[1024:1152, 128 * c : 128 * c + 128] = dot(mask, tail).astype(BF)


def order_kernel(in_ref, out_ref):
    i, j = iota((256, 256), 0), iota((256, 256), 1)
    turn = jnp.where((i // 16 == j % 16) & (i % 16 == j // 16), 1.0, 0.0).astype(BF)
    for b in range(4):
        x = in_ref[0:MAIN, 16 * b : 16 * b + 16, :].reshape(256, -1)
        out_ref[256 * b : 256 * b + 256, :] = dot(turn, x).astype(BF)
    i, j = iota((128, 128), 0), iota((128, 128), 1)
    turn = jnp.where((i // 2 == j % 64) & (i % 2 == j // 64), 1.0, 0.0).astype(BF)
    x = in_ref[MAIN:CAP, :, :].reshape(128, -1)
    out_ref[1024:1152, :] = dot(turn, x).astype(BF)


def ordered_rows(rows):
    width = rows.shape[-1]
    return call(
        order_kernel,
        [sds((PEERS * CAP, width), BF)],
        (jnp.transpose(rows, (1, 0, 2)),),
        10**9,
        10**7,
        limit=16,
        name="ordered_rows",
    )[0]


def first_half_kernel(tp_ref, mine_ref, down_ref, arr_ref, part_ref):
    place_rows(mine_ref, arr_ref)
    part_ref[...] = dot(arr_ref[...], down_ref[:, half_of(tp_ref)], NT)


def second_half_kernel(
    tp_ref, other_ref, down_ref, part_ref, a1_ref, a2_ref, arr_ref, gg_ref, ug_ref
):
    place_rows(other_ref, arr_ref)
    act_grad = part_ref[...] + dot(arr_ref[...], down_ref[:, half_of(tp_ref, True)], NT)
    gg_ref[...] = (act_grad * a1_ref[...]).astype(BF)
    ug_ref[...] = (act_grad * a2_ref[...]).astype(BF)


def hidden_grads(tp, mine, other, down, a1, a2):
    rows = PEERS * CAP
    own_cols, part = call(
        first_half_kernel,
        [sds((rows, HALF), BF), sds((rows, FH), F32)],
        (mine, down),
        2 * 10**9,
        10**7,
        scalar=tp,
        name="hidden_first",
    )
    other_cols, gg, ug = call(
        second_half_kernel,
        [sds((rows, HALF), BF), sds((rows, FH), BF), sds((rows, FH), BF)],
        (other, down, part, a1, a2),
        2 * 10**9,
        10**7,
        scalar=tp,
        name="hidden_second",
    )
    return (own_cols, other_cols), gg, ug


def down_kernel(tp_ref, act_ref, own_ref, other_ref, out_ref):
    def step(n, carry):
        cols = pl.ds(pl.multiple_of(256 * n, 256), 256)
        for other, ref in ((False, own_ref), (True, other_ref)):
            half = 1 - tp_ref[0] if other else tp_ref[0]
            to = pl.ds(pl.multiple_of(half * HALF + 256 * n, 256), 256)
            out_ref[:, to] = dot(act_ref[...], ref[:, cols], TN).astype(BF)
        return carry

    lax.fori_loop(0, 4, step, 0)


def down_grad(tp, act, arrived):
    return call(
        down_kernel,
        [sds((FH, 2 * HALF), BF)],
        (act, *arrived),
        2 * 10**9,
        10**7,
        scalar=tp,
        name="down_grad",
    )[0]


def span_kernel(other, half_ref, gg_ref, ug_ref, gw_ref, uw_ref, out_ref, tail_ref):
    base = (1 - half_ref[0] if other else half_ref[0]) * HALF

    def block(n):
        cols = pl.ds(pl.multiple_of(base + 256 * n, 256), 256)
        d = dot(gg_ref[...], gw_ref[cols, :], NT) + dot(ug_ref[...], uw_ref[cols, :], NT)
        d = d.astype(BF)
        for k in range(2):
            c = 2 * n + k
            part = d[:, 128 * k : 128 * k + 128]
            rows = pl.ds(pl.multiple_of(16 * c, 16), 16)
            out_ref[:, rows, :] = part[:1024].reshape(PEERS, 16, 128)
            tail_ref[:, pl.ds(pl.multiple_of(128 * c, 128), 128)] = part[1024:]

    def step(n, carry):
        block(2 * n)
        block(2 * n + 1)
        return carry

    lax.fori_loop(0, 2, step, 0)
    tail = pack_tail(tail_ref[...]).astype(BF)
    out_ref[:, 16 * COLS : MSG, :] = tail.reshape(PEERS, 16, 128)


def span_half(tp, other, gg, ug, gw, uw):
    return call(
        functools.partial(span_kernel, other),
        [sds((PEERS, MSG, 128), BF)],
        (gg, ug, gw, uw),
        4 * 10**9,
        10**7,
        scalar=tp,
        scratch=[pltpu.VMEM((128, HALF), BF)],
        name="span_half",
    )[0]


def decay_sums(decay):
    upto = jnp.where(iota((TOK, TOK), 0) <= iota((TOK, TOK), 1), 1.0, 0.0)
    down = jnp.where(iota((TOK, TOK), 0) >= iota((TOK, TOK), 1), 1.0, 0.0)
    return dotp(decay, upto), dotp(down, decay, NT)


def decay_weights(cum, cum_t, h):
    causal = iota((TOK, TOK), 0) >= iota((TOK, TOK), 1)
    spread = cum_t[:, h : h + 1] - cum[h : h + 1, :]
    return jnp.where(causal, jnp.exp(jnp.where(causal, spread, 0.0)), 0.0)


def head(h):
    return slice(HD * h, HD * h + HD)


def group(g):
    return slice(NS * g, NS * g + NS)


def forward_kernel(
    v_ref, k_ref, q_ref, decay_ref, gate_ref, e_ref, routes_ref, core_ref, mixed_ref, meta_ref, fade_ref
):
    r0, r1, f0, f1 = slots(routes_ref[...])
    zero = jnp.zeros((4, TOK), F32)
    table = jnp.concatenate([r0.astype(F32), f0, r1.astype(F32), f1, zero], axis=0).astype(BF)
    eye = jnp.where(iota((TOK, TOK), 0) == iota((TOK, TOK), 1), 1.0, 0.0).astype(BF)
    meta_ref[...] = dot(eye, table, NT)
    cum, cum_t = decay_sums(decay_ref[...])
    fade_ref[:, 0:HEADS] = jnp.exp(cum_t)
    fade_ref[:, HEADS : 2 * HEADS] = jnp.exp(cum_t[TOK - 1 : TOK, :] - cum_t)
    for g in range(GROUPS):
        q, k = q_ref[:, group(g)], k_ref[:, group(g)]
        scores = dot(q, k, NT)
        for h in range(PER_GROUP * g, PER_GROUP * g + PER_GROUP):
            m = scores * decay_weights(cum, cum_t, h)
            within = dot2(m, v_ref[:, head(h)])
            carried = dot2r(q, e_ref[h], NT)
            core = within + carried * jnp.exp(cum_t[:, h : h + 1])
            core_ref[:, head(h)] = core
            gate = gate_ref[:, head(h)].astype(F32)
            mixed_ref[:, head(h)] = (core * (gate * jax.nn.sigmoid(gate))).astype(BF)


def low_part(a, hi):
    return a - hi.astype(F32)


def cotangent_kernel(
    tp_ref, mine_ref, other_ref, ow_ref, core_ref, gate_ref, decay_ref, q_ref, fade_ref,
    hidden_ref, dcore_ref, dgate_ref, msg_ref,
):
    first = tp_ref[0] == 0
    x, y = mine_ref[...], other_ref[...]
    lo, hi = jnp.where(first, x, y), jnp.where(first, y, x)
    hidden_ref[:, :HALF] = lo
    hidden_ref[:, HALF:] = hi
    cot = dot(lo, ow_ref[:HALF, :]) + dot(hi, ow_ref[HALF:, :])
    gate = gate_ref[...].astype(F32)
    sig = jax.nn.sigmoid(gate)
    dcore = cot * (gate * sig)
    dcore_ref[...] = dcore
    dgate_ref[...] = (cot * core_ref[...] * (sig * (1.0 + gate * (1.0 - sig)))).astype(BF)
    growth = fade_ref[:, 0:HEADS]
    logs = jnp.sum(decay_ref[...], axis=1, keepdims=True)
    high, low = split(logs)
    mid, _ = split(low_part(logs, high))
    rest = low_part(logs, high) - mid.astype(F32)
    row = iota((8, 8, 128), 1)
    states = []
    for g in range(GROUPS):
        heads = range(PER_GROUP * g, PER_GROUP * g + PER_GROUP)
        grown = [dcore[:, head(h)] * growth[:, h : h + 1] for h in heads]
        states.append(dot2(jnp.concatenate(grown, axis=1), q_ref[:, group(g)], TN))
    for h in range(HEADS):
        at = HD * (h % PER_GROUP)
        state = states[h // PER_GROUP][at : at + HD]
        parts = [
            jnp.broadcast_to(p[h : h + 1, :], (8, 128)).reshape(1, 8, 128)
            for p in (high.astype(F32), mid.astype(F32), rest)
        ]
        extra = jnp.where(row == 0, parts[0], jnp.where(row == 1, parts[1], parts[2]))
        extra = jnp.where(row < 3, extra, 0.0)
        both = jnp.concatenate([state.reshape(8, 8, 128), extra], axis=1)
        msg_ref[8 * h : 8 * h + 8] = both.astype(BF)


def shares_kernel(hidden_ref, mixed_ref, msg_ref):
    def step(b, carry):
        rows = hidden_ref[:, pl.ds(pl.multiple_of(512 * b, 512), 512)]
        share = dot(rows, mixed_ref[...], TN).astype(BF)
        peers = pl.ds(pl.multiple_of(16 * b, 16), 16)
        for c in range(4):
            msg_ref[peers, 32 * c : 32 * c + 32, :] = share[:, 128 * c : 128 * c + 128].reshape(
                16, 32, 128
            )
        return carry

    lax.fori_loop(0, 4, step, 0)
    msg_ref[:, 128:136, :] = jnp.zeros((PEERS, 8, 128), BF)


def backward_kernel(
    v_far, k_far, q_far, decay_far, e_far, core_far, dcore_far,
    dv_far, dk_far, dq_far, diff_far,
    v_ref, k_ref, q_ref, decay_ref, e_ref, core_ref, dcore_ref,
    dv_ref, dk_ref, dq_ref, diff_ref, sems,
):
    load(
        (
            (decay_far, decay_ref),
            (q_far, q_ref),
            (k_far, k_ref),
            (v_far, v_ref),
            (e_far, e_ref),
            (dcore_far, dcore_ref),
            (core_far, core_ref),
        ),
        sems,
    )
    cum, cum_t = decay_sums(decay_ref[...])
    causal = iota((TOK, TOK), 0) >= iota((TOK, TOK), 1)
    lane = iota((TOK, HEADS), 1)

    def step(g, diff):
        span = pl.ds(pl.multiple_of(g * NS, NS), NS)
        wide = pl.ds(pl.multiple_of(g * 256, 256), 256)
        q, k = q_ref[:, span], k_ref[:, span]
        v4, dcore4, core4 = v_ref[:, wide], dcore_ref[:, wide], core_ref[:, wide]
        scores = dot(q, k, NT)
        ds = jnp.zeros((TOK, TOK), F32)
        dq = jnp.zeros((TOK, NS), F32)
        dvs = []
        for i in range(PER_GROUP):
            h = g * PER_GROUP + i
            row = jnp.sum(jnp.where(iota((HEADS, TOK), 0) == h, cum, 0.0), axis=0, keepdims=True)
            col = jnp.sum(jnp.where(lane == h, cum_t, 0.0), axis=1, keepdims=True)
            w = jnp.where(causal, jnp.exp(jnp.where(causal, col - row, 0.0)), 0.0)
            dcore = dcore4[:, head(i)]
            dv = dot3(scores * w, dcore, TN)
            dvs.append(dv)
            v = v4[:, head(i)]
            change = dcore * core4[:, head(i)] - v.astype(F32) * dv
            diff = diff + jnp.where(lane == h, jnp.sum(change, axis=1, keepdims=True), 0.0)
            ds = ds + dot2(dcore, v, NT) * w
            dq = dq + dot3(dcore * jnp.exp(col), e_ref[h])
        dv_ref[:, wide] = jnp.concatenate(dvs, axis=1)
        dq_ref[:, span] = (dq + dot2(ds, k)).astype(BF)
        dk_ref[:, span] = dot2(ds, q, TN)
        return diff

    diff_ref[...] = lax.fori_loop(0, GROUPS, step, jnp.zeros((TOK, HEADS), F32))
    load(((dv_ref, dv_far), (dk_ref, dk_far), (dq_ref, dq_far), (diff_ref, diff_far)), sems)


def ending_kernel(
    in_ref, v_ref, k_ref, fade_ref, e_ref, dv_ref, dk_ref, diff_ref, gv_ref, gk_ref, gd_ref
):
    fade = fade_ref[...]
    tail = fade[:, HEADS : 2 * HEADS]
    last = fade[TOK - 1 : TOK, 0:HEADS]
    fresh, kept, diff = [], [], []
    for g in range(GROUPS):
        wide = slice(256 * g, 256 * g + 256)
        heads = range(PER_GROUP * g, PER_GROUP * g + PER_GROUP)
        state = in_ref[32 * g : 32 * g + 32, 128:136, :].astype(F32).reshape(PER_GROUP * HD, NS)
        exact = state.astype(BF)
        v = v_ref[:, wide].astype(F32)
        spread = [jnp.broadcast_to(tail[:, h : h + 1], (TOK, HD)) for h in heads]
        spread = jnp.concatenate(spread, axis=1)
        dv2 = spread * dot(k_ref[:, group(g)], exact, NT)
        gv_ref[:, wide] = (dv_ref[:, wide] + dv2).astype(BF)
        gk_ref[:, group(g)] = (dk_ref[:, group(g)] + dot2(v * spread, exact)).astype(BF)
        change = v * dv2
        for i, h in enumerate(heads):
            moved = jnp.sum(change[:, head(i)], axis=1, keepdims=True)
            diff.append(moved)
            fresh.append(jnp.sum(moved).reshape(1, 1))
            kept.append(jnp.sum(e_ref[h] * state[head(i)]).reshape(1, 1))
    diff = diff_ref[...] - jnp.concatenate(diff, axis=1)
    at_end = jnp.concatenate(fresh, axis=1) + last * jnp.concatenate(kept, axis=1)
    diff = diff + jnp.where(iota((TOK, HEADS), 0) == TOK - 1, at_end, 0.0)
    later = jnp.where(iota((TOK, TOK), 0) >= iota((TOK, TOK), 1), 1.0, 0.0)
    gd_ref[...] = dotp(diff, later, TN)


def chain_kernel(in_ref, shares_ref, out_ref):
    del shares_ref
    wide = in_ref[...].astype(F32)
    states = wide[:, 0:8, :].reshape(512, 128).astype(BF)
    logs = jnp.sum(wide[:, 8:16, :], axis=1)
    segment, entry = iota((512, PEERS), 0) // 8, iota((512, PEERS), 1)
    before = dotp(jnp.where(entry < segment, 1.0, 0.0), logs)
    through = dotp(jnp.where(entry <= segment, 1.0, 0.0), logs)
    i, j = iota((512, 512), 0), iota((512, 512), 1)
    later = (j // 8 > i // 8) & (j % 8 == i % 8)
    spread = jnp.transpose(before)[0:1, :] - through[:, 0:1]
    weights = jnp.where(later, jnp.exp(jnp.where(later, spread, 0.0)), 0.0)
    out_ref[:, 128:136, :] = dot2(weights, states).reshape(PEERS, 8, 128).astype(BF)


def share_kernel(in_ref, out_ref):
    for c in range(4):
        total = in_ref[0, 32 * c : 32 * c + 32, :].astype(F32)
        for peer in range(1, PEERS):
            total = total + in_ref[peer, 32 * c : 32 * c + 32, :].astype(F32)
        out_ref[:, 128 * c : 128 * c + 128] = total


def per_device(
    out_grad,
    routes,
    route_weights,
    routed_rows,
    gate_weight,
    up_weight,
    down_weight,
    values,
    key_side,
    query_side,
    decay_log,
    gate_in,
    entry_states,
    out_weight,
):
    tp_index = lax.axis_index("tp").astype(jnp.int32)
    tp = tp_index.reshape(1)
    gate_w, up_w, down_w = gate_weight[0], up_weight[0], down_weight[0]
    entry = entry_states[0]

    def swap(x):
        return lax.ppermute(x, "tp", [(0, 1), (1, 0)])

    message = dispatch(tp, routes.T, route_weights.T, out_grad)
    moved = lax.all_to_all(message, SP, split_axis=0, concat_axis=0, tiled=True)

    _, rows = lax.optimization_barrier((message, routed_rows[0]))
    rows = ordered_rows(rows)
    gate_pre = jnp.dot(rows, gate_w, preferred_element_type=F32)
    up_pre = jnp.dot(rows, up_w, preferred_element_type=F32)
    sig = jax.nn.sigmoid(gate_pre)
    silu = gate_pre * sig
    act = (silu * up_pre).astype(BF)
    a1 = up_pre * sig * (1.0 + gate_pre * (1.0 - sig))
    _, later_values = lax.optimization_barrier((message, values))
    core, mixer_out, meta, fade = call(
        forward_kernel,
        [sds((TOK, HEADS * HD), F32), sds((TOK, HEADS * HD), BF), sds((TOK, 8), F32), sds((TOK, 16), F32)],
        (later_values, key_side, query_side, decay_log, gate_in, entry, routes.T),
        10**9,
        10**6,
        name="mixer_forward",
    )
    moved, rows, act, a1, silu, core, mixer_out, meta, fade = lax.optimization_barrier(
        (moved, rows, act, a1, silu, core, mixer_out, meta, fade)
    )

    arrived, gate_grad, up_grad = hidden_grads(tp, moved, swap(moved), down_w, a1, silu)
    for_peer = swap(span_half(tp, True, gate_grad, up_grad, gate_w, up_w))
    own_span = span_half(tp, False, gate_grad, up_grad, gate_w, up_w)
    back = (own_span.astype(F32) + for_peer.astype(F32)).astype(BF)
    returned = lax.all_to_all(back, SP, split_axis=0, concat_axis=0, tiled=True)

    _, gate_grad, up_grad, act = lax.optimization_barrier((back, gate_grad, up_grad, act))
    grad_down = down_grad(tp, act, arrived)
    grad_gate = dot(rows, gate_grad, TN).astype(BF)
    grad_up = dot(rows, up_grad, TN).astype(BF)
    returned, grad_down, grad_gate, grad_up = lax.optimization_barrier(
        (returned, grad_down, grad_gate, grad_up)
    )

    hidden_half = combine_rows(tp, meta, returned, out_grad)
    grad_hidden, dcore, dgate, own_state = call(
        cotangent_kernel,
        [
            sds((TOK, 2 * HALF), BF),
            sds((TOK, FH), F32),
            sds((TOK, FH), BF),
            sds((PEERS, 16, NS), BF),
        ],
        (
            hidden_half,
            swap(hidden_half),
            out_weight,
            core,
            gate_in,
            decay_log,
            query_side,
            fade,
        ),
        10**9,
        5 * 10**6,
        scalar=tp,
        name="mixer_cotangent",
    )
    gathered = lax.all_to_all(own_state, SP, split_axis=0, concat_axis=0, tiled=True)
    dv, dk, grad_query, diff = call(
        backward_kernel,
        [
            sds((TOK, HEADS * HD), F32),
            sds((TOK, GROUPS * NS), F32),
            sds((TOK, GROUPS * NS), BF),
            sds((TOK, HEADS), F32),
        ],
        (values, key_side, query_side, decay_log, entry, core, dcore),
        2 * 10**9,
        10**6,
        scratch=[
            pltpu.VMEM((TOK, HEADS * HD), BF),
            pltpu.VMEM((TOK, GROUPS * NS), BF),
            pltpu.VMEM((TOK, GROUPS * NS), BF),
            pltpu.VMEM((HEADS, TOK), F32),
            pltpu.VMEM((HEADS, HD, NS), F32),
            pltpu.VMEM((TOK, HEADS * HD), F32),
            pltpu.VMEM((TOK, HEADS * HD), F32),
            pltpu.VMEM((TOK, HEADS * HD), F32),
            pltpu.VMEM((TOK, GROUPS * NS), F32),
            pltpu.VMEM((TOK, GROUPS * NS), BF),
            pltpu.VMEM((TOK, HEADS), F32),
            pltpu.SemaphoreType.DMA((7,)),
        ],
        hbm_ins=tuple(range(7)),
        hbm_outs=tuple(range(4)),
        limit=60,
        name="mixer_backward",
    )
    shares_hidden, dv, dk, grad_query, diff = lax.optimization_barrier(
        (grad_hidden, dv, dk, grad_query, diff)
    )
    shares = call(
        shares_kernel,
        [sds((PEERS, 136, NS), BF)],
        (shares_hidden, mixer_out),
        10**9,
        10**6,
        name="shares",
    )[0]
    gathered, shares, dv, dk, grad_query, diff = lax.optimization_barrier(
        (gathered, shares, dv, dk, grad_query, diff)
    )
    message = call(
        chain_kernel,
        [sds((PEERS, 136, NS), BF)],
        (gathered, shares),
        10**8,
        10**6,
        aliases={1: 0},
        name="state_chain",
    )[0]
    received = lax.all_to_all(message, SP, split_axis=0, concat_axis=0, tiled=True)
    grad_out_weight = call(
        share_kernel,
        [sds((32, FH), F32)],
        (received,),
        10**7,
        10**6,
        name="share_sum",
    )[0]
    grad_values, grad_key, grad_decay = call(
        ending_kernel,
        [
            sds((TOK, HEADS * HD), BF),
            sds((TOK, GROUPS * NS), BF),
            sds((HEADS, TOK), F32),
        ],
        (received, values, key_side, fade, entry, dv, dk, diff),
        10**9,
        10**6,
        name="mixer_ending",
    )
    return (
        grad_hidden,
        grad_gate[None],
        grad_up[None],
        grad_down[None],
        grad_out_weight,
        grad_values,
        grad_key,
        grad_query,
        grad_decay,
        dgate,
    )


def solution(mesh):
    grid = Mesh(mesh.devices.reshape(4, 4, 4, mesh.shape["tp"]), ("sp_0", "sp_1", "sp_2", "tp"))
    placed = (
        P(SP, None),
        P(SP, None),
        P(SP, None),
        P(SP, None, None, None),
        P(SP, None, "tp"),
        P(SP, None, "tp"),
        P(SP, "tp", None),
        P(SP, "tp"),
        P(SP, "tp"),
        P(SP, "tp"),
        P("tp", SP),
        P(SP, "tp"),
        P(SP, "tp", None, None),
        P(None, "tp"),
    )
    return jax.shard_map(
        per_device,
        mesh=grid,
        in_specs=placed,
        out_specs=(
            P(SP, None),
            P(SP, None, "tp"),
            P(SP, None, "tp"),
            P(SP, "tp", None),
            P(SP, "tp"),
            P(SP, "tp"),
            P(SP, "tp"),
            P(SP, "tp"),
            P("tp", SP),
            P(SP, "tp"),
        ),
        check_vma=False,
    )
```

```python
import functools

import jax
import jax.numpy as jnp
from jax import lax
from jax.experimental import pallas as pl
from jax.experimental.pallas import tpu as pltpu
from jax.sharding import Mesh
from jax.sharding import PartitionSpec as P

BF = jnp.bfloat16
F32 = jnp.float32
SP = ("sp_0", "sp_1", "sp_2")
PEERS = 64
CAP = 18
MAIN = 16
TAIL = CAP - MAIN
TOK = 224
HALF = 1024
COLS = HALF // 128
MSG = COLS * CAP
FH = 512
HEADS = 8
HD = 64
NS = 128
PER_GROUP = 4
GROUPS = 2

NT = (((1,), (1,)), ((), ()))
TN = (((0,), (0,)), ((), ()))
NN = (((1,), (0,)), ((), ()))


def cost(flops, nbytes):
    return pl.CostEstimate(flops=flops, bytes_accessed=nbytes, transcendentals=0)


def iota(shape, dim):
    return lax.broadcasted_iota(jnp.int32, shape, dim)


def dot(a, b, dims=NN):
    return lax.dot_general(a, b, dims, preferred_element_type=F32)


def split(a):
    hi = a.astype(BF)
    return hi, (a - hi.astype(F32)).astype(BF)


def dot2(a, b, dims=NN):
    hi, lo = split(a)
    return dot(hi, b, dims) + dot(lo, b, dims)


def dot2r(a, b, dims=NN):
    hi, lo = split(b)
    return dot(a, hi, dims) + dot(a, lo, dims)


def dot3(a, b, dims=NN):
    ah, al = split(a)
    bh, bl = split(b)
    return dot(ah, bh, dims) + (dot(ah, bl, dims) + dot(al, bh, dims))


def dotp(a, b, dims=NN):
    return lax.dot_general(
        a, b, dims, precision=lax.Precision.HIGHEST, preferred_element_type=F32
    )


def tail_rows(shape, row_dim):
    r = iota(shape, row_dim)
    return (r // TAIL) * 16 + (r % TAIL) * 8


def pack_tail(dt):
    place = iota((1024, 128), 0) - tail_rows((1024, 128), 1)
    out = None
    for c in range(COLS):
        mask = jnp.where(place == c, 1.0, 0.0).astype(BF)
        part = dot(mask, dt[:, c * 128 : (c + 1) * 128])
        out = part if out is None else out + part
    return out


def begin(far, near, sem):
    copy = pltpu.make_async_copy(far, near, sem)
    copy.start()
    return copy


def load(pairs, sems):
    copies = [
        pltpu.make_async_copy(far, near, sems.at[i]) for i, (far, near) in enumerate(pairs)
    ]
    for copy in copies:
        copy.start()
    for copy in copies:
        copy.wait()


def slots(routes):
    experts = iota((PEERS, TOK), 0)
    r0, r1 = routes[0:1, :], routes[1:2, :]
    h0, h1 = experts == r0, experts == r1
    counts = jnp.where(h0, 1.0, 0.0) + jnp.where(h1, 1.0, 0.0)
    before = jnp.where(iota((TOK, TOK), 0) < iota((TOK, TOK), 1), 1.0, 0.0).astype(BF)
    earlier = dot(counts.astype(BF), before)
    f0 = jnp.sum(jnp.where(h0, earlier, 0.0), axis=0, keepdims=True)
    f1 = jnp.sum(jnp.where(h1, earlier, 0.0), axis=0, keepdims=True)
    return r0, r1, f0, f1


def dispatch_kernel(
    tp_ref, far_routes, far_w, far_og, to_ref, routes_ref, w_ref, og_ref, out_ref, sems, in_sems
):
    own = half_of(tp_ref)
    load_routes = begin(far_routes, routes_ref, in_sems.at[0])
    load_w = begin(far_w, w_ref, in_sems.at[1])
    load_og = begin(far_og.at[:, own], og_ref, in_sems.at[2])
    load_routes.wait()
    r0, r1, f0, f1 = slots(routes_ref[...])
    load_w.wait()
    w0, w1 = w_ref[0:1, :], w_ref[1:2, :]
    s0, s1 = f0.astype(jnp.int32), f1.astype(jnp.int32)
    m0 = jnp.where(s0 < MAIN, r0 * MAIN + s0, -1)
    m1 = jnp.where(s1 < MAIN, r1 * MAIN + s1, -1)
    t0 = jnp.where(s0 >= MAIN, r0 * TAIL + s0 - MAIN, -1)
    t1 = jnp.where(s1 >= MAIN, r1 * TAIL + s1 - MAIN, -1)
    load_og.wait()
    og = og_ref[...]

    def rows_of(first, count, a0, a1):
        rows = iota((count, TOK), 0) + first
        q0, q1 = rows == a0, rows == a1
        pick = jnp.where(q0 | q1, 1.0, 0.0).astype(BF)
        scale = jnp.where(q0, w0, jnp.where(q1, w1, 0.0))
        scale = jnp.sum(scale, axis=1, keepdims=True)
        return (dot(pick, og) * scale).astype(BF)

    copies = []
    for b in range(4):
        block = rows_of(256 * b, 256, m0, m1)
        peers = slice(16 * b, 16 * b + 16)
        for c in range(COLS):
            out_ref[peers, 16 * c : 16 * c + 16, :] = block[:, 128 * c : 128 * c + 128].reshape(
                16, 16, 128
            )
        main = slice(0, 16 * COLS)
        copies.append(begin(out_ref.at[peers, main], to_ref.at[peers, main], sems.at[b]))
    tail = pack_tail(rows_of(0, 128, t0, t1)).astype(BF)
    out_ref[:, 16 * COLS : MSG, :] = tail.reshape(PEERS, 16, 128)
    rest = slice(16 * COLS, MSG)
    copies.append(begin(out_ref.at[:, rest], to_ref.at[:, rest], sems.at[4]))
    for copy in copies:
        copy.wait()


def call(
    kernel,
    outs,
    args,
    flops,
    nbytes,
    scalar=None,
    scratch=(),
    name=None,
    limit=8,
    hbm_outs=(),
    hbm_ins=(),
    aliases=None,
):
    vmem = pl.BlockSpec(memory_space=pltpu.VMEM)
    far = pl.BlockSpec(memory_space=pltpu.HBM)
    in_specs = [far if i in hbm_ins else vmem for i in range(len(args))]
    if scalar is not None:
        in_specs = [pl.BlockSpec(memory_space=pltpu.SMEM)] + in_specs
        args = (scalar, *args)
    return pl.pallas_call(
        kernel,
        out_shape=outs,
        in_specs=in_specs,
        out_specs=[far if i in hbm_outs else vmem for i in range(len(outs))],
        scratch_shapes=list(scratch),
        input_output_aliases=aliases or {},
        compiler_params=pltpu.CompilerParams(vmem_limit_bytes=limit * 1024 * 1024),
        cost_estimate=cost(flops, nbytes),
        name=name,
    )(*args)


def sds(shape, dtype):
    return jax.ShapeDtypeStruct(shape, dtype)


def dispatch(tp, routes_t, weights_t, out_grad):
    dma = pltpu.SemaphoreType.DMA
    return call(
        dispatch_kernel,
        [sds((PEERS, MSG, 128), BF)],
        (routes_t, weights_t, out_grad),
        10**9,
        3 * 10**6,
        scalar=tp,
        scratch=[
            pltpu.VMEM((2, TOK), jnp.int32),
            pltpu.VMEM((2, TOK), F32),
            pltpu.VMEM((TOK, HALF), BF),
            pltpu.VMEM((PEERS, MSG, 128), BF),
            dma((5,)),
            dma((3,)),
        ],
        hbm_ins=(0, 1, 2),
        hbm_outs=(0,),
        limit=60,
        name="dispatch",
    )[0]


def half_of(tp_ref, other=False):
    half = 1 - tp_ref[0] if other else tp_ref[0]
    return pl.ds(pl.multiple_of(half * HALF, HALF), HALF)


def combine_kernel(tp_ref, meta_ref, ret_ref, og_ref, out_ref):
    meta = meta_ref[...].astype(jnp.int32)
    e0, s0, e1, s1 = (meta[:, k : k + 1] for k in range(4))
    m0 = jnp.where(s0 < MAIN, e0 * MAIN + s0, -1)
    m1 = jnp.where(s1 < MAIN, e1 * MAIN + s1, -1)
    t0 = jnp.where(s0 >= MAIN, e0 * TAIL + s0 - MAIN, -1)
    t1 = jnp.where(s1 >= MAIN, e1 * TAIL + s1 - MAIN, -1)
    lanes = iota((TOK, 1024), 1)
    pick = jnp.where((lanes == m0) | (lanes == m1), 1.0, 0.0).astype(BF)
    tail = ret_ref[:, 16 * COLS : MSG, :].reshape(1024, 128)
    few = iota((TOK, 128), 1)
    tail_pick = jnp.where((few == t0) | (few == t1), 1.0, 0.0).astype(BF)
    at = iota((128, 1024), 1) - tail_rows((128, 1024), 0)

    for c in range(0, COLS, 2):
        pair = [ret_ref[:, 16 * k : 16 * k + 16, :].reshape(1024, 128) for k in (c, c + 1)]
        moe = dot(pick, jnp.concatenate(pair, axis=1))
        masks = [jnp.where(at == k, 1.0, 0.0).astype(BF) for k in (c, c + 1)]
        rest = jnp.concatenate([dot(m, tail).astype(BF) for m in masks], axis=1)
        moe = moe + dot(tail_pick, rest)
        own = og_ref[:, pl.ds(pl.multiple_of(tp_ref[0] * HALF + c * 128, 256), 256)]
        out_ref[:, 128 * c : 128 * c + 256] = (own.astype(F32) + moe).astype(BF)


def combine_rows(tp, meta, returned, out_grad):
    return call(
        combine_kernel,
        [sds((TOK, HALF), BF)],
        (meta, returned, out_grad),
        10**9,
        3 * 10**6,
        scalar=tp,
        name="combine",
    )[0]


def place_rows(msg_ref, arr_ref):
    for c in range(COLS):
        main = msg_ref[:, 16 * c : 16 * c + 16, :].reshape(1024, 128)
        arr_ref[0:1024, 128 * c : 128 * c + 128] = main
    tail = msg_ref[:, 16 * COLS : MSG, :].reshape(1024, 128)
    at = iota((128, 1024), 1) - tail_rows((128, 1024), 0)
    for c in range(COLS):
        mask = jnp.where(at == c, 1.0, 0.0).astype(BF)
        arr_ref[1024:1152, 128 * c : 128 * c + 128] = dot(mask, tail).astype(BF)


def order_kernel(in_ref, out_ref):
    i, j = iota((256, 256), 0), iota((256, 256), 1)
    turn = jnp.where((i // 16 == j % 16) & (i % 16 == j // 16), 1.0, 0.0).astype(BF)
    for b in range(4):
        x = in_ref[0:MAIN, 16 * b : 16 * b + 16, :].reshape(256, -1)
        out_ref[256 * b : 256 * b + 256, :] = dot(turn, x).astype(BF)
    i, j = iota((128, 128), 0), iota((128, 128), 1)
    turn = jnp.where((i // 2 == j % 64) & (i % 2 == j // 64), 1.0, 0.0).astype(BF)
    x = in_ref[MAIN:CAP, :, :].reshape(128, -1)
    out_ref[1024:1152, :] = dot(turn, x).astype(BF)


def ordered_rows(rows):
    width = rows.shape[-1]
    return call(
        order_kernel,
        [sds((PEERS * CAP, width), BF)],
        (jnp.transpose(rows, (1, 0, 2)),),
        10**9,
        10**7,
        limit=16,
        name="ordered_rows",
    )[0]


def first_half_kernel(tp_ref, mine_ref, down_ref, arr_ref, part_ref):
    place_rows(mine_ref, arr_ref)
    part_ref[...] = dot(arr_ref[...], down_ref[:, half_of(tp_ref)], NT)


def second_half_kernel(
    tp_ref, other_ref, down_ref, part_ref, a1_ref, a2_ref, arr_ref, gg_ref, ug_ref
):
    place_rows(other_ref, arr_ref)
    act_grad = part_ref[...] + dot(arr_ref[...], down_ref[:, half_of(tp_ref, True)], NT)
    gg_ref[...] = (act_grad * a1_ref[...]).astype(BF)
    ug_ref[...] = (act_grad * a2_ref[...]).astype(BF)


def hidden_grads(tp, mine, other, down, a1, a2):
    rows = PEERS * CAP
    own_cols, part = call(
        first_half_kernel,
        [sds((rows, HALF), BF), sds((rows, FH), F32)],
        (mine, down),
        2 * 10**9,
        10**7,
        scalar=tp,
        name="hidden_first",
    )
    other_cols, gg, ug = call(
        second_half_kernel,
        [sds((rows, HALF), BF), sds((rows, FH), BF), sds((rows, FH), BF)],
        (other, down, part, a1, a2),
        2 * 10**9,
        10**7,
        scalar=tp,
        name="hidden_second",
    )
    return (own_cols, other_cols), gg, ug


def down_kernel(tp_ref, act_ref, own_ref, other_ref, out_ref):
    def step(n, carry):
        cols = pl.ds(pl.multiple_of(256 * n, 256), 256)
        for other, ref in ((False, own_ref), (True, other_ref)):
            half = 1 - tp_ref[0] if other else tp_ref[0]
            to = pl.ds(pl.multiple_of(half * HALF + 256 * n, 256), 256)
            out_ref[:, to] = dot(act_ref[...], ref[:, cols], TN).astype(BF)
        return carry

    lax.fori_loop(0, 4, step, 0)


def down_grad(tp, act, arrived):
    return call(
        down_kernel,
        [sds((FH, 2 * HALF), BF)],
        (act, *arrived),
        2 * 10**9,
        10**7,
        scalar=tp,
        name="down_grad",
    )[0]


def span_kernel(other, half_ref, gg_ref, ug_ref, gw_ref, uw_ref, out_ref, tail_ref):
    base = (1 - half_ref[0] if other else half_ref[0]) * HALF

    def block(n):
        cols = pl.ds(pl.multiple_of(base + 256 * n, 256), 256)
        d = dot(gg_ref[...], gw_ref[cols, :], NT) + dot(ug_ref[...], uw_ref[cols, :], NT)
        d = d.astype(BF)
        for k in range(2):
            c = 2 * n + k
            part = d[:, 128 * k : 128 * k + 128]
            rows = pl.ds(pl.multiple_of(16 * c, 16), 16)
            out_ref[:, rows, :] = part[:1024].reshape(PEERS, 16, 128)
            tail_ref[:, pl.ds(pl.multiple_of(128 * c, 128), 128)] = part[1024:]

    def step(n, carry):
        block(2 * n)
        block(2 * n + 1)
        return carry

    lax.fori_loop(0, 2, step, 0)
    tail = pack_tail(tail_ref[...]).astype(BF)
    out_ref[:, 16 * COLS : MSG, :] = tail.reshape(PEERS, 16, 128)


def span_half(tp, other, gg, ug, gw, uw):
    return call(
        functools.partial(span_kernel, other),
        [sds((PEERS, MSG, 128), BF)],
        (gg, ug, gw, uw),
        4 * 10**9,
        10**7,
        scalar=tp,
        scratch=[pltpu.VMEM((128, HALF), BF)],
        name="span_half",
    )[0]


def decay_sums(decay):
    upto = jnp.where(iota((TOK, TOK), 0) <= iota((TOK, TOK), 1), 1.0, 0.0)
    down = jnp.where(iota((TOK, TOK), 0) >= iota((TOK, TOK), 1), 1.0, 0.0)
    return dotp(decay, upto), dotp(down, decay, NT)


def decay_weights(cum, cum_t, h):
    causal = iota((TOK, TOK), 0) >= iota((TOK, TOK), 1)
    spread = cum_t[:, h : h + 1] - cum[h : h + 1, :]
    return jnp.where(causal, jnp.exp(jnp.where(causal, spread, 0.0)), 0.0)


def head(h):
    return slice(HD * h, HD * h + HD)


def group(g):
    return slice(NS * g, NS * g + NS)


def forward_kernel(
    v_ref, k_ref, q_ref, decay_ref, gate_ref, e_ref, routes_ref,
    core_ref, mixed_ref, meta_ref, fade_ref, cum_ref,
):
    r0, r1, f0, f1 = slots(routes_ref[...])
    zero = jnp.zeros((4, TOK), F32)
    table = jnp.concatenate([r0.astype(F32), f0, r1.astype(F32), f1, zero], axis=0).astype(BF)
    eye = jnp.where(iota((TOK, TOK), 0) == iota((TOK, TOK), 1), 1.0, 0.0).astype(BF)
    meta_ref[...] = dot(eye, table, NT)
    cum, cum_t = decay_sums(decay_ref[...])
    cum_ref[...] = cum
    fade_ref[:, 2 * HEADS : 3 * HEADS] = cum_t
    fade_ref[:, 0:HEADS] = jnp.exp(cum_t)
    fade_ref[:, HEADS : 2 * HEADS] = jnp.exp(cum_t[TOK - 1 : TOK, :] - cum_t)
    for g in range(GROUPS):
        q, k = q_ref[:, group(g)], k_ref[:, group(g)]
        scores = dot(q, k, NT)
        for h in range(PER_GROUP * g, PER_GROUP * g + PER_GROUP):
            m = scores * decay_weights(cum, cum_t, h)
            within = dot2(m, v_ref[:, head(h)])
            carried = dot2r(q, e_ref[h], NT)
            core = within + carried * jnp.exp(cum_t[:, h : h + 1])
            core_ref[:, head(h)] = core
            gate = gate_ref[:, head(h)].astype(F32)
            mixed_ref[:, head(h)] = (core * (gate * jax.nn.sigmoid(gate))).astype(BF)


def low_part(a, hi):
    return a - hi.astype(F32)


def cotangent_kernel(
    tp_ref, mine_ref, other_ref, ow_ref, core_ref, gate_ref, decay_ref, q_ref, fade_ref,
    hidden_ref, dcore_ref, dgate_ref, msg_ref,
):
    first = tp_ref[0] == 0
    x, y = mine_ref[...], other_ref[...]
    lo, hi = jnp.where(first, x, y), jnp.where(first, y, x)
    hidden_ref[:, :HALF] = lo
    hidden_ref[:, HALF:] = hi
    cot = dot(lo, ow_ref[:HALF, :]) + dot(hi, ow_ref[HALF:, :])
    gate = gate_ref[...].astype(F32)
    sig = jax.nn.sigmoid(gate)
    dcore = cot * (gate * sig)
    dcore_ref[...] = dcore
    dgate_ref[...] = (cot * core_ref[...] * (sig * (1.0 + gate * (1.0 - sig)))).astype(BF)
    growth = fade_ref[:, 0:HEADS]
    logs = jnp.sum(decay_ref[...], axis=1, keepdims=True)
    high, low = split(logs)
    mid, _ = split(low_part(logs, high))
    rest = low_part(logs, high) - mid.astype(F32)
    row = iota((8, 8, 128), 1)
    states = []
    for g in range(GROUPS):
        heads = range(PER_GROUP * g, PER_GROUP * g + PER_GROUP)
        grown = [dcore[:, head(h)] * growth[:, h : h + 1] for h in heads]
        states.append(dot2(jnp.concatenate(grown, axis=1), q_ref[:, group(g)], TN))
    for h in range(HEADS):
        at = HD * (h % PER_GROUP)
        state = states[h // PER_GROUP][at : at + HD]
        parts = [
            jnp.broadcast_to(p[h : h + 1, :], (8, 128)).reshape(1, 8, 128)
            for p in (high.astype(F32), mid.astype(F32), rest)
        ]
        extra = jnp.where(row == 0, parts[0], jnp.where(row == 1, parts[1], parts[2]))
        extra = jnp.where(row < 3, extra, 0.0)
        both = jnp.concatenate([state.reshape(8, 8, 128), extra], axis=1)
        msg_ref[8 * h : 8 * h + 8] = both.astype(BF)


def shares_kernel(hidden_ref, mixed_ref, msg_ref):
    def step(b, carry):
        rows = hidden_ref[:, pl.ds(pl.multiple_of(512 * b, 512), 512)]
        share = dot(rows, mixed_ref[...], TN).astype(BF)
        peers = pl.ds(pl.multiple_of(16 * b, 16), 16)
        for c in range(4):
            msg_ref[peers, 32 * c : 32 * c + 32, :] = share[:, 128 * c : 128 * c + 128].reshape(
                16, 32, 128
            )
        return carry

    lax.fori_loop(0, 4, step, 0)
    msg_ref[:, 128:136, :] = jnp.zeros((PEERS, 8, 128), BF)


def backward_kernel(
    v_far, k_far, q_far, cum_far, e_far, core_far, dcore_far, fade_far,
    dv_far, dk_far, dq_far, diff_far,
    v_ref, k_ref, q_ref, cum_ref, e_ref, core_ref, dcore_ref, fade_ref,
    dv_ref, dk_ref, dq_ref, diff_ref, sems,
):
    load(
        (
            (cum_far, cum_ref),
            (fade_far, fade_ref),
            (q_far, q_ref),
            (k_far, k_ref),
            (dcore_far, dcore_ref),
            (v_far, v_ref),
            (e_far, e_ref),
            (core_far, core_ref),
        ),
        sems,
    )
    cum, cum_t = cum_ref[...], fade_ref[:, 2 * HEADS : 3 * HEADS]
    causal = iota((TOK, TOK), 0) >= iota((TOK, TOK), 1)
    lane = iota((TOK, HEADS), 1)

    def step(g, diff):
        span = pl.ds(pl.multiple_of(g * NS, NS), NS)
        wide = pl.ds(pl.multiple_of(g * 256, 256), 256)
        q, k = q_ref[:, span], k_ref[:, span]
        v4, dcore4, core4 = v_ref[:, wide], dcore_ref[:, wide], core_ref[:, wide]
        scores = dot(q, k, NT)
        ds = jnp.zeros((TOK, TOK), F32)
        dq = jnp.zeros((TOK, NS), F32)
        dvs = []
        for i in range(PER_GROUP):
            h = g * PER_GROUP + i
            row = jnp.sum(jnp.where(iota((HEADS, TOK), 0) == h, cum, 0.0), axis=0, keepdims=True)
            col = jnp.sum(jnp.where(lane == h, cum_t, 0.0), axis=1, keepdims=True)
            w = jnp.where(causal, jnp.exp(jnp.where(causal, col - row, 0.0)), 0.0)
            dcore = dcore4[:, head(i)]
            dv = dot3(scores * w, dcore, TN)
            dvs.append(dv)
            v = v4[:, head(i)]
            change = dcore * core4[:, head(i)] - v.astype(F32) * dv
            diff = diff + jnp.where(lane == h, jnp.sum(change, axis=1, keepdims=True), 0.0)
            ds = ds + dot2(dcore, v, NT) * w
            dq = dq + dot3(dcore * jnp.exp(col), e_ref[h])
        dv_ref[:, wide] = jnp.concatenate(dvs, axis=1)
        dq_ref[:, span] = (dq + dot2(ds, k)).astype(BF)
        dk_ref[:, span] = dot2(ds, q, TN)
        return diff

    diff_ref[...] = lax.fori_loop(0, GROUPS, step, jnp.zeros((TOK, HEADS), F32))
    load(((dv_ref, dv_far), (dk_ref, dk_far), (dq_ref, dq_far), (diff_ref, diff_far)), sems)


def ending_kernel(
    in_ref, v_ref, k_ref, fade_ref, e_ref, dv_ref, dk_ref, diff_ref, gv_ref, gk_ref, gd_ref
):
    fade = fade_ref[...]
    tail = fade[:, HEADS : 2 * HEADS]
    last = fade[TOK - 1 : TOK, 0:HEADS]
    fresh, kept, diff = [], [], []
    for g in range(GROUPS):
        wide = slice(256 * g, 256 * g + 256)
        heads = range(PER_GROUP * g, PER_GROUP * g + PER_GROUP)
        state = in_ref[32 * g : 32 * g + 32, 128:136, :].astype(F32).reshape(PER_GROUP * HD, NS)
        exact = state.astype(BF)
        v = v_ref[:, wide].astype(F32)
        spread = [jnp.broadcast_to(tail[:, h : h + 1], (TOK, HD)) for h in heads]
        spread = jnp.concatenate(spread, axis=1)
        dv2 = spread * dot(k_ref[:, group(g)], exact, NT)
        gv_ref[:, wide] = (dv_ref[:, wide] + dv2).astype(BF)
        gk_ref[:, group(g)] = (dk_ref[:, group(g)] + dot2(v * spread, exact)).astype(BF)
        change = v * dv2
        for i, h in enumerate(heads):
            moved = jnp.sum(change[:, head(i)], axis=1, keepdims=True)
            diff.append(moved)
            fresh.append(jnp.sum(moved).reshape(1, 1))
            kept.append(jnp.sum(e_ref[h] * state[head(i)]).reshape(1, 1))
    diff = diff_ref[...] - jnp.concatenate(diff, axis=1)
    at_end = jnp.concatenate(fresh, axis=1) + last * jnp.concatenate(kept, axis=1)
    diff = diff + jnp.where(iota((TOK, HEADS), 0) == TOK - 1, at_end, 0.0)
    later = jnp.where(iota((TOK, TOK), 0) >= iota((TOK, TOK), 1), 1.0, 0.0)
    gd_ref[...] = dotp(diff, later, TN)


def chain_kernel(in_ref, shares_ref, out_ref):
    del shares_ref
    wide = in_ref[...].astype(F32)
    states = wide[:, 0:8, :].reshape(512, 128).astype(BF)
    logs = jnp.sum(wide[:, 8:16, :], axis=1)
    segment, entry = iota((512, PEERS), 0) // 8, iota((512, PEERS), 1)
    before = dotp(jnp.where(entry < segment, 1.0, 0.0), logs)
    through = dotp(jnp.where(entry <= segment, 1.0, 0.0), logs)
    i, j = iota((512, 512), 0), iota((512, 512), 1)
    later = (j // 8 > i // 8) & (j % 8 == i % 8)
    spread = jnp.transpose(before)[0:1, :] - through[:, 0:1]
    weights = jnp.where(later, jnp.exp(jnp.where(later, spread, 0.0)), 0.0)
    out_ref[:, 128:136, :] = dot2(weights, states).reshape(PEERS, 8, 128).astype(BF)


def share_kernel(in_ref, out_ref):
    for c in range(4):
        total = in_ref[0, 32 * c : 32 * c + 32, :].astype(F32)
        for peer in range(1, PEERS):
            total = total + in_ref[peer, 32 * c : 32 * c + 32, :].astype(F32)
        out_ref[:, 128 * c : 128 * c + 128] = total


def per_device(
    out_grad,
    routes,
    route_weights,
    routed_rows,
    gate_weight,
    up_weight,
    down_weight,
    values,
    key_side,
    query_side,
    decay_log,
    gate_in,
    entry_states,
    out_weight,
):
    tp_index = lax.axis_index("tp").astype(jnp.int32)
    tp = tp_index.reshape(1)
    gate_w, up_w, down_w = gate_weight[0], up_weight[0], down_weight[0]
    entry = entry_states[0]

    def swap(x):
        return lax.ppermute(x, "tp", [(0, 1), (1, 0)])

    message = dispatch(tp, routes.T, route_weights.T, out_grad)
    moved = lax.all_to_all(message, SP, split_axis=0, concat_axis=0, tiled=True)

    _, rows = lax.optimization_barrier((message, routed_rows[0]))
    rows = ordered_rows(rows)
    gate_pre = jnp.dot(rows, gate_w, preferred_element_type=F32)
    up_pre = jnp.dot(rows, up_w, preferred_element_type=F32)
    sig = jax.nn.sigmoid(gate_pre)
    silu = gate_pre * sig
    act = (silu * up_pre).astype(BF)
    a1 = up_pre * sig * (1.0 + gate_pre * (1.0 - sig))
    _, later_values = lax.optimization_barrier((message, values))
    core, mixer_out, meta, fade, cum = call(
        forward_kernel,
        [
            sds((TOK, HEADS * HD), F32),
            sds((TOK, HEADS * HD), BF),
            sds((TOK, 8), F32),
            sds((TOK, 3 * HEADS), F32),
            sds((HEADS, TOK), F32),
        ],
        (later_values, key_side, query_side, decay_log, gate_in, entry, routes.T),
        10**9,
        10**6,
        name="mixer_forward",
    )
    moved, rows, act, a1, silu, core, mixer_out, meta, fade, cum = lax.optimization_barrier(
        (moved, rows, act, a1, silu, core, mixer_out, meta, fade, cum)
    )

    arrived, gate_grad, up_grad = hidden_grads(tp, moved, swap(moved), down_w, a1, silu)
    for_peer = swap(span_half(tp, True, gate_grad, up_grad, gate_w, up_w))
    own_span = span_half(tp, False, gate_grad, up_grad, gate_w, up_w)
    back = (own_span.astype(F32) + for_peer.astype(F32)).astype(BF)
    returned = lax.all_to_all(back, SP, split_axis=0, concat_axis=0, tiled=True)

    _, gate_grad, up_grad, act = lax.optimization_barrier((back, gate_grad, up_grad, act))
    grad_down = down_grad(tp, act, arrived)
    grad_gate = dot(rows, gate_grad, TN).astype(BF)
    grad_up = dot(rows, up_grad, TN).astype(BF)
    returned, grad_down, grad_gate, grad_up = lax.optimization_barrier(
        (returned, grad_down, grad_gate, grad_up)
    )

    hidden_half = combine_rows(tp, meta, returned, out_grad)
    grad_hidden, dcore, dgate, own_state = call(
        cotangent_kernel,
        [
            sds((TOK, 2 * HALF), BF),
            sds((TOK, FH), F32),
            sds((TOK, FH), BF),
            sds((PEERS, 16, NS), BF),
        ],
        (
            hidden_half,
            swap(hidden_half),
            out_weight,
            core,
            gate_in,
            decay_log,
            query_side,
            fade,
        ),
        10**9,
        5 * 10**6,
        scalar=tp,
        name="mixer_cotangent",
    )
    gathered = lax.all_to_all(own_state, SP, split_axis=0, concat_axis=0, tiled=True)
    dv, dk, grad_query, diff = call(
        backward_kernel,
        [
            sds((TOK, HEADS * HD), F32),
            sds((TOK, GROUPS * NS), F32),
            sds((TOK, GROUPS * NS), BF),
            sds((TOK, HEADS), F32),
        ],
        (values, key_side, query_side, cum, entry, core, dcore, fade),
        2 * 10**9,
        10**6,
        scratch=[
            pltpu.VMEM((TOK, HEADS * HD), BF),
            pltpu.VMEM((TOK, GROUPS * NS), BF),
            pltpu.VMEM((TOK, GROUPS * NS), BF),
            pltpu.VMEM((HEADS, TOK), F32),
            pltpu.VMEM((HEADS, HD, NS), F32),
            pltpu.VMEM((TOK, HEADS * HD), F32),
            pltpu.VMEM((TOK, HEADS * HD), F32),
            pltpu.VMEM((TOK, 3 * HEADS), F32),
            pltpu.VMEM((TOK, HEADS * HD), F32),
            pltpu.VMEM((TOK, GROUPS * NS), F32),
            pltpu.VMEM((TOK, GROUPS * NS), BF),
            pltpu.VMEM((TOK, HEADS), F32),
            pltpu.SemaphoreType.DMA((8,)),
        ],
        hbm_ins=tuple(range(8)),
        hbm_outs=tuple(range(4)),
        limit=60,
        name="mixer_backward",
    )
    shares_hidden, dv, dk, grad_query, diff = lax.optimization_barrier(
        (grad_hidden, dv, dk, grad_query, diff)
    )
    shares = call(
        shares_kernel,
        [sds((PEERS, 136, NS), BF)],
        (shares_hidden, mixer_out),
        10**9,
        10**6,
        name="shares",
    )[0]
    gathered, shares, dv, dk, grad_query, diff = lax.optimization_barrier(
        (gathered, shares, dv, dk, grad_query, diff)
    )
    message = call(
        chain_kernel,
        [sds((PEERS, 136, NS), BF)],
        (gathered, shares),
        10**8,
        10**6,
        aliases={1: 0},
        name="state_chain",
    )[0]
    received = lax.all_to_all(message, SP, split_axis=0, concat_axis=0, tiled=True)
    grad_out_weight = call(
        share_kernel,
        [sds((32, FH), F32)],
        (received,),
        10**7,
        10**6,
        name="share_sum",
    )[0]
    grad_values, grad_key, grad_decay = call(
        ending_kernel,
        [
            sds((TOK, HEADS * HD), BF),
            sds((TOK, GROUPS * NS), BF),
            sds((HEADS, TOK), F32),
        ],
        (received, values, key_side, fade, entry, dv, dk, diff),
        10**9,
        10**6,
        name="mixer_ending",
    )
    return (
        grad_hidden,
        grad_gate[None],
        grad_up[None],
        grad_down[None],
        grad_out_weight,
        grad_values,
        grad_key,
        grad_query,
        grad_decay,
        dgate,
    )


def solution(mesh):
    grid = Mesh(mesh.devices.reshape(4, 4, 4, mesh.shape["tp"]), ("sp_0", "sp_1", "sp_2", "tp"))
    placed = (
        P(SP, None),
        P(SP, None),
        P(SP, None),
        P(SP, None, None, None),
        P(SP, None, "tp"),
        P(SP, None, "tp"),
        P(SP, "tp", None),
        P(SP, "tp"),
        P(SP, "tp"),
        P(SP, "tp"),
        P("tp", SP),
        P(SP, "tp"),
        P(SP, "tp", None, None),
        P(None, "tp"),
    )
    return jax.shard_map(
        per_device,
        mesh=grid,
        in_specs=placed,
        out_specs=(
            P(SP, None),
            P(SP, None, "tp"),
            P(SP, None, "tp"),
            P(SP, "tp", None),
            P(SP, "tp"),
            P(SP, "tp"),
            P(SP, "tp"),
            P(SP, "tp"),
            P("tp", SP),
            P(SP, "tp"),
        ),
        check_vma=False,
    )
```

```python
import functools

import jax
import jax.numpy as jnp
from jax import lax
from jax.experimental import pallas as pl
from jax.experimental.pallas import tpu as pltpu
from jax.sharding import Mesh
from jax.sharding import PartitionSpec as P

BF = jnp.bfloat16
F32 = jnp.float32
SP = ("sp_0", "sp_1", "sp_2")
PEERS = 64
CAP = 18
MAIN = 16
TAIL = CAP - MAIN
TOK = 224
HALF = 1024
COLS = HALF // 128
MSG = COLS * CAP
FH = 512
HEADS = 8
HD = 64
NS = 128
PER_GROUP = 4
GROUPS = 2

NT = (((1,), (1,)), ((), ()))
TN = (((0,), (0,)), ((), ()))
NN = (((1,), (0,)), ((), ()))


def cost(flops, nbytes):
    return pl.CostEstimate(flops=flops, bytes_accessed=nbytes, transcendentals=0)


def iota(shape, dim):
    return lax.broadcasted_iota(jnp.int32, shape, dim)


def dot(a, b, dims=NN):
    return lax.dot_general(a, b, dims, preferred_element_type=F32)


def split(a):
    hi = a.astype(BF)
    return hi, (a - hi.astype(F32)).astype(BF)


def dot2(a, b, dims=NN):
    hi, lo = split(a)
    return dot(hi, b, dims) + dot(lo, b, dims)


def dot2r(a, b, dims=NN):
    hi, lo = split(b)
    return dot(a, hi, dims) + dot(a, lo, dims)


def dot3(a, b, dims=NN):
    ah, al = split(a)
    bh, bl = split(b)
    return dot(ah, bh, dims) + (dot(ah, bl, dims) + dot(al, bh, dims))


def dotp(a, b, dims=NN):
    return lax.dot_general(
        a, b, dims, precision=lax.Precision.HIGHEST, preferred_element_type=F32
    )


def tail_rows(shape, row_dim):
    r = iota(shape, row_dim)
    return (r // TAIL) * 16 + (r % TAIL) * 8


def pack_tail(dt):
    place = iota((1024, 128), 0) - tail_rows((1024, 128), 1)
    out = None
    for c in range(COLS):
        mask = jnp.where(place == c, 1.0, 0.0).astype(BF)
        part = dot(mask, dt[:, c * 128 : (c + 1) * 128])
        out = part if out is None else out + part
    return out


def begin(far, near, sem):
    copy = pltpu.make_async_copy(far, near, sem)
    copy.start()
    return copy


def load(pairs, sems):
    copies = [
        pltpu.make_async_copy(far, near, sems.at[i]) for i, (far, near) in enumerate(pairs)
    ]
    for copy in copies:
        copy.start()
    for copy in copies:
        copy.wait()


def slots(routes):
    experts = iota((PEERS, TOK), 0)
    r0, r1 = routes[0:1, :], routes[1:2, :]
    h0, h1 = experts == r0, experts == r1
    counts = jnp.where(h0, 1.0, 0.0) + jnp.where(h1, 1.0, 0.0)
    before = jnp.where(iota((TOK, TOK), 0) < iota((TOK, TOK), 1), 1.0, 0.0).astype(BF)
    earlier = dot(counts.astype(BF), before)
    f0 = jnp.sum(jnp.where(h0, earlier, 0.0), axis=0, keepdims=True)
    f1 = jnp.sum(jnp.where(h1, earlier, 0.0), axis=0, keepdims=True)
    return r0, r1, f0, f1


def dispatch_kernel(
    tp_ref, far_routes, far_w, far_og, to_ref, routes_ref, w_ref, og_ref, out_ref, sems, in_sems
):
    own = half_of(tp_ref)
    load_routes = begin(far_routes, routes_ref, in_sems.at[0])
    load_w = begin(far_w, w_ref, in_sems.at[1])
    load_og = begin(far_og.at[:, own], og_ref, in_sems.at[2])
    load_routes.wait()
    r0, r1, f0, f1 = slots(routes_ref[...])
    load_w.wait()
    w0, w1 = w_ref[0:1, :], w_ref[1:2, :]
    s0, s1 = f0.astype(jnp.int32), f1.astype(jnp.int32)
    m0 = jnp.where(s0 < MAIN, r0 * MAIN + s0, -1)
    m1 = jnp.where(s1 < MAIN, r1 * MAIN + s1, -1)
    t0 = jnp.where(s0 >= MAIN, r0 * TAIL + s0 - MAIN, -1)
    t1 = jnp.where(s1 >= MAIN, r1 * TAIL + s1 - MAIN, -1)
    load_og.wait()
    og = og_ref[...]

    def rows_of(first, count, a0, a1):
        rows = iota((count, TOK), 0) + first
        q0, q1 = rows == a0, rows == a1
        pick = jnp.where(q0 | q1, 1.0, 0.0).astype(BF)
        scale = jnp.where(q0, w0, jnp.where(q1, w1, 0.0))
        scale = jnp.sum(scale, axis=1, keepdims=True)
        return (dot(pick, og) * scale).astype(BF)

    copies = []
    for b in range(4):
        block = rows_of(256 * b, 256, m0, m1)
        peers = slice(16 * b, 16 * b + 16)
        for c in range(COLS):
            out_ref[peers, 16 * c : 16 * c + 16, :] = block[:, 128 * c : 128 * c + 128].reshape(
                16, 16, 128
            )
        main = slice(0, 16 * COLS)
        copies.append(begin(out_ref.at[peers, main], to_ref.at[peers, main], sems.at[b]))
    tail = pack_tail(rows_of(0, 128, t0, t1)).astype(BF)
    out_ref[:, 16 * COLS : MSG, :] = tail.reshape(PEERS, 16, 128)
    rest = slice(16 * COLS, MSG)
    copies.append(begin(out_ref.at[:, rest], to_ref.at[:, rest], sems.at[4]))
    for copy in copies:
        copy.wait()


def call(
    kernel,
    outs,
    args,
    flops,
    nbytes,
    scalar=None,
    scratch=(),
    name=None,
    limit=8,
    hbm_outs=(),
    hbm_ins=(),
    aliases=None,
):
    vmem = pl.BlockSpec(memory_space=pltpu.VMEM)
    far = pl.BlockSpec(memory_space=pltpu.HBM)
    in_specs = [far if i in hbm_ins else vmem for i in range(len(args))]
    if scalar is not None:
        in_specs = [pl.BlockSpec(memory_space=pltpu.SMEM)] + in_specs
        args = (scalar, *args)
    return pl.pallas_call(
        kernel,
        out_shape=outs,
        in_specs=in_specs,
        out_specs=[far if i in hbm_outs else vmem for i in range(len(outs))],
        scratch_shapes=list(scratch),
        input_output_aliases=aliases or {},
        compiler_params=pltpu.CompilerParams(vmem_limit_bytes=limit * 1024 * 1024),
        cost_estimate=cost(flops, nbytes),
        name=name,
    )(*args)


def sds(shape, dtype):
    return jax.ShapeDtypeStruct(shape, dtype)


def dispatch(tp, routes_t, weights_t, out_grad):
    dma = pltpu.SemaphoreType.DMA
    return call(
        dispatch_kernel,
        [sds((PEERS, MSG, 128), BF)],
        (routes_t, weights_t, out_grad),
        10**9,
        3 * 10**6,
        scalar=tp,
        scratch=[
            pltpu.VMEM((2, TOK), jnp.int32),
            pltpu.VMEM((2, TOK), F32),
            pltpu.VMEM((TOK, HALF), BF),
            pltpu.VMEM((PEERS, MSG, 128), BF),
            dma((5,)),
            dma((3,)),
        ],
        hbm_ins=(0, 1, 2),
        hbm_outs=(0,),
        limit=60,
        name="dispatch",
    )[0]


def half_of(tp_ref, other=False):
    half = 1 - tp_ref[0] if other else tp_ref[0]
    return pl.ds(pl.multiple_of(half * HALF, HALF), HALF)


def combine_kernel(tp_ref, meta_ref, ret_ref, og_ref, out_ref):
    meta = meta_ref[...].astype(jnp.int32)
    e0, s0, e1, s1 = (meta[:, k : k + 1] for k in range(4))
    m0 = jnp.where(s0 < MAIN, e0 * MAIN + s0, -1)
    m1 = jnp.where(s1 < MAIN, e1 * MAIN + s1, -1)
    t0 = jnp.where(s0 >= MAIN, e0 * TAIL + s0 - MAIN, -1)
    t1 = jnp.where(s1 >= MAIN, e1 * TAIL + s1 - MAIN, -1)
    lanes = iota((TOK, 1024), 1)
    pick = jnp.where((lanes == m0) | (lanes == m1), 1.0, 0.0).astype(BF)
    tail = ret_ref[:, 16 * COLS : MSG, :].reshape(1024, 128)
    few = iota((TOK, 128), 1)
    tail_pick = jnp.where((few == t0) | (few == t1), 1.0, 0.0).astype(BF)
    at = iota((128, 1024), 1) - tail_rows((128, 1024), 0)

    for c in range(0, COLS, 2):
        pair = [ret_ref[:, 16 * k : 16 * k + 16, :].reshape(1024, 128) for k in (c, c + 1)]
        moe = dot(pick, jnp.concatenate(pair, axis=1))
        masks = [jnp.where(at == k, 1.0, 0.0).astype(BF) for k in (c, c + 1)]
        rest = jnp.concatenate([dot(m, tail).astype(BF) for m in masks], axis=1)
        moe = moe + dot(tail_pick, rest)
        own = og_ref[:, pl.ds(pl.multiple_of(tp_ref[0] * HALF + c * 128, 256), 256)]
        out_ref[:, 128 * c : 128 * c + 256] = (own.astype(F32) + moe).astype(BF)


def combine_rows(tp, meta, returned, out_grad):
    return call(
        combine_kernel,
        [sds((TOK, HALF), BF)],
        (meta, returned, out_grad),
        10**9,
        3 * 10**6,
        scalar=tp,
        name="combine",
    )[0]


def place_rows(msg_ref, arr_ref):
    for c in range(COLS):
        main = msg_ref[:, 16 * c : 16 * c + 16, :].reshape(1024, 128)
        arr_ref[0:1024, 128 * c : 128 * c + 128] = main
    tail = msg_ref[:, 16 * COLS : MSG, :].reshape(1024, 128)
    at = iota((128, 1024), 1) - tail_rows((128, 1024), 0)
    for c in range(COLS):
        mask = jnp.where(at == c, 1.0, 0.0).astype(BF)
        arr_ref[1024:1152, 128 * c : 128 * c + 128] = dot(mask, tail).astype(BF)


def order_kernel(in_ref, out_ref):
    i, j = iota((256, 256), 0), iota((256, 256), 1)
    turn = jnp.where((i // 16 == j % 16) & (i % 16 == j // 16), 1.0, 0.0).astype(BF)
    for b in range(4):
        x = in_ref[0:MAIN, 16 * b : 16 * b + 16, :].reshape(256, -1)
        out_ref[256 * b : 256 * b + 256, :] = dot(turn, x).astype(BF)
    i, j = iota((128, 128), 0), iota((128, 128), 1)
    turn = jnp.where((i // 2 == j % 64) & (i % 2 == j // 64), 1.0, 0.0).astype(BF)
    x = in_ref[MAIN:CAP, :, :].reshape(128, -1)
    out_ref[1024:1152, :] = dot(turn, x).astype(BF)


def ordered_rows(rows):
    width = rows.shape[-1]
    return call(
        order_kernel,
        [sds((PEERS * CAP, width), BF)],
        (jnp.transpose(rows, (1, 0, 2)),),
        10**9,
        10**7,
        limit=16,
        name="ordered_rows",
    )[0]


def first_half_kernel(tp_ref, mine_ref, down_ref, arr_ref, part_ref):
    place_rows(mine_ref, arr_ref)
    part_ref[...] = dot(arr_ref[...], down_ref[:, half_of(tp_ref)], NT)


def second_half_kernel(
    tp_ref, other_ref, down_ref, part_ref, a1_ref, a2_ref, arr_ref, gg_ref, ug_ref
):
    place_rows(other_ref, arr_ref)
    act_grad = part_ref[...] + dot(arr_ref[...], down_ref[:, half_of(tp_ref, True)], NT)
    gg_ref[...] = (act_grad * a1_ref[...]).astype(BF)
    ug_ref[...] = (act_grad * a2_ref[...]).astype(BF)


def hidden_grads(tp, mine, other, down, a1, a2):
    rows = PEERS * CAP
    own_cols, part = call(
        first_half_kernel,
        [sds((rows, HALF), BF), sds((rows, FH), F32)],
        (mine, down),
        2 * 10**9,
        10**7,
        scalar=tp,
        name="hidden_first",
    )
    other_cols, gg, ug = call(
        second_half_kernel,
        [sds((rows, HALF), BF), sds((rows, FH), BF), sds((rows, FH), BF)],
        (other, down, part, a1, a2),
        2 * 10**9,
        10**7,
        scalar=tp,
        name="hidden_second",
    )
    return (own_cols, other_cols), gg, ug


def down_kernel(tp_ref, act_ref, own_ref, other_ref, out_ref):
    def step(n, carry):
        cols = pl.ds(pl.multiple_of(256 * n, 256), 256)
        for other, ref in ((False, own_ref), (True, other_ref)):
            half = 1 - tp_ref[0] if other else tp_ref[0]
            to = pl.ds(pl.multiple_of(half * HALF + 256 * n, 256), 256)
            out_ref[:, to] = dot(act_ref[...], ref[:, cols], TN).astype(BF)
        return carry

    lax.fori_loop(0, 4, step, 0)


def down_grad(tp, act, arrived):
    return call(
        down_kernel,
        [sds((FH, 2 * HALF), BF)],
        (act, *arrived),
        2 * 10**9,
        10**7,
        scalar=tp,
        name="down_grad",
    )[0]


def span_kernel(other, half_ref, gg_ref, ug_ref, gw_ref, uw_ref, out_ref, tail_ref):
    base = (1 - half_ref[0] if other else half_ref[0]) * HALF

    def block(n):
        cols = pl.ds(pl.multiple_of(base + 256 * n, 256), 256)
        d = dot(gg_ref[...], gw_ref[cols, :], NT) + dot(ug_ref[...], uw_ref[cols, :], NT)
        d = d.astype(BF)
        for k in range(2):
            c = 2 * n + k
            part = d[:, 128 * k : 128 * k + 128]
            rows = pl.ds(pl.multiple_of(16 * c, 16), 16)
            out_ref[:, rows, :] = part[:1024].reshape(PEERS, 16, 128)
            tail_ref[:, pl.ds(pl.multiple_of(128 * c, 128), 128)] = part[1024:]

    def step(n, carry):
        block(2 * n)
        block(2 * n + 1)
        return carry

    lax.fori_loop(0, 2, step, 0)
    tail = pack_tail(tail_ref[...]).astype(BF)
    out_ref[:, 16 * COLS : MSG, :] = tail.reshape(PEERS, 16, 128)


def span_half(tp, other, gg, ug, gw, uw):
    return call(
        functools.partial(span_kernel, other),
        [sds((PEERS, MSG, 128), BF)],
        (gg, ug, gw, uw),
        4 * 10**9,
        10**7,
        scalar=tp,
        scratch=[pltpu.VMEM((128, HALF), BF)],
        name="span_half",
    )[0]


def decay_sums(decay):
    upto = jnp.where(iota((TOK, TOK), 0) <= iota((TOK, TOK), 1), 1.0, 0.0)
    down = jnp.where(iota((TOK, TOK), 0) >= iota((TOK, TOK), 1), 1.0, 0.0)
    return dotp(decay, upto), dotp(down, decay, NT)


def decay_weights(cum, cum_t, h):
    causal = iota((TOK, TOK), 0) >= iota((TOK, TOK), 1)
    spread = cum_t[:, h : h + 1] - cum[h : h + 1, :]
    return jnp.where(causal, jnp.exp(jnp.where(causal, spread, 0.0)), 0.0)


def head(h):
    return slice(HD * h, HD * h + HD)


def group(g):
    return slice(NS * g, NS * g + NS)


def forward_kernel(
    v_ref, k_ref, q_ref, decay_ref, gate_ref, e_ref, routes_ref,
    core_ref, mixed_ref, meta_ref, fade_ref, cum_ref,
):
    r0, r1, f0, f1 = slots(routes_ref[...])
    zero = jnp.zeros((4, TOK), F32)
    table = jnp.concatenate([r0.astype(F32), f0, r1.astype(F32), f1, zero], axis=0).astype(BF)
    eye = jnp.where(iota((TOK, TOK), 0) == iota((TOK, TOK), 1), 1.0, 0.0).astype(BF)
    meta_ref[...] = dot(eye, table, NT)
    cum, cum_t = decay_sums(decay_ref[...])
    cum_ref[...] = cum
    fade_ref[:, 2 * HEADS : 3 * HEADS] = cum_t
    fade_ref[:, 0:HEADS] = jnp.exp(cum_t)
    fade_ref[:, HEADS : 2 * HEADS] = jnp.exp(cum_t[TOK - 1 : TOK, :] - cum_t)
    for g in range(GROUPS):
        q, k = q_ref[:, group(g)], k_ref[:, group(g)]
        scores = dot(q, k, NT)
        for h in range(PER_GROUP * g, PER_GROUP * g + PER_GROUP):
            m = scores * decay_weights(cum, cum_t, h)
            within = dot2(m, v_ref[:, head(h)])
            carried = dot2r(q, e_ref[h], NT)
            core = within + carried * jnp.exp(cum_t[:, h : h + 1])
            core_ref[:, head(h)] = core
            gate = gate_ref[:, head(h)].astype(F32)
            mixed_ref[:, head(h)] = (core * (gate * jax.nn.sigmoid(gate))).astype(BF)


def low_part(a, hi):
    return a - hi.astype(F32)


def own_half_kernel(
    tp_ref, mine_ref, ow_ref, core_ref, gate_ref, part_ref, rise_ref, slope_ref
):
    part_ref[...] = dot(mine_ref[...], ow_ref[half_of(tp_ref), :])
    gate = gate_ref[...].astype(F32)
    sig = jax.nn.sigmoid(gate)
    rise_ref[...] = gate * sig
    slope_ref[...] = core_ref[...] * (sig * (1.0 + gate * (1.0 - sig)))


def cotangent_kernel(
    tp_ref, mine_ref, other_ref, ow_ref, part_ref, rise_ref, slope_ref, decay_ref, q_ref, fade_ref,
    hidden_ref, dcore_ref, dgate_ref, msg_ref,
):
    first = tp_ref[0] == 0
    x, y = mine_ref[...], other_ref[...]
    hidden_ref[:, :HALF] = jnp.where(first, x, y)
    hidden_ref[:, HALF:] = jnp.where(first, y, x)
    cot = part_ref[...] + dot(y, ow_ref[half_of(tp_ref, True), :])
    dcore = cot * rise_ref[...]
    dcore_ref[...] = dcore
    dgate_ref[...] = (cot * slope_ref[...]).astype(BF)
    growth = fade_ref[:, 0:HEADS]
    logs = jnp.sum(decay_ref[...], axis=1, keepdims=True)
    high, low = split(logs)
    mid, _ = split(low_part(logs, high))
    rest = low_part(logs, high) - mid.astype(F32)
    row = iota((8, 8, 128), 1)
    states = []
    for g in range(GROUPS):
        heads = range(PER_GROUP * g, PER_GROUP * g + PER_GROUP)
        grown = [dcore[:, head(h)] * growth[:, h : h + 1] for h in heads]
        states.append(dot2(jnp.concatenate(grown, axis=1), q_ref[:, group(g)], TN))
    for h in range(HEADS):
        at = HD * (h % PER_GROUP)
        state = states[h // PER_GROUP][at : at + HD]
        parts = [
            jnp.broadcast_to(p[h : h + 1, :], (8, 128)).reshape(1, 8, 128)
            for p in (high.astype(F32), mid.astype(F32), rest)
        ]
        extra = jnp.where(row == 0, parts[0], jnp.where(row == 1, parts[1], parts[2]))
        extra = jnp.where(row < 3, extra, 0.0)
        both = jnp.concatenate([state.reshape(8, 8, 128), extra], axis=1)
        msg_ref[8 * h : 8 * h + 8] = both.astype(BF)


def shares_kernel(hidden_ref, mixed_ref, msg_ref):
    def step(b, carry):
        rows = hidden_ref[:, pl.ds(pl.multiple_of(512 * b, 512), 512)]
        share = dot(rows, mixed_ref[...], TN).astype(BF)
        peers = pl.ds(pl.multiple_of(16 * b, 16), 16)
        for c in range(4):
            msg_ref[peers, 32 * c : 32 * c + 32, :] = share[:, 128 * c : 128 * c + 128].reshape(
                16, 32, 128
            )
        return carry

    lax.fori_loop(0, 4, step, 0)
    msg_ref[:, 128:136, :] = jnp.zeros((PEERS, 8, 128), BF)


def backward_kernel(
    v_far, k_far, q_far, cum_far, e_far, core_far, dcore_far, fade_far,
    dv_far, dk_far, dq_far, diff_far,
    v_ref, k_ref, q_ref, cum_ref, e_ref, core_ref, dcore_ref, fade_ref,
    dv_ref, dk_ref, dq_ref, diff_ref, sems,
):
    load(
        (
            (cum_far, cum_ref),
            (fade_far, fade_ref),
            (q_far, q_ref),
            (k_far, k_ref),
            (dcore_far, dcore_ref),
            (v_far, v_ref),
            (e_far, e_ref),
            (core_far, core_ref),
        ),
        sems,
    )
    cum, cum_t = cum_ref[...], fade_ref[:, 2 * HEADS : 3 * HEADS]
    causal = iota((TOK, TOK), 0) >= iota((TOK, TOK), 1)
    lane = iota((TOK, HEADS), 1)

    def step(g, diff):
        span = pl.ds(pl.multiple_of(g * NS, NS), NS)
        wide = pl.ds(pl.multiple_of(g * 256, 256), 256)
        q, k = q_ref[:, span], k_ref[:, span]
        v4, dcore4, core4 = v_ref[:, wide], dcore_ref[:, wide], core_ref[:, wide]
        scores = dot(q, k, NT)
        ds = jnp.zeros((TOK, TOK), F32)
        dq = jnp.zeros((TOK, NS), F32)
        dvs = []
        for i in range(PER_GROUP):
            h = g * PER_GROUP + i
            row = jnp.sum(jnp.where(iota((HEADS, TOK), 0) == h, cum, 0.0), axis=0, keepdims=True)
            col = jnp.sum(jnp.where(lane == h, cum_t, 0.0), axis=1, keepdims=True)
            w = jnp.where(causal, jnp.exp(jnp.where(causal, col - row, 0.0)), 0.0)
            dcore = dcore4[:, head(i)]
            dv = dot3(scores * w, dcore, TN)
            dvs.append(dv)
            v = v4[:, head(i)]
            change = dcore * core4[:, head(i)] - v.astype(F32) * dv
            diff = diff + jnp.where(lane == h, jnp.sum(change, axis=1, keepdims=True), 0.0)
            ds = ds + dot2(dcore, v, NT) * w
            dq = dq + dot3(dcore * jnp.exp(col), e_ref[h])
        dv_ref[:, wide] = jnp.concatenate(dvs, axis=1)
        dq_ref[:, span] = (dq + dot2(ds, k)).astype(BF)
        dk_ref[:, span] = dot2(ds, q, TN)
        return diff

    diff_ref[...] = lax.fori_loop(0, GROUPS, step, jnp.zeros((TOK, HEADS), F32))
    load(((dv_ref, dv_far), (dk_ref, dk_far), (dq_ref, dq_far), (diff_ref, diff_far)), sems)


def ending_kernel(
    in_ref, v_ref, k_ref, fade_ref, e_ref, dv_ref, dk_ref, diff_ref, gv_ref, gk_ref, gd_ref
):
    fade = fade_ref[...]
    tail = fade[:, HEADS : 2 * HEADS]
    last = fade[TOK - 1 : TOK, 0:HEADS]
    fresh, kept, diff = [], [], []
    for g in range(GROUPS):
        wide = slice(256 * g, 256 * g + 256)
        heads = range(PER_GROUP * g, PER_GROUP * g + PER_GROUP)
        state = in_ref[32 * g : 32 * g + 32, 128:136, :].astype(F32).reshape(PER_GROUP * HD, NS)
        exact = state.astype(BF)
        v = v_ref[:, wide].astype(F32)
        spread = [jnp.broadcast_to(tail[:, h : h + 1], (TOK, HD)) for h in heads]
        spread = jnp.concatenate(spread, axis=1)
        dv2 = spread * dot(k_ref[:, group(g)], exact, NT)
        gv_ref[:, wide] = (dv_ref[:, wide] + dv2).astype(BF)
        gk_ref[:, group(g)] = (dk_ref[:, group(g)] + dot2(v * spread, exact)).astype(BF)
        change = v * dv2
        for i, h in enumerate(heads):
            moved = jnp.sum(change[:, head(i)], axis=1, keepdims=True)
            diff.append(moved)
            fresh.append(jnp.sum(moved).reshape(1, 1))
            kept.append(jnp.sum(e_ref[h] * state[head(i)]).reshape(1, 1))
    diff = diff_ref[...] - jnp.concatenate(diff, axis=1)
    at_end = jnp.concatenate(fresh, axis=1) + last * jnp.concatenate(kept, axis=1)
    diff = diff + jnp.where(iota((TOK, HEADS), 0) == TOK - 1, at_end, 0.0)
    later = jnp.where(iota((TOK, TOK), 0) >= iota((TOK, TOK), 1), 1.0, 0.0)
    gd_ref[...] = dotp(diff, later, TN)


def chain_kernel(in_ref, shares_ref, out_ref):
    del shares_ref
    wide = in_ref[...].astype(F32)
    states = wide[:, 0:8, :].reshape(512, 128).astype(BF)
    logs = jnp.sum(wide[:, 8:16, :], axis=1)
    segment, entry = iota((512, PEERS), 0) // 8, iota((512, PEERS), 1)
    before = dotp(jnp.where(entry < segment, 1.0, 0.0), logs)
    through = dotp(jnp.where(entry <= segment, 1.0, 0.0), logs)
    i, j = iota((512, 512), 0), iota((512, 512), 1)
    later = (j // 8 > i // 8) & (j % 8 == i % 8)
    spread = jnp.transpose(before)[0:1, :] - through[:, 0:1]
    weights = jnp.where(later, jnp.exp(jnp.where(later, spread, 0.0)), 0.0)
    out_ref[:, 128:136, :] = dot2(weights, states).reshape(PEERS, 8, 128).astype(BF)


def share_kernel(in_ref, out_ref):
    for c in range(4):
        total = in_ref[0, 32 * c : 32 * c + 32, :].astype(F32)
        for peer in range(1, PEERS):
            total = total + in_ref[peer, 32 * c : 32 * c + 32, :].astype(F32)
        out_ref[:, 128 * c : 128 * c + 128] = total


def per_device(
    out_grad,
    routes,
    route_weights,
    routed_rows,
    gate_weight,
    up_weight,
    down_weight,
    values,
    key_side,
    query_side,
    decay_log,
    gate_in,
    entry_states,
    out_weight,
):
    tp_index = lax.axis_index("tp").astype(jnp.int32)
    tp = tp_index.reshape(1)
    gate_w, up_w, down_w = gate_weight[0], up_weight[0], down_weight[0]
    entry = entry_states[0]

    def swap(x):
        return lax.ppermute(x, "tp", [(0, 1), (1, 0)])

    message = dispatch(tp, routes.T, route_weights.T, out_grad)
    moved = lax.all_to_all(message, SP, split_axis=0, concat_axis=0, tiled=True)

    _, rows = lax.optimization_barrier((message, routed_rows[0]))
    rows = ordered_rows(rows)
    gate_pre = jnp.dot(rows, gate_w, preferred_element_type=F32)
    up_pre = jnp.dot(rows, up_w, preferred_element_type=F32)
    sig = jax.nn.sigmoid(gate_pre)
    silu = gate_pre * sig
    act = (silu * up_pre).astype(BF)
    a1 = up_pre * sig * (1.0 + gate_pre * (1.0 - sig))
    _, later_values = lax.optimization_barrier((message, values))
    core, mixer_out, meta, fade, cum = call(
        forward_kernel,
        [
            sds((TOK, HEADS * HD), F32),
            sds((TOK, HEADS * HD), BF),
            sds((TOK, 8), F32),
            sds((TOK, 3 * HEADS), F32),
            sds((HEADS, TOK), F32),
        ],
        (later_values, key_side, query_side, decay_log, gate_in, entry, routes.T),
        10**9,
        10**6,
        name="mixer_forward",
    )
    moved, rows, act, a1, silu, core, mixer_out, meta, fade, cum = lax.optimization_barrier(
        (moved, rows, act, a1, silu, core, mixer_out, meta, fade, cum)
    )

    arrived, gate_grad, up_grad = hidden_grads(tp, moved, swap(moved), down_w, a1, silu)
    for_peer = swap(span_half(tp, True, gate_grad, up_grad, gate_w, up_w))
    own_span = span_half(tp, False, gate_grad, up_grad, gate_w, up_w)
    back = (own_span.astype(F32) + for_peer.astype(F32)).astype(BF)
    returned = lax.all_to_all(back, SP, split_axis=0, concat_axis=0, tiled=True)

    _, gate_grad, up_grad, act = lax.optimization_barrier((back, gate_grad, up_grad, act))
    grad_down = down_grad(tp, act, arrived)
    grad_gate = dot(rows, gate_grad, TN).astype(BF)
    grad_up = dot(rows, up_grad, TN).astype(BF)
    returned, grad_down, grad_gate, grad_up = lax.optimization_barrier(
        (returned, grad_down, grad_gate, grad_up)
    )

    hidden_half = combine_rows(tp, meta, returned, out_grad)
    part, rise, slope = call(
        own_half_kernel,
        [sds((TOK, FH), F32)] * 3,
        (hidden_half, out_weight, core, gate_in),
        10**9,
        5 * 10**6,
        scalar=tp,
        name="mixer_own_half",
    )
    grad_hidden, dcore, dgate, own_state = call(
        cotangent_kernel,
        [
            sds((TOK, 2 * HALF), BF),
            sds((TOK, FH), F32),
            sds((TOK, FH), BF),
            sds((PEERS, 16, NS), BF),
        ],
        (
            hidden_half,
            swap(hidden_half),
            out_weight,
            part,
            rise,
            slope,
            decay_log,
            query_side,
            fade,
        ),
        10**9,
        5 * 10**6,
        scalar=tp,
        name="mixer_cotangent",
    )
    gathered = lax.all_to_all(own_state, SP, split_axis=0, concat_axis=0, tiled=True)
    dv, dk, grad_query, diff = call(
        backward_kernel,
        [
            sds((TOK, HEADS * HD), F32),
            sds((TOK, GROUPS * NS), F32),
            sds((TOK, GROUPS * NS), BF),
            sds((TOK, HEADS), F32),
        ],
        (values, key_side, query_side, cum, entry, core, dcore, fade),
        2 * 10**9,
        10**6,
        scratch=[
            pltpu.VMEM((TOK, HEADS * HD), BF),
            pltpu.VMEM((TOK, GROUPS * NS), BF),
            pltpu.VMEM((TOK, GROUPS * NS), BF),
            pltpu.VMEM((HEADS, TOK), F32),
            pltpu.VMEM((HEADS, HD, NS), F32),
            pltpu.VMEM((TOK, HEADS * HD), F32),
            pltpu.VMEM((TOK, HEADS * HD), F32),
            pltpu.VMEM((TOK, 3 * HEADS), F32),
            pltpu.VMEM((TOK, HEADS * HD), F32),
            pltpu.VMEM((TOK, GROUPS * NS), F32),
            pltpu.VMEM((TOK, GROUPS * NS), BF),
            pltpu.VMEM((TOK, HEADS), F32),
            pltpu.SemaphoreType.DMA((8,)),
        ],
        hbm_ins=tuple(range(8)),
        hbm_outs=tuple(range(4)),
        limit=60,
        name="mixer_backward",
    )
    shares_hidden, dv, dk, grad_query, diff = lax.optimization_barrier(
        (grad_hidden, dv, dk, grad_query, diff)
    )
    shares = call(
        shares_kernel,
        [sds((PEERS, 136, NS), BF)],
        (shares_hidden, mixer_out),
        10**9,
        10**6,
        name="shares",
    )[0]
    gathered, shares, dv, dk, grad_query, diff = lax.optimization_barrier(
        (gathered, shares, dv, dk, grad_query, diff)
    )
    message = call(
        chain_kernel,
        [sds((PEERS, 136, NS), BF)],
        (gathered, shares),
        10**8,
        10**6,
        aliases={1: 0},
        name="state_chain",
    )[0]
    received = lax.all_to_all(message, SP, split_axis=0, concat_axis=0, tiled=True)
    grad_out_weight = call(
        share_kernel,
        [sds((32, FH), F32)],
        (received,),
        10**7,
        10**6,
        name="share_sum",
    )[0]
    grad_values, grad_key, grad_decay = call(
        ending_kernel,
        [
            sds((TOK, HEADS * HD), BF),
            sds((TOK, GROUPS * NS), BF),
            sds((HEADS, TOK), F32),
        ],
        (received, values, key_side, fade, entry, dv, dk, diff),
        10**9,
        10**6,
        name="mixer_ending",
    )
    return (
        grad_hidden,
        grad_gate[None],
        grad_up[None],
        grad_down[None],
        grad_out_weight,
        grad_values,
        grad_key,
        grad_query,
        grad_decay,
        dgate,
    )


def solution(mesh):
    grid = Mesh(mesh.devices.reshape(4, 4, 4, mesh.shape["tp"]), ("sp_0", "sp_1", "sp_2", "tp"))
    placed = (
        P(SP, None),
        P(SP, None),
        P(SP, None),
        P(SP, None, None, None),
        P(SP, None, "tp"),
        P(SP, None, "tp"),
        P(SP, "tp", None),
        P(SP, "tp"),
        P(SP, "tp"),
        P(SP, "tp"),
        P("tp", SP),
        P(SP, "tp"),
        P(SP, "tp", None, None),
        P(None, "tp"),
    )
    return jax.shard_map(
        per_device,
        mesh=grid,
        in_specs=placed,
        out_specs=(
            P(SP, None),
            P(SP, None, "tp"),
            P(SP, None, "tp"),
            P(SP, "tp", None),
            P(SP, "tp"),
            P(SP, "tp"),
            P(SP, "tp"),
            P(SP, "tp"),
            P("tp", SP),
            P(SP, "tp"),
        ),
        check_vma=False,
    )
```
